512 devices in a mesh: sp: 32 (over z, core), tp: 16 (over y, x).
Axes of the slice: x: 4, y: 4, z: 16, core: 2. Of those that a mesh axis runs over, the one named last changes fastest.
Arguments:
- query_a: bfloat16 [6144, 2048], P('sp', 'tp'), may hold values from -6 to 6
- key_a: bfloat16 [6144, 2048], P('sp', 'tp'), may hold values from -6 to 6
- value_a: bfloat16 [6144, 2048], P('sp', 'tp'), may hold values from -6 to 6
- query_b: bfloat16 [6144, 2048], P('sp', 'tp'), may hold values from -6 to 6
- key_b: bfloat16 [6144, 2048], P('sp', 'tp'), may hold values from -6 to 6
- value_b: bfloat16 [6144, 2048], P('sp', 'tp'), may hold values from -6 to 6
- stop_a: float32 [6144, 32], P('sp', 'tp'), may hold values from -14 to -1
- stop_b: float32 [6144, 16], P('sp', 'tp'), may hold values from -14 to -1
- out_a: bfloat16 [2048, 2048], P('tp'), may hold values from -4 to 4
- out_b: bfloat16 [2048, 2048], P('tp'), may hold values from -4 to 4
- resid: bfloat16 [6144, 2048], P('sp', 'tp'), may hold values from -20 to 20
- mix_gain: float32 [2048], P('tp'), may hold values from 0.1 to 1.9
- ffn_gain: float32 [2048], P('tp'), may hold values from 0.1 to 1.9
- routes: int32 [6144, 2], P('sp'), may hold values from 0 to 127, all different within a row; in each aligned block of 192 rows (0 to 191, 192 to 383, ...) at most 5 rows name the same one
- gates: float32 [6144, 2], P('sp'), may hold values from 0.25 to 1.5
- exp_gate: bfloat16 [128, 2048, 512], P('sp', 'tp'), may hold values from -0.125 to 0.125
- exp_up: bfloat16 [128, 2048, 512], P('sp', 'tp'), may hold values from -0.125 to 0.125
- exp_down: bfloat16 [128, 512, 2048], P('sp', None, 'tp'), may hold values from -0.25 to 0.25
- sh_gate: bfloat16 [2048, 512], P('tp'), may hold values from -0.125 to 0.125
- sh_up: bfloat16 [2048, 512], P('tp'), may hold values from -0.125 to 0.125
- sh_down: bfloat16 [512, 2048], P(None, 'tp'), may hold values from -4 to 4
Outputs:
- result: bfloat16 [6144, 2048], P('sp', 'tp')
The draws below stay inside these ranges and needn't reach their ends.
Inputs may be any that keep to these rules, and one draw needn't show every extreme that they name: `routes`: each row names 2 different experts. Within the rows of one index of sp (aligned blocks of 192 rows) no expert is named by more than 5 rows, a bound that some block reaches.
All inputs are finite; a program needn't handle non-finite values.
Results may differ from the reference program's by a relative error of at most 0.02.
Values may be sent and summed in bfloat16 or wider, within the bound.
A program may use at most 64 MiB of HBM per device.

```python
import math
import jax
import jax.numpy as jnp
import numpy as np
from jax import lax

D = 2048
HA = 32
HEAD_A = 64
HB = 16
HEAD_B = 128
F = 512
FS = 512
TOP_K = 2
TOK = 192
TOKENS = 6144
EXPERTS = 128
CAP = 5
N_SP = 32
N_TP = 16


def column_scales(key, columns):
    width = max(1, columns // 32)
    count = (columns + width - 1) // width
    levels = jnp.exp(jax.random.uniform(key, (count,), jnp.float32, math.log(0.33), math.log(3.0)))
    return levels[jnp.arange(columns) // width]


def scaled_normal(key, rows, columns, spread, scale_key):
    values = jnp.clip(jax.random.normal(key, (rows, columns), jnp.float32), -5.0, 5.0) * spread
    return values * column_scales(scale_key, columns)[None, :]


def stop_offsets(key, heads):
    parts = jax.random.split(key, 5)
    chance = jax.random.uniform(parts[0], (heads,), jnp.float32)
    slow = chance < 0.5
    base = jnp.where(slow, -math.log(TOKENS) - 0.5, -4.0)
    base = base + jax.random.uniform(parts[1], (heads,), jnp.float32, -0.5, 0.5)
    phase = jax.random.uniform(parts[2], (heads,), jnp.float32, 0.0, 2.0 * math.pi)
    position = jnp.arange(TOKENS, dtype=jnp.float32) / TOKENS
    trend = 0.8 * jnp.sin(6.0 * math.pi * position[:, None] + phase[None, :])
    count = (TOKENS + 7) // 8
    jitter = jax.random.uniform(parts[3], (count, heads), jnp.float32, -0.8, 0.8)[jnp.arange(TOKENS) // 8]
    rough = jax.random.uniform(parts[4], (TOKENS, heads), jnp.float32, -0.3, 0.3)
    return base[None, :] + trend + jitter + rough


def draw_stop_a(key, part):
    return stop_offsets(jax.random.fold_in(key, 21), HA)


def draw_stop_b(key, part):
    return stop_offsets(jax.random.fold_in(key, 22), HB)


def draw_out_a(key, part):
    spread = (HA * HEAD_A + HB * HEAD_B) ** (-0.5)
    values = scaled_normal(jax.random.fold_in(key, 31), HA * HEAD_A, D, spread, jax.random.fold_in(key, 7))
    return values.astype(jnp.bfloat16)


def draw_out_b(key, part):
    spread = (HA * HEAD_A + HB * HEAD_B) ** (-0.5)
    values = scaled_normal(jax.random.fold_in(key, 32), HB * HEAD_B, D, spread, jax.random.fold_in(key, 7))
    return values.astype(jnp.bfloat16)


def draw_resid(key, part):
    values = scaled_normal(jax.random.fold_in(key, 41), TOKENS, D, 1.0, jax.random.fold_in(key, 5))
    return values.astype(jnp.bfloat16)


def draw_sh_down(key, part):
    values = scaled_normal(jax.random.fold_in(key, 51), FS, D, FS ** (-0.5), jax.random.fold_in(key, 9))
    return values.astype(jnp.bfloat16)


def block_scale(stream_key, shape, cuts, least, top_value):
    def one(dim, blocks):
        heights = jax.random.uniform(jax.random.fold_in(jax.random.fold_in(stream_key, 6), dim), (blocks,), jnp.float32, least / len(cuts), top_value / len(cuts))
        return jnp.repeat(jnp.exp(heights), shape[dim] // blocks).reshape((-1,) + (1,) * (len(shape) - dim - 1))

    factor_of = one(*cuts[0])
    for cut in cuts[1:]:
        factor_of = factor_of * one(*cut)
    return factor_of


def deal_out(rng, own, number, rows, number_of, top, reach, skew):
    order = jax.random.permutation(rng, number_of)
    packed, ordinary = load_shares(number_of, rows * top, reach, skew, True), load_shares(number_of, rows * top, reach, skew, False)
    places = jnp.arange(number_of)

    def named(tallies, turn):
        used = int((tallies > 0).sum())
        fixed = max(1, used // 4)
        moved = fixed + (places - fixed + turn * (used - fixed)) % max(1, number_of - fixed)
        return jnp.zeros((number_of,), jnp.int32).at[order[jnp.where(places < fixed, places, moved)]].set(jnp.asarray(tallies, jnp.int32))

    tallies = jnp.where(number % 4 == 0, named(packed, number // 4), named(ordinary, number - number // 4 - 1))
    mixed = jax.random.permutation(jax.random.fold_in(own, 3), number_of)
    source_of, sink = mixed[0:number_of // 2 * 2:2], mixed[1:number_of // 2 * 2:2]
    slack = jnp.minimum(tallies[source_of] - 1, reach - tallies[sink]) // 2
    slack = jnp.where((source_of == order[0]) | (sink == order[0]) | (tallies[sink] == 0), 0, jnp.maximum(slack, 0))
    moved = jax.random.randint(jax.random.fold_in(own, 4), (number_of // 2,), 0, 1 << 20) % (slack + 1)
    tallies = tallies.at[source_of].add(-moved).at[sink].add(moved)
    labels = jnp.searchsorted(jnp.cumsum(tallies), jnp.arange(rows * top), side="right").astype(jnp.int32)
    grid = labels.reshape(top, rows).T
    grid = grid[jax.random.permutation(jax.random.fold_in(own, 1), rows)]
    turn = jax.random.randint(jax.random.fold_in(own, 2), (rows, 1), 0, top)
    return jnp.take_along_axis(grid, (jnp.arange(top)[None, :] + turn) % top, axis=1)


def load_shares(number_of, total, reach, slope, full):
    weights = [(1 << 20) // math.isqrt(standing ** slope) + 1 for standing in range(1, number_of + 1)]
    largest = reach if full else min(reach, max(-(-total // number_of), total * weights[0] // sum(weights)))
    least = 1 if total - largest >= number_of - 1 else 0
    given, surplus = [largest] + [least] * (number_of - 1), total - largest - least * (number_of - 1)
    while surplus > 0:
        movable = [i for i in range(1, number_of) if given[i] < largest] or [i for i in range(1, number_of) if given[i] < reach]
        pool, budget = sum([weights[i] for i in movable]), surplus
        for i in movable:
            more = min(reach - given[i], max(1, budget * weights[i] // pool), surplus)
            given[i] = given[i] + more
            surplus = surplus - more
    return np.array(given)


def scatter_about(stream_key, extent, deviation, most, cuts=(), kind=jnp.bfloat16):
    array = deviation * jax.random.normal(stream_key, extent, jnp.float32)
    if cuts:
        array = array * block_scale(stream_key, extent, cuts, -0.22, 0.18)
    return jnp.clip(array, -most, most).astype(kind)


def setup_inputs(seed: int = 0) -> dict:
    seeds = jax.random.split(jax.random.key(seed), 22)
    query_a = scatter_about(seeds[0], (TOKENS, HA * HEAD_A), 1.0, 6.0, ((0, 32), (1, 16)))
    key_a = scatter_about(seeds[1], (TOKENS, HA * HEAD_A), 1.0, 6.0, ((0, 32), (1, 16)))
    value_a = scatter_about(seeds[2], (TOKENS, HA * HEAD_A), 1.0, 6.0, ((0, 32), (1, 16)))
    query_b = scatter_about(seeds[3], (TOKENS, HB * HEAD_B), 1.0, 6.0, ((0, 32), (1, 16)))
    key_b = scatter_about(seeds[4], (TOKENS, HB * HEAD_B), 1.0, 6.0, ((0, 32), (1, 16)))
    value_b = scatter_about(seeds[5], (TOKENS, HB * HEAD_B), 1.0, 6.0, ((0, 32), (1, 16)))
    stop_a = draw_stop_a(jax.random.fold_in(seeds[21], 71), 0)
    stop_b = draw_stop_b(jax.random.fold_in(seeds[21], 71), 0)
    out_a = draw_out_a(jax.random.fold_in(seeds[21], 71), 0)
    out_b = draw_out_b(jax.random.fold_in(seeds[21], 71), 0)
    resid = draw_resid(jax.random.fold_in(seeds[21], 71), 0)
    mix_gain = jnp.clip(1.0 + 0.18 * jax.random.normal(seeds[11], (D,), jnp.float32), 0.1, 1.9)
    ffn_gain = jnp.clip(1.0 + 0.18 * jax.random.normal(seeds[12], (D,), jnp.float32), 0.1, 1.9)
    routes_keys = jax.random.split(jax.random.fold_in(seeds[13], 1), TOKENS // TOK)
    routes_turns = jax.random.permutation(jax.random.fold_in(seeds[13], 3), TOKENS // TOK)
    routes = jax.vmap(lambda own, number: deal_out(jax.random.fold_in(seeds[13], 2), own, number, TOK, EXPERTS, TOP_K, CAP, 1))(routes_keys, routes_turns).reshape((TOKENS, TOP_K))
    gates = jnp.clip(0.25 + 1.25 * jax.random.uniform(seeds[14], (TOKENS, TOP_K), jnp.float32) ** block_scale(seeds[14], (TOKENS, TOP_K), ((0, 32),), -0.2, 0.2), 0.25, 1.5)
    exp_gate = scatter_about(seeds[15], (EXPERTS, D, F), D ** -0.5, 0.125, ((0, 32), (1, 16)))
    exp_up = scatter_about(seeds[16], (EXPERTS, D, F), D ** -0.5, 0.125, ((0, 32), (1, 16)))
    exp_down = scatter_about(seeds[17], (EXPERTS, F, D), F ** -0.5, 0.25, ((0, 32), (2, 16)))
    sh_gate = scatter_about(seeds[18], (D, FS), D ** -0.5, 0.125, ((0, 16),))
    sh_up = scatter_about(seeds[19], (D, FS), D ** -0.5, 0.125, ((0, 16),))
    sh_down = draw_sh_down(jax.random.fold_in(seeds[21], 71), 0)
    return {"query_a": query_a, "key_a": key_a, "value_a": value_a, "query_b": query_b, "key_b": key_b, "value_b": value_b, "stop_a": stop_a, "stop_b": stop_b, "out_a": out_a, "out_b": out_b, "resid": resid, "mix_gain": mix_gain, "ffn_gain": ffn_gain, "routes": routes, "gates": gates, "exp_gate": exp_gate, "exp_up": exp_up, "exp_down": exp_down, "sh_gate": sh_gate, "sh_up": sh_up, "sh_down": sh_down}


epsilon = 1e-06

def stick_group(query, keys, values, stop, heads):
    size = query.shape[1] // heads
    scale = size ** (-0.5)
    blocks = TOKENS // TOK
    query_blocks = query.reshape(blocks, TOK, heads, size).astype(jnp.float32)
    key_blocks = keys.reshape(blocks, TOK, heads, size).astype(jnp.float32)
    value_blocks = values.reshape(blocks, TOK, heads, size).astype(jnp.float32)
    stop_blocks = stop.reshape(blocks, TOK, heads).astype(jnp.float32)
    places = jnp.arange(TOK, dtype=jnp.int32)

    def one_query_block(number):
        query_here = query_blocks[number]
        stop_here = jnp.transpose(stop_blocks[number])[:, :, None]

        def visit(offset, state):
            source = number - offset

            def work(inner):
                output, carried = inner
                safe = jnp.maximum(source, 0)
                key_here = key_blocks[safe]
                value_here = value_blocks[safe]
                scores = jnp.einsum('qhd,khd->hqk', query_here, key_here, precision=lax.Precision.HIGHEST) * scale + stop_here
                causal = (source * TOK + places)[None, :] < (number * TOK + places)[:, None]
                failing = jnp.where(causal[None], jax.nn.log_sigmoid(-scores), 0.0)
                after = lax.cumsum(failing, axis=2, reverse=True) - failing + carried[:, :, None]
                weight = jnp.where(causal[None], jnp.exp(jax.nn.log_sigmoid(scores) + after), 0.0)
                weight = lax.optimization_barrier(weight.astype(jnp.bfloat16)).astype(jnp.float32)
                output = output + jnp.einsum('hqk,khe->qhe', weight, value_here, precision=lax.Precision.HIGHEST)
                return (output, carried + lax.optimization_barrier(jnp.sum(failing, axis=2)))
            return lax.cond(source >= 0, work, lambda inner: inner, state)
        start = (jnp.zeros((TOK, heads, size), jnp.float32), jnp.zeros((heads, TOK), jnp.float32))
        output, _ = lax.fori_loop(0, blocks, visit, start)
        return output
    gathered = lax.map(one_query_block, jnp.arange(blocks, dtype=jnp.int32))
    return gathered.reshape(TOKENS, heads * size).astype(jnp.bfloat16)

def grouped_product(rows, weight):
    count = rows.shape[0]
    width = weight.shape[1]
    part_rows = rows.reshape(count, N_TP, D // N_TP).astype(jnp.float32)
    part_weight = weight.reshape(N_TP, D // N_TP, width).astype(jnp.float32)
    partial_value = jnp.einsum('rgd,gdf->grf', part_rows, part_weight, precision=lax.Precision.HIGHEST)
    rounded = lax.optimization_barrier(partial_value.astype(jnp.bfloat16))
    return lax.optimization_barrier(jnp.sum(rounded.astype(jnp.float32), axis=0))

def row_scale(values):
    return lax.rsqrt(lax.optimization_barrier(jnp.mean(values * values, axis=1, keepdims=True)) + epsilon)

def reference(query_a, key_a, value_a, query_b, key_b, value_b, stop_a, stop_b, out_a, out_b, resid, mix_gain, ffn_gain, routes, gates, exp_gate, exp_up, exp_down, sh_gate, sh_up, sh_down):
    attended_a = stick_group(query_a, key_a, value_a, stop_a, HA)
    attended_b = stick_group(query_b, key_b, value_b, stop_b, HB)
    rows_a = HA * HEAD_A // N_TP
    rows_b = HB * HEAD_B // N_TP
    sets_a = jnp.transpose(attended_a.reshape(TOKENS, N_TP, rows_a), (1, 0, 2))
    sets_b = jnp.transpose(attended_b.reshape(TOKENS, N_TP, rows_b), (1, 0, 2))
    weights_a = out_a.reshape(N_TP, rows_a, D)
    weights_b = out_b.reshape(N_TP, rows_b, D)

    def add_set(total, pieces):
        left_a, right_a, left_b, right_b = pieces
        partial_value = jnp.dot(left_a, right_a, preferred_element_type=jnp.float32)
        partial_value = partial_value + jnp.dot(left_b, right_b, preferred_element_type=jnp.float32)
        return (total + lax.optimization_barrier(partial_value.astype(jnp.bfloat16)).astype(jnp.float32), None)
    mixed, _ = lax.scan(add_set, jnp.zeros((TOKENS, D), jnp.float32), (sets_a, weights_a, sets_b, weights_b))
    branch = mixed * row_scale(mixed) * mix_gain.astype(jnp.float32)[None, :]
    stream = lax.optimization_barrier((resid.astype(jnp.float32) + branch).astype(jnp.bfloat16))
    stream_f = stream.astype(jnp.float32)
    normed = (stream_f * row_scale(stream_f) * ffn_gain.astype(jnp.float32)[None, :]).astype(jnp.bfloat16)
    pairs = routes.reshape(N_SP, TOK * TOP_K).astype(jnp.int32)
    onehot = (pairs[:, :, None] == jnp.arange(EXPERTS, dtype=jnp.int32)[None, None, :]).astype(jnp.int32)
    earlier = jnp.cumsum(onehot, axis=1) - onehot
    ranks = lax.optimization_barrier(jnp.sum(earlier * onehot, axis=2))
    group = jnp.arange(N_SP, dtype=jnp.int32)[:, None]
    index = ((pairs * N_SP + group) * CAP + ranks).reshape(-1).astype(jnp.int32)
    source_rows = jnp.repeat(jnp.arange(TOKENS, dtype=jnp.int32), TOP_K)
    buffer = jnp.zeros((EXPERTS * N_SP * CAP, D), jnp.bfloat16).at[index].set(normed[source_rows])
    buffer = buffer.reshape(EXPERTS, N_SP * CAP, D)

    def one_expert(pieces):
        rows_here, gate_here, up_here, down_here = pieces
        gate_pre = grouped_product(rows_here, gate_here)
        up_pre = grouped_product(rows_here, up_here)
        hidden = (jax.nn.silu(gate_pre) * up_pre).astype(jnp.bfloat16)
        return jnp.dot(hidden, down_here, preferred_element_type=jnp.float32).astype(jnp.bfloat16)
    produced = lax.map(one_expert, (buffer, exp_gate, exp_up, exp_down)).reshape(EXPERTS * N_SP * CAP, D)
    picked = produced[index].reshape(TOKENS, TOP_K, D).astype(jnp.float32)
    routed = lax.optimization_barrier(jnp.sum(gates.astype(jnp.float32)[:, :, None] * picked, axis=1))
    shared_gate = grouped_product(normed, sh_gate)
    shared_up = grouped_product(normed, sh_up)
    shared_hidden = (jax.nn.silu(shared_gate) * shared_up).astype(jnp.bfloat16)
    shared_out = jnp.dot(shared_hidden, sh_down, preferred_element_type=jnp.float32)
    moe = routed + shared_out
    result = stream_f + moe
    return result.astype(jnp.bfloat16)
```

```python
import functools

import jax
import jax.numpy as jnp
import numpy as np
from jax import lax
from jax.experimental import pallas as pl
from jax.experimental.pallas import tpu as pltpu
from jax.sharding import PartitionSpec as P

D = 2048
EPS = 1e-06
MESH = pl.DeviceIdType.MESH
BF = jnp.bfloat16
F32 = jnp.float32
LANES = 128
CAP = 5
PADDED = 24


def dot(a, b):
    return jnp.dot(a, b, preferred_element_type=F32)


def softplus_block(query, keys, stop, scale, later, valid):
    scores = lax.dot_general(query, keys, (((1,), (1,)), ((), ())), preferred_element_type=F32)
    z = scores * scale + stop
    sp = jnp.maximum(z, 0.0) + jnp.log(1.0 + jnp.exp(-jnp.abs(z)))
    if valid is not None:
        sp = jnp.where(valid, sp, 0.0)
    after = dot(sp.astype(BF), later)
    weight = jnp.exp(z - sp - after)
    if valid is not None:
        weight = jnp.where(valid, weight, 0.0)
    return weight.astype(BF), jnp.sum(sp, axis=1, keepdims=True)


def attention_kernel(
    nz, qa, ka, va, qb, kb, vb, sa, sb, out, buf, accn, accf, ln, later, ssu, rsu, ssd, rsd, ssp, rsp, sloc
):
    rows = qa.shape[0]
    up_steps = nz // 2
    down_steps = nz - 1 - up_steps
    last_far = nz - 2 - up_steps
    sp = lax.axis_index("sp")
    tp = lax.axis_index("tp")
    z = sp // 2
    c = sp % 2
    up_id = (2 * ((z + 1) % nz) + c, tp)
    down_id = (2 * ((z + nz - 1) % nz) + c, tp)
    pair_id = (2 * z + 1 - c, tp)
    barrier = pltpu.get_barrier_semaphore()
    for peer in (up_id, down_id, pair_id):
        pl.semaphore_signal(barrier, inc=1, device_id=peer, device_id_type=MESH)
    pl.semaphore_wait(barrier, 3)

    mine = pl.ds(pl.multiple_of(c * rows, rows), rows)
    srcs = (ka, va, kb, vb)

    def place(block, a):
        return buf.at[block, a, mine, :]

    def other(block, a):
        return buf.at[block, a, pl.ds(pl.multiple_of((1 - c) * rows, rows), rows), :]

    def up_copy(step, a, src):
        block = z + 1 - step
        return pltpu.make_async_remote_copy(
            src_ref=src, dst_ref=place(block, a), send_sem=ssu.at[step - 1, a], recv_sem=rsu.at[step - 1, a],
            device_id=up_id, device_id_type=MESH)

    def down_copy(step, a, src):
        block = (z + step - 1) % nz
        return pltpu.make_async_remote_copy(
            src_ref=src, dst_ref=place(block, a), send_sem=ssd.at[step - 1, a], recv_sem=rsd.at[step - 1, a],
            device_id=down_id, device_id_type=MESH)

    def pair_copy(index, block, a, src):
        return pltpu.make_async_remote_copy(
            src_ref=src, dst_ref=place(block, a), send_sem=ssp.at[index, a], recv_sem=rsp.at[index, a],
            device_id=pair_id, device_id_type=MESH)

    def wait_on(block_ref, sem):
        pltpu.make_async_copy(block_ref, block_ref, sem).wait()

    def sends_up(step):
        return (z < nz - 1) & (z + 1 - step >= 0)

    def sends_down(step):
        return (z + step - 1) % nz <= last_far

    def gets_up(step):
        return z - step >= 0

    def gets_down(step):
        return (z + step) % nz <= last_far

    def far(step):
        return z + step >= nz

    for a in range(4):
        @pl.when(sends_up(1))
        def _(a=a):
            up_copy(1, a, srcs[a]).start()

        @pl.when(sends_down(1))
        def _(a=a):
            down_copy(1, a, srcs[a]).start()

        pair_copy(0, z, a, srcs[a]).start()
        pltpu.make_async_copy(srcs[a], place(z, a), sloc.at[a]).start()

    wide = 2 * rows
    j = lax.broadcasted_iota(jnp.int32, (wide, wide), 0)
    s = lax.broadcasted_iota(jnp.int32, (wide, wide), 1)
    later[...] = (j > s).astype(BF)
    accf[...] = jnp.zeros_like(accf)
    half = lax.broadcasted_iota(jnp.int32, (rows, LANES), 1) < LANES // 2
    qa_all = qa[...]
    zero = jnp.zeros_like(qa_all)
    qa_heads = (jnp.where(half, qa_all, zero), jnp.where(half, zero, qa_all))

    def group_a(block, valid=None):
        keys = buf[block, 0]
        values = buf[block, 1]
        pieces = [
            softplus_block(qa_heads[h], keys, sa[:, h : h + 1], 64 ** -0.5, later[...], valid) for h in range(2)
        ]
        added = jnp.where(half, dot(pieces[0][0], values), dot(pieces[1][0], values))
        return added, jnp.where(half, pieces[0][1], pieces[1][1])

    def group_b(block, valid=None):
        weight, total = softplus_block(qb[...], buf[block, 2], sb[...], 128 ** -0.5, later[...], valid)
        return dot(weight, buf[block, 3]), jnp.broadcast_to(total, (rows, LANES))

    groups = (group_a, group_b)

    def cols(g):
        return slice(g * LANES, (g + 1) * LANES)

    def near(g, step):
        block = z - step
        for a in (2 * g, 2 * g + 1):
            wait_on(other(block, a), rsp.at[step, a])
        added, total = groups[g](block)
        accn[:, cols(g)] += jnp.exp(-ln[:, cols(g)]) * added
        ln[:, cols(g)] += total

    def distant(g, step):
        block = z + step - nz
        for a in (2 * g, 2 * g + 1):
            wait_on(other(block, a), rsp.at[up_steps + step, a])
        added, total = groups[g](block)
        accf[:, cols(g)] = jnp.exp(-total) * accf[:, cols(g)] + added

    def poll_up(step, a):
        @pl.when(gets_up(step))
        def _():
            ref = place(z - step, a)
            wait_on(ref, rsu.at[step - 1, a])

            @pl.when((step < up_steps) & (z < nz - 1))
            def _():
                up_copy(step + 1, a, ref).start()

            pair_copy(step, z - step, a, ref).start()

    def poll_down(step, a):
        @pl.when((step <= down_steps) & gets_down(step))
        def _():
            block = (z + step) % nz
            ref = place(block, a)
            wait_on(ref, rsd.at[step - 1, a])

            @pl.when(step < down_steps)
            def _():
                down_copy(step + 1, a, ref).start()

            @pl.when(far(step))
            def _():
                pair_copy(up_steps + step, block, a, ref).start()

    row_at = lax.broadcasted_iota(jnp.int32, (rows, wide), 0) + c * rows
    key_at = lax.broadcasted_iota(jnp.int32, (rows, wide), 1)
    valid = key_at < row_at
    for g in range(2):
        for a in (2 * g, 2 * g + 1):
            wait_on(place(z, a), sloc.at[a])
            wait_on(other(z, a), rsp.at[0, a])
        added, total = groups[g](z, valid)
        accn[:, cols(g)] = added
        ln[:, cols(g)] = total
        for a in (2 * g, 2 * g + 1):
            poll_up(1, a)
            poll_down(1, a)

    @pl.loop(2, up_steps + 1)
    def _(step):
        before = step - 1
        for a in range(4):
            poll_up(step, a)
            poll_down(step, a)
            g = a // 2
            if a % 2 == 0:
                @pl.when(gets_up(before))
                def _():
                    near(g, before)
            else:
                @pl.when(far(before))
                def _():
                    distant(g, before)

    @pl.when(gets_up(up_steps))
    def _():
        for g in range(2):
            near(g, up_steps)

    out[...] = (accn[...] + jnp.exp(-ln[...]) * accf[...]).astype(BF)

    for a in range(4):
        pair_copy(0, z, a, srcs[a]).wait_send()

    @pl.loop(1, up_steps + 1)
    def _(step):
        for a in range(4):
            @pl.when(sends_up(step))
            def _():
                up_copy(step, a, place(z + 1 - step, a)).wait_send()

            @pl.when(gets_up(step))
            def _():
                pair_copy(step, z - step, a, place(z - step, a)).wait_send()

    @pl.loop(1, down_steps + 1)
    def _(step):
        for a in range(4):
            @pl.when(sends_down(step))
            def _():
                down_copy(step, a, place((z + step - 1) % nz, a)).wait_send()

            @pl.when(far(step))
            def _():
                pair_copy(up_steps + step, z + step - nz, a, place(z + step - nz, a)).wait_send()


def attention(nz, *arrays):
    rows = arrays[0].shape[0]
    up_steps = nz // 2
    down_steps = nz - 1 - up_steps
    dma = pltpu.SemaphoreType.DMA
    return pl.pallas_call(
        functools.partial(attention_kernel, nz),
        out_shape=jax.ShapeDtypeStruct((rows, 2 * LANES), BF),
        in_specs=[pl.BlockSpec(memory_space=pltpu.VMEM)] * 8,
        out_specs=pl.BlockSpec(memory_space=pltpu.VMEM),
        scratch_shapes=[
            pltpu.VMEM((nz, 4, 2 * rows, LANES), BF),
            pltpu.VMEM((rows, 2 * LANES), F32),
            pltpu.VMEM((rows, 2 * LANES), F32),
            pltpu.VMEM((rows, 2 * LANES), F32),
            pltpu.VMEM((2 * rows, 2 * rows), BF),
            dma((up_steps, 4)),
            dma((up_steps, 4)),
            dma((down_steps, 4)),
            dma((down_steps, 4)),
            dma((nz, 4)),
            dma((nz, 4)),
            dma((4,)),
        ],
        compiler_params=pltpu.CompilerParams(
            collective_id=0, has_side_effects=True, vmem_limit_bytes=48 * 1024 * 1024),
    )(*arrays)


TP = ("tp",)


def sum_at_owner(x, axis, dim):
    n = lax.axis_size(axis)
    tiles = jnp.moveaxis(x.reshape(x.shape[0], n, -1), 1, 0)
    arrived = lax.all_to_all(tiles, axis, split_axis=0, concat_axis=0, tiled=True)
    return arrived.astype(F32).sum(axis=0)


def rest(attended, out_a, out_b, resid, mix_gain, ffn_gain, routes, gates, exp_gate, exp_up, exp_down, sh_gate, sh_up, sh_down):
    rows = resid.shape[0]
    n_sp = lax.axis_size("sp")
    part = dot(attended[:, :LANES], out_a) + dot(attended[:, LANES:], out_b)
    mixed = sum_at_owner(part.astype(BF), "tp", 1)
    mix_total = lax.psum(jnp.sum(mixed * mixed, axis=1), "tp")
    branch = mixed * lax.rsqrt(mix_total / D + EPS)[:, None] * mix_gain[None, :]
    stream = lax.optimization_barrier((resid.astype(F32) + branch).astype(BF))
    stream_f = stream.astype(F32)
    ffn_total = lax.psum(jnp.sum(stream_f * stream_f, axis=1), "tp")
    normed = (stream_f * lax.rsqrt(ffn_total / D + EPS)[:, None] * ffn_gain[None, :]).astype(BF)
    shared_gate = lax.psum(dot(normed, sh_gate).astype(BF), "tp").astype(F32)
    shared_up = lax.psum(dot(normed, sh_up).astype(BF), "tp").astype(F32)
    shared_hidden = (jax.nn.silu(shared_gate) * shared_up).astype(BF)
    shared_out = dot(shared_hidden, sh_down)
    local_experts = exp_gate.shape[0]
    experts = local_experts * n_sp
    top_count = routes.shape[1]
    capacity = CAP
    flat_routes = routes.reshape(-1)
    onehot = (flat_routes[:, None] == jnp.arange(experts, dtype=jnp.int32)[None, :]).astype(jnp.int32)
    earlier = jnp.cumsum(onehot, axis=0) - onehot
    slot = flat_routes * capacity + jnp.sum(earlier * onehot, axis=1)
    chooser = (slot[:, None] == jnp.arange(experts * capacity, dtype=jnp.int32)[None, :]).astype(BF)
    chooser = jnp.sum(chooser.reshape(rows, top_count, experts * capacity), axis=1)
    outgoing = jnp.einsum("rs,rc->sc", chooser, normed, preferred_element_type=F32).astype(BF)
    outgoing = outgoing.reshape(n_sp, local_experts, capacity, normed.shape[1])
    arrived = lax.all_to_all(outgoing, "sp", split_axis=0, concat_axis=0, tiled=True)
    gate_part = jnp.einsum("segd,edf->segf", arrived, exp_gate, preferred_element_type=F32)
    up_part = jnp.einsum("segd,edf->segf", arrived, exp_up, preferred_element_type=F32)
    gate_pre = lax.psum(gate_part.astype(BF), "tp").astype(F32)
    up_pre = lax.psum(up_part.astype(BF), "tp").astype(F32)
    hidden = (jax.nn.silu(gate_pre) * up_pre).astype(BF)
    produced = jnp.einsum("segf,efd->segd", hidden, exp_down, preferred_element_type=F32)
    returned = lax.all_to_all(produced.astype(BF), "sp", split_axis=0, concat_axis=0, tiled=True)
    flat_back = returned.reshape(experts * capacity, returned.shape[3])
    picked = jnp.take(flat_back, slot, axis=0).reshape(rows, top_count, returned.shape[3])
    routed = jnp.sum(gates[:, :, None] * picked.astype(F32), axis=1)
    return (stream_f + (routed + shared_out)).astype(BF)


def shards(query_a, key_a, value_a, query_b, key_b, value_b, stop_a, stop_b, *others):
    nz = lax.axis_size("sp") // 2
    attended = attention(nz, query_a, key_a, value_a, query_b, key_b, value_b, stop_a, stop_b)
    return rest(attended, *others)


def solution(mesh):
    row, col, both = P("tp", None), P("tp"), P("sp", "tp")
    in_specs = (both,) * 8 + (
        row, row, both, col, col, P("sp", None), P("sp", None),
        P("sp", "tp", None), P("sp", "tp", None), P("sp", None, "tp"), row, row, P(None, "tp"))
    return jax.shard_map(shards, mesh=mesh, in_specs=in_specs, out_specs=both, check_vma=False)
```

```python
import functools

import jax
import jax.numpy as jnp
import numpy as np
from jax import lax
from jax.experimental import pallas as pl
from jax.experimental.pallas import tpu as pltpu
from jax.sharding import PartitionSpec as P

D = 2048
EPS = 1e-06
MESH = pl.DeviceIdType.MESH
BF = jnp.bfloat16
F32 = jnp.float32
LANES = 128
CAP = 5
PADDED = 24


def dot(a, b):
    return jnp.dot(a, b, preferred_element_type=F32)


def softplus_block(query, keys, stop, scale, later, valid):
    scores = lax.dot_general(query, keys, (((1,), (1,)), ((), ())), preferred_element_type=F32)
    z = scores * scale + stop
    sp = jnp.maximum(z, 0.0) + jnp.log(1.0 + jnp.exp(-jnp.abs(z)))
    if valid is not None:
        sp = jnp.where(valid, sp, 0.0)
    after = dot(sp.astype(BF), later)
    weight = jnp.exp(z - sp - after)
    if valid is not None:
        weight = jnp.where(valid, weight, 0.0)
    return weight.astype(BF), jnp.sum(sp, axis=1, keepdims=True)


def attention_kernel(
    nz, qa, ka, va, qb, kb, vb, sa, sb, out, buf, accn, accf, ln, later, ssu, rsu, ssd, rsd, ssp, rsp, sloc
):
    rows = qa.shape[0]
    up_steps = nz // 2
    down_steps = nz - 1 - up_steps
    last_far = nz - 2 - up_steps
    sp = lax.axis_index("sp")
    tp = lax.axis_index("tp")
    z = sp // 2
    c = sp % 2
    up_id = (2 * ((z + 1) % nz) + c, tp)
    down_id = (2 * ((z + nz - 1) % nz) + c, tp)
    pair_id = (2 * z + 1 - c, tp)
    barrier = pltpu.get_barrier_semaphore()
    for peer in (up_id, down_id, pair_id):
        pl.semaphore_signal(barrier, inc=1, device_id=peer, device_id_type=MESH)
    pl.semaphore_wait(barrier, 3)

    mine = pl.ds(pl.multiple_of(c * rows, rows), rows)
    srcs = (ka, va, kb, vb)

    def place(block, a):
        return buf.at[block, a, mine, :]

    def other(block, a):
        return buf.at[block, a, pl.ds(pl.multiple_of((1 - c) * rows, rows), rows), :]

    def up_copy(step, a, src):
        block = z + 1 - step
        return pltpu.make_async_remote_copy(
            src_ref=src, dst_ref=place(block, a), send_sem=ssu.at[step - 1, a], recv_sem=rsu.at[step - 1, a],
            device_id=up_id, device_id_type=MESH)

    def down_copy(step, a, src):
        block = (z + step - 1) % nz
        return pltpu.make_async_remote_copy(
            src_ref=src, dst_ref=place(block, a), send_sem=ssd.at[step - 1, a], recv_sem=rsd.at[step - 1, a],
            device_id=down_id, device_id_type=MESH)

    def pair_copy(index, block, a, src):
        return pltpu.make_async_remote_copy(
            src_ref=src, dst_ref=place(block, a), send_sem=ssp.at[index, a], recv_sem=rsp.at[index, a],
            device_id=pair_id, device_id_type=MESH)

    def wait_on(block_ref, sem):
        pltpu.make_async_copy(block_ref, block_ref, sem).wait()

    def sends_up(step):
        return (z < nz - 1) & (z + 1 - step >= 0)

    def sends_down(step):
        return (z + step - 1) % nz <= last_far

    def gets_up(step):
        return z - step >= 0

    def gets_down(step):
        return (z + step) % nz <= last_far

    def far(step):
        return z + step >= nz

    for a in range(4):
        @pl.when(sends_up(1))
        def _(a=a):
            up_copy(1, a, srcs[a]).start()

        @pl.when(sends_down(1))
        def _(a=a):
            down_copy(1, a, srcs[a]).start()

        pair_copy(0, z, a, srcs[a]).start()
        pltpu.make_async_copy(srcs[a], place(z, a), sloc.at[a]).start()

    wide = 2 * rows
    j = lax.broadcasted_iota(jnp.int32, (wide, wide), 0)
    s = lax.broadcasted_iota(jnp.int32, (wide, wide), 1)
    later[...] = (j > s).astype(BF)
    accf[...] = jnp.zeros_like(accf)
    half = lax.broadcasted_iota(jnp.int32, (rows, LANES), 1) < LANES // 2
    qa_all = qa[...]
    zero = jnp.zeros_like(qa_all)
    qa_heads = (jnp.where(half, qa_all, zero), jnp.where(half, zero, qa_all))

    def group_a(block, valid=None):
        keys = buf[block, 0]
        values = buf[block, 1]
        pieces = [
            softplus_block(qa_heads[h], keys, sa[:, h : h + 1], 64 ** -0.5, later[...], valid) for h in range(2)
        ]
        added = jnp.where(half, dot(pieces[0][0], values), dot(pieces[1][0], values))
        return added, jnp.where(half, pieces[0][1], pieces[1][1])

    def group_b(block, valid=None):
        weight, total = softplus_block(qb[...], buf[block, 2], sb[...], 128 ** -0.5, later[...], valid)
        return dot(weight, buf[block, 3]), jnp.broadcast_to(total, (rows, LANES))

    groups = (group_a, group_b)

    def cols(g):
        return slice(g * LANES, (g + 1) * LANES)

    def near(g, step):
        block = z - step
        for a in (2 * g, 2 * g + 1):
            wait_on(other(block, a), rsp.at[step, a])
        added, total = groups[g](block)
        accn[:, cols(g)] += jnp.exp(-ln[:, cols(g)]) * added
        ln[:, cols(g)] += total

    def distant(g, step):
        block = z + step - nz
        for a in (2 * g, 2 * g + 1):
            wait_on(other(block, a), rsp.at[up_steps + step, a])
        added, total = groups[g](block)
        accf[:, cols(g)] = jnp.exp(-total) * accf[:, cols(g)] + added

    def poll_up(step, a):
        @pl.when(gets_up(step))
        def _():
            ref = place(z - step, a)
            wait_on(ref, rsu.at[step - 1, a])

            @pl.when((step < up_steps) & (z < nz - 1))
            def _():
                up_copy(step + 1, a, ref).start()

            pair_copy(step, z - step, a, ref).start()

    def poll_down(step, a):
        @pl.when((step <= down_steps) & gets_down(step))
        def _():
            block = (z + step) % nz
            ref = place(block, a)
            wait_on(ref, rsd.at[step - 1, a])

            @pl.when(step < down_steps)
            def _():
                down_copy(step + 1, a, ref).start()

            @pl.when(far(step))
            def _():
                pair_copy(up_steps + step, block, a, ref).start()

    row_at = lax.broadcasted_iota(jnp.int32, (rows, wide), 0) + c * rows
    key_at = lax.broadcasted_iota(jnp.int32, (rows, wide), 1)
    valid = key_at < row_at
    for g in range(2):
        for a in (2 * g, 2 * g + 1):
            wait_on(place(z, a), sloc.at[a])
            wait_on(other(z, a), rsp.at[0, a])
        added, total = groups[g](z, valid)
        accn[:, cols(g)] = added
        ln[:, cols(g)] = total
        for a in (2 * g, 2 * g + 1):
            poll_up(1, a)
            poll_down(1, a)

    @pl.loop(2, up_steps + 1)
    def _(step):
        before = step - 1
        for a in range(4):
            poll_up(step, a)
            poll_down(step, a)
            g = a // 2
            if a % 2 == 0:
                @pl.when(gets_up(before))
                def _():
                    near(g, before)
            else:
                @pl.when(far(before))
                def _():
                    distant(g, before)

    @pl.when(gets_up(up_steps))
    def _():
        for g in range(2):
            near(g, up_steps)

    out[...] = (accn[...] + jnp.exp(-ln[...]) * accf[...]).astype(BF)

    for a in range(4):
        pair_copy(0, z, a, srcs[a]).wait_send()

    @pl.loop(1, up_steps + 1)
    def _(step):
        for a in range(4):
            @pl.when(sends_up(step))
            def _():
                up_copy(step, a, place(z + 1 - step, a)).wait_send()

            @pl.when(gets_up(step))
            def _():
                pair_copy(step, z - step, a, place(z - step, a)).wait_send()

    @pl.loop(1, down_steps + 1)
    def _(step):
        for a in range(4):
            @pl.when(sends_down(step))
            def _():
                down_copy(step, a, place((z + step - 1) % nz, a)).wait_send()

            @pl.when(far(step))
            def _():
                pair_copy(up_steps + step, z + step - nz, a, place(z + step - nz, a)).wait_send()


def attention(nz, *arrays):
    rows = arrays[0].shape[0]
    up_steps = nz // 2
    down_steps = nz - 1 - up_steps
    dma = pltpu.SemaphoreType.DMA
    return pl.pallas_call(
        functools.partial(attention_kernel, nz),
        out_shape=jax.ShapeDtypeStruct((rows, 2 * LANES), BF),
        in_specs=[pl.BlockSpec(memory_space=pltpu.VMEM)] * 8,
        out_specs=pl.BlockSpec(memory_space=pltpu.VMEM),
        scratch_shapes=[
            pltpu.VMEM((nz, 4, 2 * rows, LANES), BF),
            pltpu.VMEM((rows, 2 * LANES), F32),
            pltpu.VMEM((rows, 2 * LANES), F32),
            pltpu.VMEM((rows, 2 * LANES), F32),
            pltpu.VMEM((2 * rows, 2 * rows), BF),
            dma((up_steps, 4)),
            dma((up_steps, 4)),
            dma((down_steps, 4)),
            dma((down_steps, 4)),
            dma((nz, 4)),
            dma((nz, 4)),
            dma((4,)),
        ],
        compiler_params=pltpu.CompilerParams(
            collective_id=0, has_side_effects=True, vmem_limit_bytes=48 * 1024 * 1024),
    )(*arrays)


def rest_kernel(
    n_sp, n_tp, att, oa, ob, resid, mg, fg, routes, gates, eg, eu, ed, sg, su, sd, tcol, rcol, out,
    part, rs, sts, st, dsp_out, dsp_in, ret_out, ret_in, shp, shr, shs, shh, xbuf, gp, gin, hs, hin, obuf, oh, smat, rmat,
    tp_send, tp_recv, sp_send, sp_recv
):
    rows = resid.shape[0]
    units = eg.shape[2]
    local = eg.shape[0]
    share = hs.shape[0]
    quarters = n_tp // local
    seats = n_sp * PADDED
    strips = rows // 16
    sp = lax.axis_index("sp")
    tp = lax.axis_index("tp")
    barrier = pltpu.get_barrier_semaphore()

    @pl.loop(1, n_tp)
    def _(k):
        pl.semaphore_signal(barrier, inc=1, device_id=(sp, (tp + k) % n_tp), device_id_type=MESH)

    @pl.loop(1, n_sp)
    def _(k):
        pl.semaphore_signal(barrier, inc=1, device_id=((sp + k) % n_sp, tp), device_id_type=MESH)

    pl.semaphore_wait(barrier, n_tp + n_sp - 2)

    def tp_copy(phase, g, src, dst):
        return pltpu.make_async_remote_copy(
            src_ref=src, dst_ref=dst, send_sem=tp_send.at[phase, g], recv_sem=tp_recv.at[phase, tp],
            device_id=(sp, g), device_id_type=MESH)

    def sp_copy(phase, d, src, dst):
        return pltpu.make_async_remote_copy(
            src_ref=src, dst_ref=dst, send_sem=sp_send.at[phase, d], recv_sem=sp_recv.at[phase, sp],
            device_id=(d, tp), device_id_type=MESH)

    def landed(ref, sem):
        pltpu.make_async_copy(ref, ref, sem).wait()

    def after_tp(k):
        return (tp + k) % n_tp

    def before_tp(k):
        return (tp + n_tp - k) % n_tp

    low, high = att[:, :LANES], att[:, LANES:]

    @pl.loop(1, n_tp + 1)
    def _(k):
        g = after_tp(k)
        cols = pl.ds(pl.multiple_of(g * LANES, LANES), LANES)
        part[g] = (dot(low, oa[:, cols]) + dot(high, ob[:, cols])).astype(BF)

        @pl.when(k < n_tp)
        def _():
            tp_copy(0, g, part.at[g], rs.at[tp]).start()

    experts = local * n_sp
    e_at = lax.broadcasted_iota(jnp.int32, (rows, experts), 1)
    named = [e_at == routes[:, k : k + 1] for k in range(2)]
    members = jnp.where(named[0] | named[1], 1.0, 0.0).astype(BF)
    r_at = lax.broadcasted_iota(jnp.int32, (rows, rows), 0)
    c_at = lax.broadcasted_iota(jnp.int32, (rows, rows), 1)
    prior = dot((c_at < r_at).astype(BF), members)
    seat_at = lax.broadcasted_iota(jnp.int32, (rows, seats), 1).astype(F32)
    wide = 2 * LANES
    line_at = lax.broadcasted_iota(jnp.int32, (seats, wide), 0).astype(F32)
    chooser = None
    for k in range(2):
        e = routes[:, k : k + 1]
        rank = jnp.sum(jnp.where(named[k], prior, 0.0), axis=1, keepdims=True)
        seat = ((e // local) * PADDED + (e % local) * CAP).astype(F32) + rank
        oh[k] = (seat_at == seat).astype(BF)
        tall = jnp.concatenate(
            [jnp.broadcast_to(seat, (rows, LANES)), jnp.full((wide - rows, LANES), -1.0, F32)], axis=0)
        line = jnp.transpose(tall)[0:1, :]
        hit = line_at == line
        chooser = hit if chooser is None else chooser | hit
    chooser = chooser.astype(BF)
    lane_at = lax.broadcasted_iota(jnp.int32, (local * n_sp * CAP, seats), 1)
    smat[...] = (lane_at == tcol[...]).astype(BF)
    lane_at = lax.broadcasted_iota(jnp.int32, (seats, local * n_sp * CAP), 1)
    rmat[...] = (lane_at == rcol[...]).astype(BF)

    def gather_rs(k, total):
        src = before_tp(k)
        landed(rs.at[src], tp_recv.at[0, src])
        return total + rs[src].astype(F32)

    mixed = lax.fori_loop(1, n_tp, gather_rs, part[tp].astype(F32))

    def row_total(which, values):
        own = jnp.broadcast_to(jnp.sum(values, axis=1, keepdims=True), (rows, LANES))
        tall = jnp.concatenate([own, jnp.zeros((wide - rows, LANES), F32)], axis=0)
        lines = jnp.transpose(tall)[0:8, :]
        sts[which] = lines

        @pl.loop(1, n_tp)
        def _(k):
            g = after_tp(k)
            tp_copy(1 + which, g, sts.at[which], st.at[which, tp]).start()

        def gather(k, total):
            src = before_tp(k)
            landed(st.at[which, src], tp_recv.at[1 + which, src])
            return total + st[which, src]

        total = lax.fori_loop(1, n_tp, gather, lines)
        return jnp.transpose(jnp.broadcast_to(total[0:1, :], (LANES, wide)))[:rows, :]

    scale = lax.rsqrt(row_total(0, mixed * mixed) / D + EPS)
    stream = (resid[...].astype(F32) + mixed * scale * mg[...]).astype(BF).astype(F32)
    scale = lax.rsqrt(row_total(1, stream * stream) / D + EPS)
    normed = (stream * scale * fg[...]).astype(BF)

    tall = jnp.concatenate([normed, jnp.zeros((wide - rows, LANES), BF)], axis=0)
    dsp_out[...] = dot(chooser, tall).reshape(n_sp, PADDED, LANES).astype(BF)

    @pl.loop(1, n_sp)
    def _(k):
        d = (sp + k) % n_sp
        sp_copy(0, d, dsp_out.at[d], dsp_in.at[sp]).start()

    dsp_in[sp] = dsp_out[sp]

    shp[:, :, :units] = dot(normed, sg[...]).reshape(strips, 16, units).astype(BF)
    shp[:, :, units:] = dot(normed, su[...]).reshape(strips, 16, units).astype(BF)

    @pl.loop(1, n_tp)
    def _(k):
        g = after_tp(k)

        @pl.when(g < strips)
        def _():
            tp_copy(3, g, shp.at[g], shr.at[tp]).start()

    def gated(total):
        gate, up = total[:, :units], total[:, units:]
        return (gate / (1.0 + jnp.exp(-gate)) * up).astype(BF)

    @pl.when(tp < strips)
    def _():
        def gather(k, total):
            src = before_tp(k)
            landed(shr.at[src], tp_recv.at[3, src])
            return total + shr[src].astype(F32)

        hidden = gated(lax.fori_loop(1, n_tp, gather, shp[tp].astype(F32)))
        shs[...] = hidden
        shh[tp] = hidden

        @pl.loop(1, n_tp)
        def _(k):
            g = after_tp(k)
            tp_copy(4, g, shs, shh.at[tp]).start()

    @pl.loop(1, n_sp)
    def _(k):
        src = (sp + n_sp - k) % n_sp
        landed(dsp_in.at[src], sp_recv.at[0, src])

    flat = dsp_in[...].astype(F32).reshape(seats, LANES).astype(BF)
    xbuf[...] = dot(smat[...], flat).reshape(local, quarters * share, LANES).astype(BF)

    @pl.loop(0, local)
    def _(i):
        e = (tp // quarters + i) % local
        x = xbuf[e]
        for half, weights in ((0, eg), (1, eu)):
            made = dot(x, weights[e]).astype(BF).astype(F32)
            for q in range(quarters):
                gp[quarters * e + q, :, half * units : (half + 1) * units] = made[q * share : (q + 1) * share].astype(BF)

        @pl.loop(0, quarters)
        def _(q):
            g = quarters * e + (tp + q) % quarters

            @pl.when(g != tp)
            def _():
                tp_copy(5, g, gp.at[g], gin.at[tp]).start()

    def gather_gate(k, total):
        src = before_tp(k)
        landed(gin.at[src], tp_recv.at[5, src])
        return total + gin[src].astype(F32)

    hidden = gated(lax.fori_loop(1, n_tp, gather_gate, gp[tp].astype(F32)))
    hs[...] = hidden
    hin[tp] = hidden

    @pl.loop(1, n_tp)
    def _(k):
        g = after_tp(k)
        tp_copy(6, g, hs, hin.at[tp]).start()

    @pl.loop(0, strips)
    def _(src):
        @pl.when(src != tp)
        def _():
            landed(shh.at[src], tp_recv.at[4, src])

    shared_out = dot(shh[...].reshape(rows, units), sd[...])

    @pl.loop(1, n_tp)
    def _(k):
        src = before_tp(k)
        landed(hin.at[src], tp_recv.at[6, src])

    for e in range(local):
        h = jnp.concatenate([hin[quarters * e + q].astype(F32) for q in range(quarters)], axis=0).astype(BF)
        obuf[e * quarters * share : (e + 1) * quarters * share, :] = dot(h, ed[e]).astype(BF)
    ret_out[...] = dot(rmat[...], obuf[...]).reshape(n_sp, PADDED, LANES).astype(BF)

    @pl.loop(1, n_sp)
    def _(k):
        d = (sp + k) % n_sp
        sp_copy(1, d, ret_out.at[d], ret_in.at[sp]).start()

    ret_in[sp] = ret_out[sp]

    @pl.loop(1, n_sp)
    def _(k):
        src = (sp + n_sp - k) % n_sp
        landed(ret_in.at[src], sp_recv.at[1, src])

    flat = ret_in[...].astype(F32).reshape(seats, LANES).astype(BF)
    routed = gates[:, 0:1] * dot(oh[0], flat) + gates[:, 1:2] * dot(oh[1], flat)
    out[...] = (stream + (routed + shared_out)).astype(BF)

    @pl.loop(1, n_tp)
    def _(k):
        g = after_tp(k)
        tp_copy(0, g, part.at[g], rs.at[tp]).wait_send()
        tp_copy(1, g, sts.at[0], st.at[0, tp]).wait_send()
        tp_copy(2, g, sts.at[1], st.at[1, tp]).wait_send()

        @pl.when(g < strips)
        def _():
            tp_copy(3, g, shp.at[g], shr.at[tp]).wait_send()

        @pl.when(tp < strips)
        def _():
            tp_copy(4, g, shs, shh.at[tp]).wait_send()

        tp_copy(5, g, gp.at[g], gin.at[tp]).wait_send()
        tp_copy(6, g, hs, hin.at[tp]).wait_send()

    @pl.loop(1, n_sp)
    def _(k):
        d = (sp + k) % n_sp
        sp_copy(0, d, dsp_out.at[d], dsp_in.at[sp]).wait_send()
        sp_copy(1, d, ret_out.at[d], ret_in.at[sp]).wait_send()


def rest(attended, *arrays):
    out_a, out_b, resid, mix_gain, ffn_gain, routes, gates, exp_gate, exp_up, exp_down, sh_gate, sh_up, sh_down = arrays
    n_sp, n_tp = lax.axis_size("sp"), lax.axis_size("tp")
    rows = resid.shape[0]
    local, _, units = exp_gate.shape
    used = n_sp * CAP
    share = local * used // n_tp
    strips = rows // 16
    seats = n_sp * PADDED
    e, s, c = np.meshgrid(np.arange(local), np.arange(n_sp), np.arange(CAP), indexing="ij")
    tcol = (s * PADDED + e * CAP + c).reshape(-1, 1).astype(np.int32)
    rcol = np.full((seats, 1), -1, np.int32)
    rcol[tcol[:, 0], 0] = np.arange(local * used)
    dma = pltpu.SemaphoreType.DMA
    vmem = pltpu.VMEM
    return pl.pallas_call(
        functools.partial(rest_kernel, n_sp, n_tp),
        out_shape=jax.ShapeDtypeStruct((rows, LANES), BF),
        in_specs=[pl.BlockSpec(memory_space=pltpu.VMEM)] * 16,
        out_specs=pl.BlockSpec(memory_space=pltpu.VMEM),
        scratch_shapes=[
            vmem((n_tp, rows, LANES), BF),
            vmem((n_tp, rows, LANES), BF),
            vmem((2, 8, 2 * LANES), F32),
            vmem((2, n_tp, 8, 2 * LANES), F32),
            vmem((n_sp, PADDED, LANES), BF),
            vmem((n_sp, PADDED, LANES), BF),
            vmem((n_sp, PADDED, LANES), BF),
            vmem((n_sp, PADDED, LANES), BF),
            vmem((strips, 16, 2 * units), BF),
            vmem((n_tp, 16, 2 * units), BF),
            vmem((16, units), BF),
            vmem((strips, 16, units), BF),
            vmem((local, used, LANES), BF),
            vmem((n_tp, share, 2 * units), BF),
            vmem((n_tp, share, 2 * units), BF),
            vmem((share, units), BF),
            vmem((n_tp, share, units), BF),
            vmem((local * used, LANES), BF),
            vmem((2, rows, seats), BF),
            vmem((local * used, seats), BF),
            vmem((seats, local * used), BF),
            dma((7, n_tp)),
            dma((7, n_tp)),
            dma((2, n_sp)),
            dma((2, n_sp)),
        ],
        compiler_params=pltpu.CompilerParams(
            collective_id=1, has_side_effects=True, vmem_limit_bytes=48 * 1024 * 1024),
    )(attended, out_a, out_b, resid, mix_gain.reshape(1, -1), ffn_gain.reshape(1, -1), routes, gates,
      exp_gate, exp_up, exp_down, sh_gate, sh_up, sh_down, jnp.asarray(tcol), jnp.asarray(rcol))


def shards(query_a, key_a, value_a, query_b, key_b, value_b, stop_a, stop_b, *others):
    nz = lax.axis_size("sp") // 2
    attended = attention(nz, query_a, key_a, value_a, query_b, key_b, value_b, stop_a, stop_b)
    return rest(attended, *others)


def solution(mesh):
    row, col, both = P("tp", None), P("tp"), P("sp", "tp")
    in_specs = (both,) * 8 + (
        row, row, both, col, col, P("sp", None), P("sp", None),
        P("sp", "tp", None), P("sp", "tp", None), P("sp", None, "tp"), row, row, P(None, "tp"))
    return jax.shard_map(shards, mesh=mesh, in_specs=in_specs, out_specs=both, check_vma=False)
```

```python
import functools

import jax
import jax.numpy as jnp
from jax import lax
from jax.experimental import pallas as pl
from jax.experimental.pallas import tpu as pltpu
from jax.sharding import PartitionSpec as P

D = 2048
EPS = 1e-06
MESH = pl.DeviceIdType.MESH
BF = jnp.bfloat16
F32 = jnp.float32
LANES = 128
CAP = 5
PADDED = 24


def dot(a, b):
    return jnp.dot(a, b, preferred_element_type=F32)


def softplus_block(query, keys, stop, scale, later, valid):
    scores = lax.dot_general(query, keys, (((1,), (1,)), ((), ())), preferred_element_type=F32)
    z = scores * scale + stop
    sp = jnp.maximum(z, 0.0) + jnp.log(1.0 + jnp.exp(-jnp.abs(z)))
    if valid is not None:
        sp = jnp.where(valid, sp, 0.0)
    after = dot(sp.astype(BF), later)
    weight = jnp.exp(z - sp - after)
    if valid is not None:
        weight = jnp.where(valid, weight, 0.0)
    return weight.astype(BF), jnp.sum(sp, axis=1, keepdims=True)


def layer_kernel(n_sp, n_tp, *refs):
    (qa_h, ka_h, va_h, qb_h, kb_h, vb_h, sa_h, sb_h, oa_h, ob_h, resid_h, mg_h, fg_h, routes_h, gates_h,
     eg, eu, ed_h, sg_h, su_h, sd_h, out,
     qa, ka, va, qb, kb, vb, sa, sb, oa, ob, resid, mg, fg, routes, gates, ed, sg, su, sd,
     buf, accn, accf, ln, later,
     part, rs, sts, st, dsp_out, dsp_in, ret_out, ret_in, shp, shr, shs, shh, xbuf, xin, wgu, hs, hin, obuf, oh,
     choose, smat, rmat,
     lsem, ssu, rsu, ssd, rsd, ssp, rsp, wsend, wrecv, wloc, tp_send, tp_recv, sp_send, sp_recv) = refs
    rows = resid.shape[0]
    local, units = ed.shape[0], ed.shape[1]
    quarters = n_tp // local
    used = n_sp * CAP
    seats = n_sp * PADDED
    strips = rows // 16
    wide = 2 * LANES
    nz = n_sp // 2
    up_steps = nz // 2
    down_steps = nz - 1 - up_steps
    last_far = nz - 2 - up_steps
    sp = lax.axis_index("sp")
    tp = lax.axis_index("tp")
    z = sp // 2
    c = sp % 2
    up_id = (2 * ((z + 1) % nz) + c, tp)
    down_id = (2 * ((z + nz - 1) % nz) + c, tp)
    pair_id = (2 * z + 1 - c, tp)
    drains = []

    barrier = pltpu.get_barrier_semaphore()

    @pl.loop(1, n_sp)
    def _(k):
        pl.semaphore_signal(barrier, inc=1, device_id=((sp + n_sp - k) % n_sp, tp), device_id_type=MESH)

    @pl.loop(1, n_tp)
    def _(k):
        pl.semaphore_signal(barrier, inc=1, device_id=(sp, (tp + k) % n_tp), device_id_type=MESH)

    staged = [
        (ka_h, ka), (va_h, va), (kb_h, kb), (vb_h, vb), (routes_h, routes), (qa_h, qa), (qb_h, qb), (sa_h, sa),
        (sb_h, sb), (oa_h, oa), (ob_h, ob), (resid_h, resid), (mg_h, mg), (fg_h, fg), (gates_h, gates),
        (ed_h, ed), (sg_h, sg), (su_h, su), (sd_h, sd)]
    loads = [pltpu.make_async_copy(a, b, lsem.at[i]) for i, (a, b) in enumerate(staged)]
    for load in loads:
        load.start()

    def column(ref, k):
        return jnp.transpose(jnp.broadcast_to(ref[k : k + 1, :].astype(F32), (LANES, rows)))

    span = 2 * rows
    j = lax.broadcasted_iota(jnp.int32, (span, span), 0)
    s = lax.broadcasted_iota(jnp.int32, (span, span), 1)
    later[...] = (j > s).astype(BF)
    accf[...] = jnp.zeros_like(accf)
    half = lax.broadcasted_iota(jnp.int32, (rows, LANES), 1) < LANES // 2

    def index_of(shape, dim):
        return lax.broadcasted_iota(jnp.int32, shape, dim).astype(F32)

    i = index_of((local * used, LANES), 0)
    e = jnp.floor((i + 0.5) * (1.0 / used))
    i = i - used * e
    g = jnp.floor((i + 0.5) * (1.0 / CAP))
    smat[...] = (index_of((local * used, seats), 1) == (g * PADDED + e * CAP + (i - CAP * g))[:, 0:1]).astype(BF)
    i = index_of((seats, LANES), 0)
    g = jnp.floor((i + 0.5) * (1.0 / PADDED))
    i = i - PADDED * g
    e = jnp.floor((i + 0.5) * (1.0 / CAP))
    target = jnp.where(e < local, e * used + g * CAP + (i - CAP * e), -1.0)
    rmat[...] = (index_of((seats, local * used), 1) == target[:, 0:1]).astype(BF)
    loads[4].wait()
    experts = local * n_sp
    e_at = index_of((rows, experts), 1)
    named_by = [column(routes, k) for k in range(2)]
    named = [e_at == named_by[k][:, 0:1] for k in range(2)]
    members = jnp.where(named[0] | named[1], 1.0, 0.0).astype(BF)
    prior = dot((index_of((rows, rows), 1) < index_of((rows, rows), 0)).astype(BF), members)
    hits = None
    for k in range(2):
        home = jnp.floor((named_by[k] + 0.5) * (1.0 / local))
        rank = jnp.sum(jnp.where(named[k], prior, 0.0), axis=1, keepdims=True)
        seat = home * PADDED + (named_by[k] - local * home) * CAP + rank
        oh[k] = (index_of((rows, seats), 1) == seat[:, 0:1]).astype(BF)
        tall = jnp.concatenate([seat, jnp.full((wide - rows, LANES), -1.0, F32)], axis=0)
        hit = index_of((seats, wide), 0) == jnp.transpose(tall)[0:1, :]
        hits = hit if hits is None else hits | hit
    choose[...] = hits.astype(BF)

    for load in loads[:4]:
        load.wait()
    pl.semaphore_wait(barrier, n_tp + n_sp - 2)

    mine = pl.ds(pl.multiple_of(c * rows, rows), rows)
    theirs = pl.ds(pl.multiple_of((1 - c) * rows, rows), rows)
    srcs = (ka, va, kb, vb)

    def place(block, a):
        return buf.at[block, a, mine, :]

    def other(block, a):
        return buf.at[block, a, theirs, :]

    def up_copy(step, a, src):
        return pltpu.make_async_remote_copy(
            src_ref=src, dst_ref=place(z + 1 - step, a), send_sem=ssu.at[step - 1, a], recv_sem=rsu.at[step - 1, a],
            device_id=up_id, device_id_type=MESH)

    def down_copy(step, a, src):
        return pltpu.make_async_remote_copy(
            src_ref=src, dst_ref=place((z + step - 1) % nz, a), send_sem=ssd.at[step - 1, a],
            recv_sem=rsd.at[step - 1, a], device_id=down_id, device_id_type=MESH)

    def pair_copy(index, block, a, src):
        return pltpu.make_async_remote_copy(
            src_ref=src, dst_ref=place(block, a), send_sem=ssp.at[index, a], recv_sem=rsp.at[index, a],
            device_id=pair_id, device_id_type=MESH)

    def landed(ref, sem):
        pltpu.make_async_copy(ref, ref, sem).wait()

    def sends_up(step):
        return (z < nz - 1) & (z + 1 - step >= 0)

    def sends_down(step):
        return (z + step - 1) % nz <= last_far

    def gets_up(step):
        return z - step >= 0

    def gets_down(step):
        return (z + step) % nz <= last_far

    def far(step):
        return z + step >= nz

    for a in range(4):
        @pl.when(sends_up(1))
        def _(a=a):
            up_copy(1, a, srcs[a]).start()

        @pl.when(sends_down(1))
        def _(a=a):
            down_copy(1, a, srcs[a]).start()

        pair_copy(0, z, a, srcs[a]).start()
        buf[z, a, mine, :] = srcs[a][...]

    def after_tp(k):
        return (tp + k) % n_tp

    def before_tp(k):
        return (tp + n_tp - k) % n_tp

    def weights_copy(h, g):
        src = (eg, eu)[h].at[g // quarters, :, pl.ds(pl.multiple_of((g % quarters) * LANES, LANES), LANES)]
        dst = wgu.at[tp, :, pl.ds(h * LANES, LANES)]
        return src, dst

    def weights_remote(h, g):
        src, dst = weights_copy(h, g)
        return pltpu.make_async_remote_copy(
            src_ref=src, dst_ref=dst, send_sem=wsend.at[h, g], recv_sem=wrecv.at[h, tp],
            device_id=(sp, g), device_id_type=MESH)

    @pl.loop(1, n_tp)
    def _(k):
        for h in range(2):
            weights_remote(h, after_tp(k)).start()

    for h in range(2):
        src, dst = weights_copy(h, tp)
        pltpu.make_async_copy(src, dst, wloc.at[h]).start()

    for load in loads[5:]:
        load.wait()
    qa_all = qa[...]
    zero = jnp.zeros_like(qa_all)
    qa_heads = (jnp.where(half, qa_all, zero), jnp.where(half, zero, qa_all))
    stops = [column(sa, 0)[:, 0:1], column(sa, 1)[:, 0:1], column(sb, 0)[:, 0:1]]

    def group_a(block, valid=None):
        keys = buf[block, 0]
        values = buf[block, 1]
        pieces = [softplus_block(qa_heads[h], keys, stops[h], 64 ** -0.5, later[...], valid) for h in range(2)]
        added = jnp.where(half, dot(pieces[0][0], values), dot(pieces[1][0], values))
        return added, jnp.where(half, pieces[0][1], pieces[1][1])

    def group_b(block, valid=None):
        weight, total = softplus_block(qb[...], buf[block, 2], stops[2], 128 ** -0.5, later[...], valid)
        return dot(weight, buf[block, 3]), jnp.broadcast_to(total, (rows, LANES))

    groups = (group_a, group_b)

    def cols(g):
        return slice(g * LANES, (g + 1) * LANES)

    def near(g, step):
        block = z - step
        for a in (2 * g, 2 * g + 1):
            landed(other(block, a), rsp.at[step, a])
        added, total = groups[g](block)
        accn[:, cols(g)] += jnp.exp(-ln[:, cols(g)]) * added
        ln[:, cols(g)] += total

    def distant(g, step):
        block = z + step - nz
        for a in (2 * g, 2 * g + 1):
            landed(other(block, a), rsp.at[up_steps + step, a])
        added, total = groups[g](block)
        accf[:, cols(g)] = jnp.exp(-total) * accf[:, cols(g)] + added

    def poll_up(step, a):
        @pl.when(gets_up(step))
        def _():
            ref = place(z - step, a)
            landed(ref, rsu.at[step - 1, a])

            @pl.when((step < up_steps) & (z < nz - 1))
            def _():
                up_copy(step + 1, a, ref).start()

            pair_copy(step, z - step, a, ref).start()

    def poll_down(step, a):
        @pl.when((step <= down_steps) & gets_down(step))
        def _():
            block = (z + step) % nz
            ref = place(block, a)
            landed(ref, rsd.at[step - 1, a])

            @pl.when(step < down_steps)
            def _():
                down_copy(step + 1, a, ref).start()

            @pl.when(far(step))
            def _():
                pair_copy(up_steps + step, block, a, ref).start()

    row_at = lax.broadcasted_iota(jnp.int32, (rows, span), 0) + c * rows
    key_at = lax.broadcasted_iota(jnp.int32, (rows, span), 1)
    valid = key_at < row_at
    for g in range(2):
        for a in (2 * g, 2 * g + 1):
            landed(other(z, a), rsp.at[0, a])
        added, total = groups[g](z, valid)
        accn[:, cols(g)] = added
        ln[:, cols(g)] = total
        for a in (2 * g, 2 * g + 1):
            poll_up(1, a)
            poll_down(1, a)

    @pl.loop(2, up_steps + 1)
    def _(step):
        before = step - 1
        for a in range(4):
            poll_up(step, a)
            poll_down(step, a)
            g = a // 2
            if a % 2 == 0:
                @pl.when(gets_up(before))
                def _():
                    near(g, before)
            else:
                @pl.when(far(before))
                def _():
                    distant(g, before)

    @pl.when(gets_up(up_steps))
    def _():
        for g in range(2):
            near(g, up_steps)

    att = (accn[...] + jnp.exp(-ln[...]) * accf[...]).astype(BF)

    @drains.append
    def _():
        for a in range(4):
            pair_copy(0, z, a, srcs[a]).wait_send()

        @pl.loop(1, up_steps + 1)
        def _(step):
            for a in range(4):
                @pl.when(sends_up(step))
                def _():
                    up_copy(step, a, place(z + 1 - step, a)).wait_send()

                @pl.when(gets_up(step))
                def _():
                    pair_copy(step, z - step, a, place(z - step, a)).wait_send()

        @pl.loop(1, down_steps + 1)
        def _(step):
            for a in range(4):
                @pl.when(sends_down(step))
                def _():
                    down_copy(step, a, place((z + step - 1) % nz, a)).wait_send()

                @pl.when(far(step))
                def _():
                    pair_copy(up_steps + step, z + step - nz, a, place(z + step - nz, a)).wait_send()

        @pl.loop(1, n_tp)
        def _(k):
            for h in range(2):
                weights_remote(h, after_tp(k)).wait_send()

    def tp_copy(phase, g, src, dst):
        return pltpu.make_async_remote_copy(
            src_ref=src, dst_ref=dst, send_sem=tp_send.at[phase, g], recv_sem=tp_recv.at[phase, tp],
            device_id=(sp, g), device_id_type=MESH)

    def sp_copy(phase, d, src, dst):
        return pltpu.make_async_remote_copy(
            src_ref=src, dst_ref=dst, send_sem=sp_send.at[phase, d], recv_sem=sp_recv.at[phase, sp],
            device_id=(d, tp), device_id_type=MESH)

    def tp_drain(phase, src, dst):
        @drains.append
        def _():
            @pl.loop(1, n_tp)
            def _(k):
                g = after_tp(k)
                tp_copy(phase, g, src(g), dst).wait_send()

    low, high = att[:, :LANES], att[:, LANES:]

    @pl.loop(1, n_tp + 1)
    def _(k):
        g = after_tp(k)
        strip = pl.ds(pl.multiple_of(g * LANES, LANES), LANES)
        part[g] = (dot(low, oa[:, strip]) + dot(high, ob[:, strip])).astype(BF)

        @pl.when(k < n_tp)
        def _():
            tp_copy(0, g, part.at[g], rs.at[tp]).start()

    tp_drain(0, lambda g: part.at[g], rs.at[tp])

    def gather_rs(k, total):
        src = before_tp(k)
        landed(rs.at[src], tp_recv.at[0, src])
        return total + rs[src].astype(F32)

    mixed = lax.fori_loop(1, n_tp, gather_rs, part[tp].astype(F32))

    gained = mixed * mg[...]
    x = resid[...].astype(F32)
    lane = lax.broadcasted_iota(jnp.int32, (rows, LANES), 1)
    own = jnp.zeros((rows, LANES), F32)
    for k, product in enumerate((mixed * mixed, x * x, x * gained, gained * gained)):
        own = jnp.where(lane == k, jnp.sum(product, axis=1, keepdims=True), own)
    lines = jnp.transpose(jnp.concatenate([own, jnp.zeros((wide - rows, LANES), F32)], axis=0))[0:8, :]
    sts[...] = lines

    @pl.loop(1, n_tp)
    def _(k):
        tp_copy(1, after_tp(k), sts, st.at[tp]).start()

    tp_drain(1, lambda g: sts, st.at[tp])

    def gather_st(k, total):
        src = before_tp(k)
        landed(st.at[src], tp_recv.at[1, src])
        return total + st[src]

    lines = lax.fori_loop(1, n_tp, gather_st, lines)
    total = jnp.transpose(jnp.concatenate([lines, jnp.zeros((LANES - 8, wide), F32)], axis=0))[:rows, :]
    scale = lax.rsqrt(total[:, 0:1] / D + EPS)
    square = total[:, 1:2] + scale * (2.0 * total[:, 2:3] + scale * total[:, 3:4])
    stream = (x + gained * scale).astype(BF).astype(F32)
    scale = lax.rsqrt(jnp.maximum(square, 0.0) / D + EPS)
    normed = (stream * scale * fg[...]).astype(BF)

    tall = jnp.concatenate([normed, jnp.zeros((wide - rows, LANES), BF)], axis=0)
    dsp_out[...] = dot(choose[...], tall).reshape(n_sp, PADDED, LANES).astype(BF)

    def sp_drain(phase, src, dst):
        @drains.append
        def _():
            @pl.loop(1, n_sp)
            def _(k):
                d = (sp + k) % n_sp
                sp_copy(phase, d, src.at[d], dst).wait_send()

    @pl.loop(1, n_sp)
    def _(k):
        d = (sp + k) % n_sp
        sp_copy(0, d, dsp_out.at[d], dsp_in.at[sp]).start()

    sp_drain(0, dsp_out, dsp_in.at[sp])
    dsp_in[sp] = dsp_out[sp]

    shp[:, :, :units] = dot(normed, sg[...]).reshape(strips, 16, units).astype(BF)
    shp[:, :, units:] = dot(normed, su[...]).reshape(strips, 16, units).astype(BF)

    @pl.loop(1, n_tp)
    def _(k):
        g = after_tp(k)

        @pl.when(g < strips)
        def _():
            tp_copy(2, g, shp.at[g], shr.at[tp]).start()

    def gated(gate, up):
        return (gate / (1.0 + jnp.exp(-gate)) * up).astype(BF)

    @pl.when(tp < strips)
    def _():
        def gather(k, total):
            src = before_tp(k)
            landed(shr.at[src], tp_recv.at[2, src])
            return total + shr[src].astype(F32)

        both = lax.fori_loop(1, n_tp, gather, shp[tp].astype(F32))
        hidden = gated(both[:, :units], both[:, units:])
        shs[...] = hidden
        shh[tp] = hidden

        @pl.loop(1, n_tp)
        def _(k):
            tp_copy(3, after_tp(k), shs, shh.at[tp]).start()

    @drains.append
    def _():
        @pl.loop(1, n_tp)
        def _(k):
            g = after_tp(k)

            @pl.when(g < strips)
            def _():
                tp_copy(2, g, shp.at[g], shr.at[tp]).wait_send()

            @pl.when(tp < strips)
            def _():
                tp_copy(3, g, shs, shh.at[tp]).wait_send()

    @pl.loop(1, n_sp)
    def _(k):
        src = (sp + n_sp - k) % n_sp
        landed(dsp_in.at[src], sp_recv.at[0, src])

    flat = dsp_in[...].astype(F32).reshape(seats, LANES).astype(BF)
    xbuf[...] = dot(smat[...], flat).reshape(local, used, LANES).astype(BF)

    @pl.loop(1, n_tp)
    def _(k):
        g = after_tp(k)
        tp_copy(4, g, xbuf.at[g // quarters], xin.at[tp]).start()

    tp_drain(4, lambda g: xbuf.at[g // quarters], xin.at[tp])
    for h in range(2):
        src, dst = weights_copy(h, tp)
        pltpu.make_async_copy(src, dst, wloc.at[h]).wait()

    def gather_x(k, total):
        src = before_tp(k)
        for h in range(2):
            landed(wgu.at[src, :, pl.ds(h * LANES, LANES)], wrecv.at[h, src])
        landed(xin.at[src], tp_recv.at[4, src])
        return total + dot(xin[src], wgu[src])

    both = lax.fori_loop(1, n_tp, gather_x, dot(xbuf[tp // quarters], wgu[tp]))
    hidden = gated(both[:, :LANES], both[:, LANES:])
    hs[...] = hidden
    hin[tp] = hidden

    @pl.loop(1, n_tp)
    def _(k):
        tp_copy(5, after_tp(k), hs, hin.at[tp]).start()

    tp_drain(5, lambda g: hs, hin.at[tp])

    @pl.loop(0, strips)
    def _(src):
        @pl.when(src != tp)
        def _():
            landed(shh.at[src], tp_recv.at[3, src])

    shared_out = dot(shh[...].reshape(rows, units), sd[...])

    @pl.loop(1, n_tp)
    def _(k):
        src = before_tp(k)
        landed(hin.at[src], tp_recv.at[5, src])

    for e in range(local):
        h = jnp.concatenate([hin[quarters * e + q] for q in range(quarters)], axis=1)
        obuf[e * used : (e + 1) * used, :] = dot(h, ed[e]).astype(BF)
    ret_out[...] = dot(rmat[...], obuf[...]).reshape(n_sp, PADDED, LANES).astype(BF)

    @pl.loop(1, n_sp)
    def _(k):
        d = (sp + k) % n_sp
        sp_copy(1, d, ret_out.at[d], ret_in.at[sp]).start()

    sp_drain(1, ret_out, ret_in.at[sp])
    ret_in[sp] = ret_out[sp]
    weights = [column(gates, k) for k in range(2)]

    @pl.loop(1, n_sp)
    def _(k):
        src = (sp + n_sp - k) % n_sp
        landed(ret_in.at[src], sp_recv.at[1, src])

    flat = ret_in[...].astype(F32).reshape(seats, LANES).astype(BF)
    routed = weights[0] * dot(oh[0], flat) + weights[1] * dot(oh[1], flat)
    out[...] = (stream + (routed + shared_out)).astype(BF)
    for drain in drains:
        drain()


def shards(query_a, key_a, value_a, query_b, key_b, value_b, stop_a, stop_b, out_a, out_b, resid, mix_gain, ffn_gain,
           routes, gates, exp_gate, exp_up, exp_down, sh_gate, sh_up, sh_down):
    n_sp, n_tp = lax.axis_size("sp"), lax.axis_size("tp")
    rows = resid.shape[0]
    local, _, units = exp_gate.shape
    used = n_sp * CAP
    strips = rows // 16
    seats = n_sp * PADDED
    nz = n_sp // 2
    up_steps = nz // 2
    down_steps = nz - 1 - up_steps
    operands = (
        query_a, key_a, value_a, query_b, key_b, value_b, stop_a.T, stop_b.T, out_a, out_b, resid,
        mix_gain.reshape(1, -1), ffn_gain.reshape(1, -1), routes.T, gates.T, exp_gate, exp_up, exp_down, sh_gate,
        sh_up, sh_down)
    dma = pltpu.SemaphoreType.DMA
    vmem = pltpu.VMEM
    held = [vmem(a.shape, a.dtype) for i, a in enumerate(operands) if i not in (15, 16)]
    return pl.pallas_call(
        functools.partial(layer_kernel, n_sp, n_tp),
        out_shape=jax.ShapeDtypeStruct((rows, LANES), BF),
        in_specs=[pl.BlockSpec(memory_space=pl.ANY)] * len(operands),
        out_specs=pl.BlockSpec(memory_space=pltpu.VMEM),
        scratch_shapes=held + [
            vmem((nz, 4, 2 * rows, LANES), BF),
            vmem((rows, 2 * LANES), F32),
            vmem((rows, 2 * LANES), F32),
            vmem((rows, 2 * LANES), F32),
            vmem((2 * rows, 2 * rows), BF),
            vmem((n_tp, rows, LANES), BF),
            vmem((n_tp, rows, LANES), BF),
            vmem((8, 2 * LANES), F32),
            vmem((n_tp, 8, 2 * LANES), F32),
            vmem((n_sp, PADDED, LANES), BF),
            vmem((n_sp, PADDED, LANES), BF),
            vmem((n_sp, PADDED, LANES), BF),
            vmem((n_sp, PADDED, LANES), BF),
            vmem((strips, 16, 2 * units), BF),
            vmem((n_tp, 16, 2 * units), BF),
            vmem((16, units), BF),
            vmem((strips, 16, units), BF),
            vmem((local, used, LANES), BF),
            vmem((n_tp, used, LANES), BF),
            vmem((n_tp, LANES, 2 * LANES), BF),
            vmem((used, LANES), BF),
            vmem((n_tp, used, LANES), BF),
            vmem((local * used, LANES), BF),
            vmem((2, rows, seats), BF),
            vmem((seats, 2 * LANES), BF),
            vmem((local * used, seats), BF),
            vmem((seats, local * used), BF),
            dma((len(held),)),
            dma((up_steps, 4)),
            dma((up_steps, 4)),
            dma((down_steps, 4)),
            dma((down_steps, 4)),
            dma((nz, 4)),
            dma((nz, 4)),
            dma((2, n_tp)),
            dma((2, n_tp)),
            dma((2,)),
            dma((6, n_tp)),
            dma((6, n_tp)),
            dma((2, n_sp)),
            dma((2, n_sp)),
        ],
        compiler_params=pltpu.CompilerParams(
            collective_id=0, has_side_effects=True, vmem_limit_bytes=56 * 1024 * 1024),
    )(*operands)


def solution(mesh):
    row, col, both = P("tp", None), P("tp"), P("sp", "tp")
    in_specs = (both,) * 8 + (
        row, row, both, col, col, P("sp", None), P("sp", None),
        P("sp", "tp", None), P("sp", "tp", None), P("sp", None, "tp"), row, row, P(None, "tp"))
    return jax.shard_map(shards, mesh=mesh, in_specs=in_specs, out_specs=both, check_vma=False)
```

```python
import functools

import jax
import jax.numpy as jnp
from jax import lax
from jax.experimental import pallas as pl
from jax.experimental.pallas import tpu as pltpu
from jax.sharding import PartitionSpec as P

D = 2048
EPS = 1e-06
MESH = pl.DeviceIdType.MESH
BF = jnp.bfloat16
F32 = jnp.float32
LANES = 128
CAP = 5
PADDED = 24


def dot(a, b):
    return jnp.dot(a, b, preferred_element_type=F32)


def softplus_block(query, keys, stop, scale, later, valid):
    scores = lax.dot_general(query, keys, (((1,), (1,)), ((), ())), preferred_element_type=F32)
    z = scores * scale + stop
    sp = jnp.maximum(z, 0.0) + jnp.log(1.0 + jnp.exp(-jnp.abs(z)))
    if valid is not None:
        sp = jnp.where(valid, sp, 0.0)
    after = dot(sp.astype(BF), later)
    weight = jnp.exp(z - sp - after)
    if valid is not None:
        weight = jnp.where(valid, weight, 0.0)
    return weight.astype(BF), jnp.sum(sp, axis=1, keepdims=True)


def layer_kernel(n_sp, n_tp, *refs):
    (qa_h, ka_h, va_h, qb_h, kb_h, vb_h, sa_h, sb_h, oa_h, ob_h, resid_h, mg_h, fg_h, routes_h, gates_h,
     eg, eu, ed_h, sg_h, su_h, sd_h, out,
     qa, ka, va, qb, kb, vb, sa, sb, oa, ob, resid, mg, fg, routes, gates, ed, sg, su, sd,
     buf, accn, accf, ln, later,
     part, rs, sts, st, dsp_out, dsp_in, ret_out, ret_in, shp, shr, shs, shh, xbuf, xin, wgu, hs, hin, obuf, oh,
     choose, smat, rmat,
     lsem, tokens, ssu, rsu, ssd, rsd, ssp, rsp, wsend, wrecv, wloc, tp_send, tp_recv, sp_send, sp_recv) = refs
    rows = resid.shape[0]
    local, units = ed.shape[0], ed.shape[1]
    quarters = n_tp // local
    used = n_sp * CAP
    seats = n_sp * PADDED
    parts = 2
    part_used = used // parts
    part_seats = seats // parts
    homes = n_sp // parts
    strips = rows // 16
    wide = 2 * LANES
    nz = n_sp // 2
    up_steps = nz // 2
    down_steps = nz - 1 - up_steps
    last_far = nz - 2 - up_steps
    sp = lax.axis_index("sp")
    tp = lax.axis_index("tp")
    z = sp // 2
    c = sp % 2
    up_id = (2 * ((z + 1) % nz) + c, tp)
    down_id = (2 * ((z + nz - 1) % nz) + c, tp)
    pair_id = (2 * z + 1 - c, tp)
    drains = []

    barrier = pltpu.get_barrier_semaphore()

    side = quarters
    row = [(sp, tp // side * side + (tp + k) % side) for k in range(1, side)]
    column_peers = [(sp, (tp + side * k) % n_tp) for k in range(1, n_tp // side)]
    across = [(2 * ((z + step) % nz) + 1 - c, tp) for step in (1, nz - 1)]
    first = [up_id, down_id, pair_id] + across + row + column_peers
    for peer in first:
        pl.semaphore_signal(barrier, inc=1, device_id=peer, device_id_type=MESH)

    def pass_on(which, peers):
        for peer in peers:
            pl.semaphore_signal(tokens.at[which], inc=1, device_id=peer, device_id_type=MESH)

    def along(distance):
        return [(2 * ((z + step) % nz) + c, tp) for step in (distance, nz - distance)]

    rounds = [1 << r for r in range((nz // 4).bit_length())]

    staged = [
        (ka_h, ka), (va_h, va), (kb_h, kb), (vb_h, vb), (routes_h, routes), (qa_h, qa), (qb_h, qb), (sa_h, sa),
        (sb_h, sb), (oa_h, oa), (ob_h, ob), (resid_h, resid), (mg_h, mg), (fg_h, fg), (gates_h, gates),
        (ed_h, ed), (sg_h, sg), (su_h, su), (sd_h, sd)]
    loads = [pltpu.make_async_copy(a, b, lsem.at[i]) for i, (a, b) in enumerate(staged)]
    for load in loads:
        load.start()

    def column(ref, k):
        return jnp.transpose(jnp.broadcast_to(ref[k : k + 1, :].astype(F32), (LANES, rows)))

    for load in loads[:4]:
        load.wait()
    pl.semaphore_wait(barrier, len(first))
    pass_on(0, row)
    pass_on(1, along(rounds[0]))

    mine = pl.ds(pl.multiple_of(c * rows, rows), rows)
    theirs = pl.ds(pl.multiple_of((1 - c) * rows, rows), rows)
    srcs = (ka, va, kb, vb)

    def place(block, a):
        return buf.at[block, a, mine, :]

    def other(block, a):
        return buf.at[block, a, theirs, :]

    def up_copy(step, a, src):
        return pltpu.make_async_remote_copy(
            src_ref=src, dst_ref=place(z + 1 - step, a), send_sem=ssu.at[step - 1, a], recv_sem=rsu.at[step - 1, a],
            device_id=up_id, device_id_type=MESH)

    def down_copy(step, a, src):
        return pltpu.make_async_remote_copy(
            src_ref=src, dst_ref=place((z + step - 1) % nz, a), send_sem=ssd.at[step - 1, a],
            recv_sem=rsd.at[step - 1, a], device_id=down_id, device_id_type=MESH)

    def pair_copy(index, block, a, src):
        return pltpu.make_async_remote_copy(
            src_ref=src, dst_ref=place(block, a), send_sem=ssp.at[index, a], recv_sem=rsp.at[index, a],
            device_id=pair_id, device_id_type=MESH)

    def landed(ref, sem):
        pltpu.make_async_copy(ref, ref, sem).wait()

    def sends_up(step):
        return (z < nz - 1) & (z + 1 - step >= 0)

    def sends_down(step):
        return (z + step - 1) % nz <= last_far

    def gets_up(step):
        return z - step >= 0

    def gets_down(step):
        return (z + step) % nz <= last_far

    def far(step):
        return z + step >= nz

    for a in range(4):
        @pl.when(sends_up(1))
        def _(a=a):
            up_copy(1, a, srcs[a]).start()

        @pl.when(sends_down(1))
        def _(a=a):
            down_copy(1, a, srcs[a]).start()

        pair_copy(0, z, a, srcs[a]).start()
        buf[z, a, mine, :] = srcs[a][...]

    span = 2 * rows
    j = lax.broadcasted_iota(jnp.int32, (span, span), 0)
    s = lax.broadcasted_iota(jnp.int32, (span, span), 1)
    later[...] = (j > s).astype(BF)
    accf[...] = jnp.zeros_like(accf)
    half = lax.broadcasted_iota(jnp.int32, (rows, LANES), 1) < LANES // 2

    def index_of(shape, dim):
        return lax.broadcasted_iota(jnp.int32, shape, dim).astype(F32)

    i = index_of((local * part_used, LANES), 0)
    e = jnp.floor((i + 0.5) * (1.0 / part_used))
    i = i - part_used * e
    g = jnp.floor((i + 0.5) * (1.0 / CAP))
    seat = g * PADDED + e * CAP + (i - CAP * g)
    smat[...] = (index_of((local * part_used, part_seats), 1) == seat[:, 0:1]).astype(BF)
    i = index_of((part_seats, LANES), 0)
    g = jnp.floor((i + 0.5) * (1.0 / PADDED))
    i = i - PADDED * g
    e = jnp.floor((i + 0.5) * (1.0 / CAP))
    seat = jnp.where(e < local, e * part_used + g * CAP + (i - CAP * e), -1.0)
    rmat[...] = (index_of((part_seats, local * part_used), 1) == seat[:, 0:1]).astype(BF)
    loads[4].wait()
    experts = local * n_sp
    e_at = index_of((rows, experts), 1)
    named_by = [column(routes, k) for k in range(2)]
    named = [e_at == named_by[k][:, 0:1] for k in range(2)]
    members = jnp.where(named[0] | named[1], 1.0, 0.0).astype(BF)
    prior = dot((index_of((rows, rows), 1) < index_of((rows, rows), 0)).astype(BF), members)
    hits = None
    for k in range(2):
        home = jnp.floor((named_by[k] + 0.5) * (1.0 / local))
        rank = jnp.sum(jnp.where(named[k], prior, 0.0), axis=1, keepdims=True)
        seat = home * PADDED + (named_by[k] - local * home) * CAP + rank
        oh[k] = (index_of((rows, seats), 1) == seat[:, 0:1]).astype(BF)
        tall = jnp.concatenate([seat, jnp.full((wide - rows, LANES), -1.0, F32)], axis=0)
        hit = index_of((seats, wide), 0) == jnp.transpose(tall)[0:1, :]
        hits = hit if hits is None else hits | hit
    choose[...] = hits.astype(BF)


    def after_tp(k):
        return (tp + k) % n_tp

    def before_tp(k):
        return (tp + n_tp - k) % n_tp

    def weights_copy(h, g):
        src = (eg, eu)[h].at[g // quarters, :, pl.ds(pl.multiple_of((g % quarters) * LANES, LANES), LANES)]
        dst = wgu.at[tp, :, pl.ds(h * LANES, LANES)]
        return src, dst

    def weights_remote(h, g):
        src, dst = weights_copy(h, g)
        return pltpu.make_async_remote_copy(
            src_ref=src, dst_ref=dst, send_sem=wsend.at[h, g], recv_sem=wrecv.at[h, tp],
            device_id=(sp, g), device_id_type=MESH)

    pl.semaphore_wait(tokens.at[0], len(row))

    @pl.loop(1, n_tp)
    def _(k):
        for h in range(2):
            weights_remote(h, after_tp(k)).start()

    for h in range(2):
        src, dst = weights_copy(h, tp)
        pltpu.make_async_copy(src, dst, wloc.at[h]).start()

    for load in loads[5:]:
        load.wait()
    pl.semaphore_wait(tokens.at[1], 2)
    pass_on(2, along(rounds[1]))
    qa_all = qa[...]
    zero = jnp.zeros_like(qa_all)
    qa_heads = (jnp.where(half, qa_all, zero), jnp.where(half, zero, qa_all))
    stops = [column(sa, 0)[:, 0:1], column(sa, 1)[:, 0:1], column(sb, 0)[:, 0:1]]

    def group_a(block, valid=None):
        keys = buf[block, 0]
        values = buf[block, 1]
        pieces = [softplus_block(qa_heads[h], keys, stops[h], 64 ** -0.5, later[...], valid) for h in range(2)]
        added = jnp.where(half, dot(pieces[0][0], values), dot(pieces[1][0], values))
        return added, jnp.where(half, pieces[0][1], pieces[1][1])

    def group_b(block, valid=None):
        weight, total = softplus_block(qb[...], buf[block, 2], stops[2], 128 ** -0.5, later[...], valid)
        return dot(weight, buf[block, 3]), jnp.broadcast_to(total, (rows, LANES))

    groups = (group_a, group_b)

    def cols(g):
        return slice(g * LANES, (g + 1) * LANES)

    def near(g, step):
        block = z - step
        for a in (2 * g, 2 * g + 1):
            landed(other(block, a), rsp.at[step, a])
        added, total = groups[g](block)
        accn[:, cols(g)] += jnp.exp(-ln[:, cols(g)]) * added
        ln[:, cols(g)] += total

    def distant(g, step):
        block = z + step - nz
        for a in (2 * g, 2 * g + 1):
            landed(other(block, a), rsp.at[up_steps + step, a])
        added, total = groups[g](block)
        accf[:, cols(g)] = jnp.exp(-total) * accf[:, cols(g)] + added

    def poll_up(step, a):
        @pl.when(gets_up(step))
        def _():
            ref = place(z - step, a)
            landed(ref, rsu.at[step - 1, a])

            @pl.when((step < up_steps) & (z < nz - 1))
            def _():
                up_copy(step + 1, a, ref).start()

            pair_copy(step, z - step, a, ref).start()

    def poll_down(step, a):
        @pl.when((step <= down_steps) & gets_down(step))
        def _():
            block = (z + step) % nz
            ref = place(block, a)
            landed(ref, rsd.at[step - 1, a])

            @pl.when(step < down_steps)
            def _():
                down_copy(step + 1, a, ref).start()

            @pl.when(far(step))
            def _():
                pair_copy(up_steps + step, block, a, ref).start()

    row_at = lax.broadcasted_iota(jnp.int32, (rows, span), 0) + c * rows
    key_at = lax.broadcasted_iota(jnp.int32, (rows, span), 1)
    valid = key_at < row_at
    for g in range(2):
        for a in (2 * g, 2 * g + 1):
            landed(other(z, a), rsp.at[0, a])
        added, total = groups[g](z, valid)
        accn[:, cols(g)] = added
        ln[:, cols(g)] = total
        for a in (2 * g, 2 * g + 1):
            poll_up(1, a)
            poll_down(1, a)

    for r in range(2, len(rounds)):
        pl.semaphore_wait(tokens.at[r], 2)
        pass_on(r + 1, along(rounds[r]))

    @pl.loop(2, up_steps + 1)
    def _(step):
        before = step - 1
        for a in range(4):
            poll_up(step, a)
            poll_down(step, a)
            g = a // 2
            if a % 2 == 0:
                @pl.when(gets_up(before))
                def _():
                    near(g, before)
            else:
                @pl.when(far(before))
                def _():
                    distant(g, before)

    @pl.when(gets_up(up_steps))
    def _():
        for g in range(2):
            near(g, up_steps)

    pl.semaphore_wait(tokens.at[len(rounds)], 2)
    att = (accn[...] + jnp.exp(-ln[...]) * accf[...]).astype(BF)

    @drains.append
    def _():
        for a in range(4):
            pair_copy(0, z, a, srcs[a]).wait_send()

        @pl.loop(1, up_steps + 1)
        def _(step):
            for a in range(4):
                @pl.when(sends_up(step))
                def _():
                    up_copy(step, a, place(z + 1 - step, a)).wait_send()

                @pl.when(gets_up(step))
                def _():
                    pair_copy(step, z - step, a, place(z - step, a)).wait_send()

        @pl.loop(1, down_steps + 1)
        def _(step):
            for a in range(4):
                @pl.when(sends_down(step))
                def _():
                    down_copy(step, a, place((z + step - 1) % nz, a)).wait_send()

                @pl.when(far(step))
                def _():
                    pair_copy(up_steps + step, z + step - nz, a, place(z + step - nz, a)).wait_send()

        @pl.loop(1, n_tp)
        def _(k):
            for h in range(2):
                weights_remote(h, after_tp(k)).wait_send()

    def tp_copy(phase, g, src, dst):
        return pltpu.make_async_remote_copy(
            src_ref=src, dst_ref=dst, send_sem=tp_send.at[phase, g], recv_sem=tp_recv.at[phase, tp],
            device_id=(sp, g), device_id_type=MESH)

    def sp_copy(phase, d, src, dst):
        return pltpu.make_async_remote_copy(
            src_ref=src, dst_ref=dst, send_sem=sp_send.at[phase, d], recv_sem=sp_recv.at[phase, sp],
            device_id=(d, tp), device_id_type=MESH)

    def tp_drain(phase, src, dst):
        @drains.append
        def _():
            @pl.loop(1, n_tp)
            def _(k):
                g = after_tp(k)
                tp_copy(phase, g, src(g), dst).wait_send()

    low, high = att[:, :LANES], att[:, LANES:]

    @pl.loop(1, n_tp + 1)
    def _(k):
        g = after_tp(k)
        strip = pl.ds(pl.multiple_of(g * LANES, LANES), LANES)
        part[g] = (dot(low, oa[:, strip]) + dot(high, ob[:, strip])).astype(BF)

        @pl.when(k < n_tp)
        def _():
            tp_copy(0, g, part.at[g], rs.at[tp]).start()

    tp_drain(0, lambda g: part.at[g], rs.at[tp])

    def gather_rs(k, total):
        src = before_tp(k)
        landed(rs.at[src], tp_recv.at[0, src])
        return total + rs[src].astype(F32)

    mixed = lax.fori_loop(1, n_tp, gather_rs, part[tp].astype(F32))

    gained = mixed * mg[...]
    x = resid[...].astype(F32)
    lane = lax.broadcasted_iota(jnp.int32, (rows, LANES), 1)
    own = jnp.zeros((rows, LANES), F32)
    for k, product in enumerate((mixed * mixed, x * x, x * gained, gained * gained)):
        own = jnp.where(lane == k, jnp.sum(product, axis=1, keepdims=True), own)
    lines = jnp.transpose(jnp.concatenate([own, jnp.zeros((wide - rows, LANES), F32)], axis=0))[0:8, :]
    sts[...] = lines

    @pl.loop(1, n_tp)
    def _(k):
        tp_copy(1, after_tp(k), sts, st.at[tp]).start()

    tp_drain(1, lambda g: sts, st.at[tp])

    def gather_st(k, total):
        src = before_tp(k)
        landed(st.at[src], tp_recv.at[1, src])
        return total + st[src]

    lines = lax.fori_loop(1, n_tp, gather_st, lines)
    total = jnp.transpose(jnp.concatenate([lines, jnp.zeros((LANES - 8, wide), F32)], axis=0))[:rows, :]
    scale = lax.rsqrt(total[:, 0:1] / D + EPS)
    square = total[:, 1:2] + scale * (2.0 * total[:, 2:3] + scale * total[:, 3:4])
    stream = (x + gained * scale).astype(BF).astype(F32)
    scale = lax.rsqrt(jnp.maximum(square, 0.0) / D + EPS)
    normed = (stream * scale * fg[...]).astype(BF)

    tall = jnp.concatenate([normed, jnp.zeros((wide - rows, LANES), BF)], axis=0)
    dsp_out[...] = dot(choose[...], tall).reshape(n_sp, PADDED, LANES).astype(BF)

    def near_first(body):
        @pl.loop(0, nz)
        def _(k):
            reach = (k + 1) // 2
            away = (z + nz + reach * (2 * (k % 2) - 1)) % nz
            body(2 * away + 1 - c)

            @pl.when(k > 0)
            def _():
                body(2 * away + c)

    def berth(src, dst):
        return 2 * ((src // 2 + nz + nz // 4 - dst // 2) % nz) + src % 2

    def tenant(place):
        return 2 * ((z + nz - nz // 4 + place // 2) % nz) + place % 2

    def dispatch(d):
        return sp_copy(0, d, dsp_out.at[d], dsp_in.at[berth(sp, d)])

    near_first(lambda d: dispatch(d).start())
    drains.append(lambda: near_first(lambda d: dispatch(d).wait_send()))
    dsp_in[berth(sp, sp)] = dsp_out[sp]

    shp[:, :, :units] = dot(normed, sg[...]).reshape(strips, 16, units).astype(BF)
    shp[:, :, units:] = dot(normed, su[...]).reshape(strips, 16, units).astype(BF)

    @pl.loop(1, n_tp)
    def _(k):
        g = after_tp(k)

        @pl.when(g < strips)
        def _():
            tp_copy(2, g, shp.at[g], shr.at[tp]).start()

    @drains.append
    def _():
        @pl.loop(1, n_tp)
        def _(k):
            g = after_tp(k)

            @pl.when(g < strips)
            def _():
                tp_copy(2, g, shp.at[g], shr.at[tp]).wait_send()

            @pl.when(tp < strips)
            def _():
                tp_copy(3, g, shs, shh.at[tp]).wait_send()

    def gated(gate, up):
        return (gate / (1.0 + jnp.exp(-gate)) * up).astype(BF)

    def reduce_shared():
        @pl.when(tp < strips)
        def _():
            def gather(k, total):
                src = before_tp(k)
                landed(shr.at[src], tp_recv.at[2, src])
                return total + shr[src].astype(F32)

            both = lax.fori_loop(1, n_tp, gather, shp[tp].astype(F32))
            hidden = gated(both[:, :units], both[:, units:])
            shs[...] = hidden
            shh[tp] = hidden

            @pl.loop(1, n_tp)
            def _(k):
                tp_copy(3, after_tp(k), shs, shh.at[tp]).start()

    def send_rows(p):
        @pl.loop(p * homes, (p + 1) * homes)
        def _(place):
            src = tenant(place)

            @pl.when(src != sp)
            def _():
                landed(dsp_in.at[place], sp_recv.at[0, src])

        flat = dsp_in[p * homes : (p + 1) * homes].astype(F32).reshape(part_seats, LANES).astype(BF)
        xbuf[p] = dot(smat[...], flat).reshape(local, part_used, LANES).astype(BF)
        xin[p, tp] = xbuf[p, tp // quarters]

        @pl.loop(1, n_tp)
        def _(k):
            g = after_tp(k)
            tp_copy(4 + p, g, xbuf.at[p, g // quarters], xin.at[p, tp]).start()

        tp_drain(4 + p, lambda g: xbuf.at[p, g // quarters], xin.at[p, tp])

    def send_hidden(p):
        @pl.loop(1, n_tp)
        def _(k):
            src = before_tp(k)
            landed(xin.at[p, src], tp_recv.at[4 + p, src])

        x = jnp.concatenate([xin[p, g] for g in range(n_tp)], axis=1)
        both = dot(x, wgu[...].reshape(n_tp * LANES, 2 * LANES))
        hidden = gated(both[:, :LANES], both[:, LANES:])
        hs[p] = hidden
        hin[p, tp] = hidden

        @pl.loop(1, n_tp)
        def _(k):
            tp_copy(4 + parts + p, after_tp(k), hs.at[p], hin.at[p, tp]).start()

        tp_drain(4 + parts + p, lambda g: hs.at[p], hin.at[p, tp])

    def giving(place):
        d = tenant(place)
        return sp_copy(1, d, ret_out.at[place], ret_in.at[sp])

    def send_back(p):
        @pl.loop(1, n_tp)
        def _(k):
            src = before_tp(k)
            landed(hin.at[p, src], tp_recv.at[4 + parts + p, src])

        for e in range(local):
            h = jnp.concatenate([hin[p, quarters * e + q] for q in range(quarters)], axis=1)
            obuf[e * part_used : (e + 1) * part_used, :] = dot(h, ed[e]).astype(BF)
        made = dot(rmat[...], obuf[...]).reshape(homes, PADDED, LANES).astype(BF)
        ret_out[p * homes : (p + 1) * homes] = made

        @pl.loop(p * homes, (p + 1) * homes)
        def _(place):
            @pl.when(tenant(place) != sp)
            def _():
                giving(place).start()

    @drains.append
    def _():
        @pl.loop(0, n_sp)
        def _(place):
            @pl.when(tenant(place) != sp)
            def _():
                giving(place).wait_send()

    send_rows(0)
    reduce_shared()
    for h in range(2):
        src, dst = weights_copy(h, tp)
        pltpu.make_async_copy(src, dst, wloc.at[h]).wait()

    @pl.loop(1, n_tp)
    def _(k):
        src = before_tp(k)
        for h in range(2):
            landed(wgu.at[src, :, pl.ds(h * LANES, LANES)], wrecv.at[h, src])

    for p in range(1, parts):
        send_rows(p)
        send_hidden(p - 1)
    send_hidden(parts - 1)
    for p in range(parts):
        send_back(p)
    ret_in[sp] = ret_out[berth(sp, sp)]
    weights = [column(gates, k) for k in range(2)]

    @pl.loop(0, strips)
    def _(src):
        @pl.when(src != tp)
        def _():
            landed(shh.at[src], tp_recv.at[3, src])

    shared_out = dot(shh[...].reshape(rows, units), sd[...])

    @pl.loop(1, n_sp)
    def _(k):
        src = (sp + n_sp - k) % n_sp
        landed(ret_in.at[src], sp_recv.at[1, src])

    flat = ret_in[...].astype(F32).reshape(seats, LANES).astype(BF)
    routed = weights[0] * dot(oh[0], flat) + weights[1] * dot(oh[1], flat)
    out[...] = (stream + (routed + shared_out)).astype(BF)
    for drain in drains:
        drain()


def shards(query_a, key_a, value_a, query_b, key_b, value_b, stop_a, stop_b, out_a, out_b, resid, mix_gain, ffn_gain,
           routes, gates, exp_gate, exp_up, exp_down, sh_gate, sh_up, sh_down):
    n_sp, n_tp = lax.axis_size("sp"), lax.axis_size("tp")
    rows = resid.shape[0]
    local, _, units = exp_gate.shape
    used = n_sp * CAP
    strips = rows // 16
    seats = n_sp * PADDED
    parts = 2
    nz = n_sp // 2
    up_steps = nz // 2
    down_steps = nz - 1 - up_steps
    operands = (
        query_a, key_a, value_a, query_b, key_b, value_b, stop_a.T, stop_b.T, out_a, out_b, resid,
        mix_gain.reshape(1, -1), ffn_gain.reshape(1, -1), routes.T, gates.T, exp_gate, exp_up, exp_down, sh_gate,
        sh_up, sh_down)
    dma = pltpu.SemaphoreType.DMA
    vmem = pltpu.VMEM
    held = [vmem(a.shape, a.dtype) for i, a in enumerate(operands) if i not in (15, 16)]
    return pl.pallas_call(
        functools.partial(layer_kernel, n_sp, n_tp),
        out_shape=jax.ShapeDtypeStruct((rows, LANES), BF),
        in_specs=[pl.BlockSpec(memory_space=pl.ANY)] * len(operands),
        out_specs=pl.BlockSpec(memory_space=pltpu.VMEM),
        scratch_shapes=held + [
            vmem((nz, 4, 2 * rows, LANES), BF),
            vmem((rows, 2 * LANES), F32),
            vmem((rows, 2 * LANES), F32),
            vmem((rows, 2 * LANES), F32),
            vmem((2 * rows, 2 * rows), BF),
            vmem((n_tp, rows, LANES), BF),
            vmem((n_tp, rows, LANES), BF),
            vmem((8, 2 * LANES), F32),
            vmem((n_tp, 8, 2 * LANES), F32),
            vmem((n_sp, PADDED, LANES), BF),
            vmem((n_sp, PADDED, LANES), BF),
            vmem((n_sp, PADDED, LANES), BF),
            vmem((n_sp, PADDED, LANES), BF),
            vmem((strips, 16, 2 * units), BF),
            vmem((n_tp, 16, 2 * units), BF),
            vmem((16, units), BF),
            vmem((strips, 16, units), BF),
            vmem((parts, local, used // parts, LANES), BF),
            vmem((parts, n_tp, used // parts, LANES), BF),
            vmem((n_tp, LANES, 2 * LANES), BF),
            vmem((parts, used // parts, LANES), BF),
            vmem((parts, n_tp, used // parts, LANES), BF),
            vmem((local * used // parts, LANES), BF),
            vmem((2, rows, seats), BF),
            vmem((seats, 2 * LANES), BF),
            vmem((local * used // parts, seats // parts), BF),
            vmem((seats // parts, local * used // parts), BF),
            dma((len(held),)),
            pltpu.SemaphoreType.REGULAR(((nz // 4).bit_length() + 1,)),
            dma((up_steps, 4)),
            dma((up_steps, 4)),
            dma((down_steps, 4)),
            dma((down_steps, 4)),
            dma((nz, 4)),
            dma((nz, 4)),
            dma((2, n_tp)),
            dma((2, n_tp)),
            dma((2,)),
            dma((4 + 2 * parts, n_tp)),
            dma((4 + 2 * parts, n_tp)),
            dma((2, n_sp)),
            dma((2, n_sp)),
        ],
        compiler_params=pltpu.CompilerParams(
            collective_id=0, has_side_effects=True, vmem_limit_bytes=56 * 1024 * 1024),
    )(*operands)


def solution(mesh):
    row, col, both = P("tp", None), P("tp"), P("sp", "tp")
    in_specs = (both,) * 8 + (
        row, row, both, col, col, P("sp", None), P("sp", None),
        P("sp", "tp", None), P("sp", "tp", None), P("sp", None, "tp"), row, row, P(None, "tp"))
    return jax.shard_map(shards, mesh=mesh, in_specs=in_specs, out_specs=both, check_vma=False)
```

```python
import functools

import jax
import jax.numpy as jnp
from jax import lax
from jax.experimental import pallas as pl
from jax.experimental.pallas import tpu as pltpu
from jax.sharding import PartitionSpec as P

D = 2048
EPS = 1e-06
MESH = pl.DeviceIdType.MESH
BF = jnp.bfloat16
F32 = jnp.float32
LANES = 128
CAP = 5
PADDED = 24


def dot(a, b):
    return jnp.dot(a, b, preferred_element_type=F32)


def softplus_block(query, keys, stop, scale, later, valid):
    scores = lax.dot_general(query, keys, (((1,), (1,)), ((), ())), preferred_element_type=F32)
    z = scores * scale + stop
    sp = jnp.maximum(z, 0.0) + jnp.log(1.0 + jnp.exp(-jnp.abs(z)))
    if valid is not None:
        sp = jnp.where(valid, sp, 0.0)
    after = dot(sp.astype(BF), later)
    weight = jnp.exp(z - sp - after)
    if valid is not None:
        weight = jnp.where(valid, weight, 0.0)
    return weight.astype(BF), jnp.sum(sp, axis=1, keepdims=True)


def layer_kernel(n_sp, n_tp, *refs):
    (qa_h, ka_h, va_h, qb_h, kb_h, vb_h, sa_h, sb_h, oa_h, ob_h, resid_h, mg_h, fg_h, routes_h, gates_h,
     eg, eu, ed_h, sg_h, su_h, sd_h, out,
     qa, ka, va, qb, kb, vb, sa, sb, oab, resid, mg, fg, routes, gates, ed, sg, su, sd,
     buf, accn, accf, ln, later,
     part, rs, sts, st, dsp_out, dsp_in, ret_out, ret_in, shp, shr, shs, shh, xbuf, xin, wgu, hs, hin, obuf, oh,
     choose, smat, rmat,
     lsem, tokens, ssu, rsu, ssd, rsd, ssp, rsp, wsend, wrecv, wloc, tp_send, tp_recv, sp_send, sp_recv) = refs
    rows = resid.shape[0]
    local, units = ed.shape[0], ed.shape[1]
    quarters = n_tp // local
    used = n_sp * CAP
    seats = n_sp * PADDED
    parts = 2
    part_used = used // parts
    part_seats = seats // parts
    homes = n_sp // parts
    strips = rows // 16
    wide = 2 * LANES
    nz = n_sp // 2
    up_steps = nz // 2
    down_steps = nz - up_steps
    ups = (up_steps, up_steps, nz - 1 - down_steps, nz - 1 - down_steps)
    downs = tuple(nz - 1 - n for n in ups)
    sp = lax.axis_index("sp")
    tp = lax.axis_index("tp")
    z = sp // 2
    c = sp % 2
    up_id = (2 * ((z + 1) % nz) + c, tp)
    down_id = (2 * ((z + nz - 1) % nz) + c, tp)
    pair_id = (2 * z + 1 - c, tp)
    drains = []

    barrier = pltpu.get_barrier_semaphore()

    side = quarters
    row = [(sp, tp // side * side + (tp + k) % side) for k in range(1, side)]
    column_peers = [(sp, (tp + side * k) % n_tp) for k in range(1, n_tp // side)]
    across = [(2 * ((z + step) % nz) + 1 - c, tp) for step in (1, nz - 1)]
    first = [up_id, down_id, pair_id] + across + row + column_peers
    for peer in first:
        pl.semaphore_signal(barrier, inc=1, device_id=peer, device_id_type=MESH)

    def pass_on(which, peers):
        for peer in peers:
            pl.semaphore_signal(tokens.at[which], inc=1, device_id=peer, device_id_type=MESH)

    def along(distance):
        return [(2 * ((z + step) % nz) + c, tp) for step in (distance, nz - distance)]

    rounds = [1 << r for r in range((nz // 4).bit_length())]

    staged = [
        (ka_h, ka), (va_h, va), (kb_h, kb), (vb_h, vb), (routes_h, routes), (qa_h, qa), (qb_h, qb), (sa_h, sa),
        (sb_h, sb), (oa_h, oab.at[:LANES]), (ob_h, oab.at[LANES:]), (resid_h, resid), (mg_h, mg), (fg_h, fg), (gates_h, gates),
        (ed_h, ed), (sg_h, sg), (su_h, su), (sd_h, sd)]
    loads = [pltpu.make_async_copy(a, b, lsem.at[i]) for i, (a, b) in enumerate(staged)]
    for load in loads:
        load.start()

    def column(ref, k):
        return jnp.transpose(jnp.broadcast_to(ref[k : k + 1, :].astype(F32), (LANES, rows)))

    for load in loads[:4]:
        load.wait()
    pl.semaphore_wait(barrier, len(first))
    pass_on(0, row)
    pass_on(1, along(rounds[0]))

    mine = pl.ds(pl.multiple_of(c * rows, rows), rows)
    theirs = pl.ds(pl.multiple_of((1 - c) * rows, rows), rows)
    srcs = (ka, va, kb, vb)

    def place(block, a):
        return buf.at[block, a, mine, :]

    def other(block, a):
        return buf.at[block, a, theirs, :]

    def up_copy(step, a, src):
        return pltpu.make_async_remote_copy(
            src_ref=src, dst_ref=place(z + 1 - step, a), send_sem=ssu.at[step - 1, a], recv_sem=rsu.at[step - 1, a],
            device_id=up_id, device_id_type=MESH)

    def down_copy(step, a, src):
        return pltpu.make_async_remote_copy(
            src_ref=src, dst_ref=place((z + step - 1) % nz, a), send_sem=ssd.at[step - 1, a],
            recv_sem=rsd.at[step - 1, a], device_id=down_id, device_id_type=MESH)

    def pair_copy(index, block, a, src):
        return pltpu.make_async_remote_copy(
            src_ref=src, dst_ref=place(block, a), send_sem=ssp.at[index, a], recv_sem=rsp.at[index, a],
            device_id=pair_id, device_id_type=MESH)

    def landed(ref, sem):
        pltpu.make_async_copy(ref, ref, sem).wait()

    def sends_up(step, a):
        return (z < nz - 1) & (z + 1 - step >= 0) & (step <= ups[a])

    def sends_down(step, a):
        return ((z + step - 1) % nz <= downs[a] - 1) & (step <= downs[a])

    def gets_up(step, a):
        return (z - step >= 0) & (step <= ups[a])

    def gets_down(step, a):
        return ((z + step) % nz <= downs[a] - 1) & (step <= downs[a])

    def far(step, a):
        return (z + step >= nz) & (step <= downs[a])

    for a in range(4):
        @pl.when(sends_up(1, a))
        def _(a=a):
            up_copy(1, a, srcs[a]).start()

        @pl.when(sends_down(1, a))
        def _(a=a):
            down_copy(1, a, srcs[a]).start()

        pair_copy(0, z, a, srcs[a]).start()
        buf[z, a, mine, :] = srcs[a][...]

    def after_tp(k):
        return (tp + k) % n_tp

    def before_tp(k):
        return (tp + n_tp - k) % n_tp

    def weights_copy(h, g):
        src = (eg, eu)[h].at[g // quarters, :, pl.ds(pl.multiple_of((g % quarters) * LANES, LANES), LANES)]
        dst = wgu.at[tp, :, pl.ds(h * LANES, LANES)]
        return src, dst

    def weights_remote(h, g):
        src, dst = weights_copy(h, g)
        return pltpu.make_async_remote_copy(
            src_ref=src, dst_ref=dst, send_sem=wsend.at[h, g], recv_sem=wrecv.at[h, tp],
            device_id=(sp, g), device_id_type=MESH)

    span = 2 * rows
    j = lax.broadcasted_iota(jnp.int32, (span, span), 0)
    s = lax.broadcasted_iota(jnp.int32, (span, span), 1)
    later[...] = (j > s).astype(BF)
    accf[...] = jnp.zeros_like(accf)
    half = lax.broadcasted_iota(jnp.int32, (rows, LANES), 1) < LANES // 2

    def index_of(shape, dim):
        return lax.broadcasted_iota(jnp.int32, shape, dim).astype(F32)

    def exchange_weights():
        pl.semaphore_wait(tokens.at[0], len(row))

        @pl.loop(1, n_tp)
        def _(k):
            for h in range(2):
                weights_remote(h, after_tp(k)).start()

        for h in range(2):
            src, dst = weights_copy(h, tp)
            pltpu.make_async_copy(src, dst, wloc.at[h]).start()

    def seat_masks():
        i = index_of((local * part_used, LANES), 0)
        e = jnp.floor((i + 0.5) * (1.0 / part_used))
        i = i - part_used * e
        g = jnp.floor((i + 0.5) * (1.0 / CAP))
        seat = g * PADDED + e * CAP + (i - CAP * g)
        smat[...] = (index_of((local * part_used, part_seats), 1) == seat[:, 0:1]).astype(BF)
        i = index_of((part_seats, LANES), 0)
        g = jnp.floor((i + 0.5) * (1.0 / PADDED))
        i = i - PADDED * g
        e = jnp.floor((i + 0.5) * (1.0 / CAP))
        seat = jnp.where(e < local, e * part_used + g * CAP + (i - CAP * e), -1.0)
        rmat[...] = (index_of((part_seats, local * part_used), 1) == seat[:, 0:1]).astype(BF)

    def seat_rows():
        loads[4].wait()
        experts = local * n_sp
        e_at = index_of((rows, experts), 1)
        named_by = [column(routes, k) for k in range(2)]
        named = [e_at == named_by[k][:, 0:1] for k in range(2)]
        members = jnp.where(named[0] | named[1], 1.0, 0.0).astype(BF)
        prior = dot((index_of((rows, rows), 1) < index_of((rows, rows), 0)).astype(BF), members)
        hits = None
        for k in range(2):
            home = jnp.floor((named_by[k] + 0.5) * (1.0 / local))
            rank = jnp.sum(jnp.where(named[k], prior, 0.0), axis=1, keepdims=True)
            seat = home * PADDED + (named_by[k] - local * home) * CAP + rank
            oh[k] = (index_of((rows, seats), 1) == seat[:, 0:1]).astype(BF)
            tall = jnp.concatenate([seat, jnp.full((wide - rows, LANES), -1.0, F32)], axis=0)
            hit = index_of((seats, wide), 0) == jnp.transpose(tall)[0:1, :]
            hits = hit if hits is None else hits | hit
        choose[...] = hits.astype(BF)

    for load in loads[5:9]:
        load.wait()
    pl.semaphore_wait(tokens.at[1], 2)
    pass_on(2, along(rounds[1]))
    qa_all = qa[...]
    zero = jnp.zeros_like(qa_all)
    qa_heads = (jnp.where(half, qa_all, zero), jnp.where(half, zero, qa_all))
    stops = [column(sa, 0)[:, 0:1], column(sa, 1)[:, 0:1], column(sb, 0)[:, 0:1]]

    def group_a(block, valid=None):
        keys = buf[block, 0]
        values = buf[block, 1]
        pieces = [softplus_block(qa_heads[h], keys, stops[h], 64 ** -0.5, later[...], valid) for h in range(2)]
        added = jnp.where(half, dot(pieces[0][0], values), dot(pieces[1][0], values))
        return added, jnp.where(half, pieces[0][1], pieces[1][1])

    def group_b(block, valid=None):
        weight, total = softplus_block(qb[...], buf[block, 2], stops[2], 128 ** -0.5, later[...], valid)
        return dot(weight, buf[block, 3]), jnp.broadcast_to(total, (rows, LANES))

    groups = (group_a, group_b)

    def cols(g):
        return slice(g * LANES, (g + 1) * LANES)

    def near(g, step):
        block = z - step
        for a in (2 * g, 2 * g + 1):
            landed(other(block, a), rsp.at[step, a])
        added, total = groups[g](block)
        accn[:, cols(g)] += jnp.exp(-ln[:, cols(g)]) * added
        ln[:, cols(g)] += total

    def distant(g, step):
        block = z + step - nz
        for a in (2 * g, 2 * g + 1):
            landed(other(block, a), rsp.at[up_steps + step, a])
        added, total = groups[g](block)
        accf[:, cols(g)] = jnp.exp(-total) * accf[:, cols(g)] + added

    def poll_up(step, a):
        @pl.when(gets_up(step, a))
        def _():
            ref = place(z - step, a)
            landed(ref, rsu.at[step - 1, a])

            @pl.when((step < ups[a]) & (z < nz - 1))
            def _():
                up_copy(step + 1, a, ref).start()

            pair_copy(step, z - step, a, ref).start()

    def poll_down(step, a):
        @pl.when(gets_down(step, a))
        def _():
            block = (z + step) % nz
            ref = place(block, a)
            landed(ref, rsd.at[step - 1, a])

            @pl.when(step < downs[a])
            def _():
                down_copy(step + 1, a, ref).start()

            @pl.when(far(step, a))
            def _():
                pair_copy(up_steps + step, block, a, ref).start()

    row_at = lax.broadcasted_iota(jnp.int32, (rows, span), 0) + c * rows
    key_at = lax.broadcasted_iota(jnp.int32, (rows, span), 1)
    valid = key_at < row_at
    for g in range(2):
        for a in (2 * g, 2 * g + 1):
            landed(other(z, a), rsp.at[0, a])
        added, total = groups[g](z, valid)
        accn[:, cols(g)] = added
        ln[:, cols(g)] = total
        for a in (2 * g, 2 * g + 1):
            poll_up(1, a)
            poll_down(1, a)

    for r in range(2, len(rounds)):
        pl.semaphore_wait(tokens.at[r], 2)
        pass_on(r + 1, along(rounds[r]))

    @pl.loop(2, up_steps + 1)
    def _(step):
        before = step - 1
        for when, piece in ((2, exchange_weights), (3, seat_rows), (4, seat_masks)):
            pl.when(step == when)(piece)
        for a in range(4):
            poll_up(step, a)
            poll_down(step, a)
            g = a // 2
            if a % 2 == 0:
                @pl.when(gets_up(before, a))
                def _():
                    near(g, before)
            else:
                @pl.when(far(before, a))
                def _():
                    distant(g, before)

    @pl.when(gets_up(up_steps, 0))
    def _():
        near(0, up_steps)

    @pl.when(far(down_steps, 2))
    def _():
        distant(1, down_steps)

    for load in loads[9:]:
        load.wait()

    pl.semaphore_wait(tokens.at[len(rounds)], 2)
    att = (accn[...] + jnp.exp(-ln[...]) * accf[...]).astype(BF)

    @drains.append
    def _():
        for a in range(4):
            pair_copy(0, z, a, srcs[a]).wait_send()

        @pl.loop(1, up_steps + 1)
        def _(step):
            for a in range(4):
                @pl.when(sends_up(step, a))
                def _():
                    up_copy(step, a, place(z + 1 - step, a)).wait_send()

                @pl.when(gets_up(step, a))
                def _():
                    pair_copy(step, z - step, a, place(z - step, a)).wait_send()

        @pl.loop(1, down_steps + 1)
        def _(step):
            for a in range(4):
                @pl.when(sends_down(step, a))
                def _():
                    down_copy(step, a, place((z + step - 1) % nz, a)).wait_send()

                @pl.when(far(step, a))
                def _():
                    pair_copy(up_steps + step, z + step - nz, a, place(z + step - nz, a)).wait_send()

        @pl.loop(1, n_tp)
        def _(k):
            for h in range(2):
                weights_remote(h, after_tp(k)).wait_send()

    def tp_copy(phase, g, src, dst):
        return pltpu.make_async_remote_copy(
            src_ref=src, dst_ref=dst, send_sem=tp_send.at[phase, g], recv_sem=tp_recv.at[phase, tp],
            device_id=(sp, g), device_id_type=MESH)

    def sp_copy(phase, d, src, dst):
        return pltpu.make_async_remote_copy(
            src_ref=src, dst_ref=dst, send_sem=sp_send.at[phase, d], recv_sem=sp_recv.at[phase, sp],
            device_id=(d, tp), device_id_type=MESH)

    def tp_drain(phase, src, dst):
        @drains.append
        def _():
            @pl.loop(1, n_tp)
            def _(k):
                g = after_tp(k)
                tp_copy(phase, g, src(g), dst).wait_send()

    @pl.loop(1, n_tp + 1)
    def _(k):
        g = after_tp(k)
        strip = pl.ds(pl.multiple_of(g * LANES, LANES), LANES)
        part[g] = dot(att, oab[:, strip]).astype(BF)

        @pl.when(k < n_tp)
        def _():
            tp_copy(0, g, part.at[g], rs.at[tp]).start()

    tp_drain(0, lambda g: part.at[g], rs.at[tp])

    def gather_rs(k, total):
        src = before_tp(k)
        landed(rs.at[src], tp_recv.at[0, src])
        return total + rs[src].astype(F32)

    mixed = lax.fori_loop(1, n_tp, gather_rs, part[tp].astype(F32))

    gained = mixed * mg[...]
    x = resid[...].astype(F32)
    lane = lax.broadcasted_iota(jnp.int32, (rows, LANES), 1)
    own = jnp.zeros((rows, LANES), F32)
    for k, product in enumerate((mixed * mixed, x * x, x * gained, gained * gained)):
        own = jnp.where(lane == k, jnp.sum(product, axis=1, keepdims=True), own)
    lines = jnp.transpose(jnp.concatenate([own, jnp.zeros((wide - rows, LANES), F32)], axis=0))[0:8, :]
    sts[...] = lines

    @pl.loop(1, n_tp)
    def _(k):
        tp_copy(1, after_tp(k), sts, st.at[tp]).start()

    tp_drain(1, lambda g: sts, st.at[tp])

    def gather_st(k, total):
        src = before_tp(k)
        landed(st.at[src], tp_recv.at[1, src])
        return total + st[src]

    lines = lax.fori_loop(1, n_tp, gather_st, lines)
    total = jnp.transpose(jnp.concatenate([lines, jnp.zeros((LANES - 8, wide), F32)], axis=0))[:rows, :]
    scale = lax.rsqrt(total[:, 0:1] / D + EPS)
    square = total[:, 1:2] + scale * (2.0 * total[:, 2:3] + scale * total[:, 3:4])
    stream = (x + gained * scale).astype(BF).astype(F32)
    scale = lax.rsqrt(jnp.maximum(square, 0.0) / D + EPS)
    normed = (stream * scale * fg[...]).astype(BF)

    tall = jnp.concatenate([normed, jnp.zeros((wide - rows, LANES), BF)], axis=0)
    dsp_out[...] = dot(choose[...], tall).reshape(n_sp, PADDED, LANES).astype(BF)

    def near_first(body):
        @pl.loop(0, nz)
        def _(k):
            reach = (k + 1) // 2
            away = (z + nz + reach * (2 * (k % 2) - 1)) % nz
            body(2 * away + 1 - c)

            @pl.when(k > 0)
            def _():
                body(2 * away + c)

    def berth(src, dst):
        return 2 * ((src // 2 + nz + nz // 4 - dst // 2) % nz) + src % 2

    def tenant(place):
        return 2 * ((z + nz - nz // 4 + place // 2) % nz) + place % 2

    def dispatch(d):
        return sp_copy(0, d, dsp_out.at[d], dsp_in.at[berth(sp, d)])

    near_first(lambda d: dispatch(d).start())
    drains.append(lambda: near_first(lambda d: dispatch(d).wait_send()))
    dsp_in[berth(sp, sp)] = dsp_out[sp]

    shp[:, :, :units] = dot(normed, sg[...]).reshape(strips, 16, units).astype(BF)
    shp[:, :, units:] = dot(normed, su[...]).reshape(strips, 16, units).astype(BF)

    @pl.loop(1, n_tp)
    def _(k):
        g = after_tp(k)

        @pl.when(g < strips)
        def _():
            tp_copy(2, g, shp.at[g], shr.at[tp]).start()

    @drains.append
    def _():
        @pl.loop(1, n_tp)
        def _(k):
            g = after_tp(k)

            @pl.when(g < strips)
            def _():
                tp_copy(2, g, shp.at[g], shr.at[tp]).wait_send()

            @pl.when(tp < strips)
            def _():
                tp_copy(3, g, shs, shh.at[tp]).wait_send()

    def gated(gate, up):
        return (gate / (1.0 + jnp.exp(-gate)) * up).astype(BF)

    def reduce_shared():
        @pl.when(tp < strips)
        def _():
            def gather(k, total):
                src = before_tp(k)
                landed(shr.at[src], tp_recv.at[2, src])
                return total + shr[src].astype(F32)

            both = lax.fori_loop(1, n_tp, gather, shp[tp].astype(F32))
            hidden = gated(both[:, :units], both[:, units:])
            shs[...] = hidden
            shh[tp] = hidden

            @pl.loop(1, n_tp)
            def _(k):
                tp_copy(3, after_tp(k), shs, shh.at[tp]).start()

    def send_rows(p):
        @pl.loop(p * homes, (p + 1) * homes)
        def _(place):
            src = tenant(place)

            @pl.when(src != sp)
            def _():
                landed(dsp_in.at[place], sp_recv.at[0, src])

        flat = dsp_in[p * homes : (p + 1) * homes].astype(F32).reshape(part_seats, LANES).astype(BF)
        xbuf[p] = dot(smat[...], flat).reshape(local, part_used, LANES).astype(BF)
        xin[p, tp] = xbuf[p, tp // quarters]

        @pl.loop(1, n_tp)
        def _(k):
            g = after_tp(k)
            tp_copy(4 + p, g, xbuf.at[p, g // quarters], xin.at[p, tp]).start()

        tp_drain(4 + p, lambda g: xbuf.at[p, g // quarters], xin.at[p, tp])

    def send_hidden(p):
        @pl.loop(1, n_tp)
        def _(k):
            src = before_tp(k)
            landed(xin.at[p, src], tp_recv.at[4 + p, src])

        x = jnp.concatenate([xin[p, g] for g in range(n_tp)], axis=1)
        both = dot(x, wgu[...].reshape(n_tp * LANES, 2 * LANES))
        hidden = gated(both[:, :LANES], both[:, LANES:])
        hs[p] = hidden
        hin[p, tp] = hidden

        @pl.loop(1, n_tp)
        def _(k):
            tp_copy(4 + parts + p, after_tp(k), hs.at[p], hin.at[p, tp]).start()

        tp_drain(4 + parts + p, lambda g: hs.at[p], hin.at[p, tp])

    def giving(place):
        d = tenant(place)
        return sp_copy(1, d, ret_out.at[place], ret_in.at[sp])

    def send_back(p):
        @pl.loop(1, n_tp)
        def _(k):
            src = before_tp(k)
            landed(hin.at[p, src], tp_recv.at[4 + parts + p, src])

        for e in range(local):
            h = jnp.concatenate([hin[p, quarters * e + q] for q in range(quarters)], axis=1)
            obuf[e * part_used : (e + 1) * part_used, :] = dot(h, ed[e]).astype(BF)
        made = dot(rmat[...], obuf[...]).reshape(homes, PADDED, LANES).astype(BF)
        ret_out[p * homes : (p + 1) * homes] = made

        @pl.loop(p * homes, (p + 1) * homes)
        def _(place):
            @pl.when(tenant(place) != sp)
            def _():
                giving(place).start()

    @drains.append
    def _():
        @pl.loop(0, n_sp)
        def _(place):
            @pl.when(tenant(place) != sp)
            def _():
                giving(place).wait_send()

    send_rows(0)
    reduce_shared()
    for h in range(2):
        src, dst = weights_copy(h, tp)
        pltpu.make_async_copy(src, dst, wloc.at[h]).wait()

    @pl.loop(1, n_tp)
    def _(k):
        src = before_tp(k)
        for h in range(2):
            landed(wgu.at[src, :, pl.ds(h * LANES, LANES)], wrecv.at[h, src])

    for p in range(1, parts):
        send_rows(p)
        send_hidden(p - 1)
    send_hidden(parts - 1)
    for p in range(parts):
        send_back(p)
    ret_in[sp] = ret_out[berth(sp, sp)]
    weights = [column(gates, k) for k in range(2)]

    @pl.loop(0, strips)
    def _(src):
        @pl.when(src != tp)
        def _():
            landed(shh.at[src], tp_recv.at[3, src])

    shared_out = dot(shh[...].reshape(rows, units), sd[...])

    @pl.loop(1, n_sp)
    def _(k):
        src = (sp + n_sp - k) % n_sp
        landed(ret_in.at[src], sp_recv.at[1, src])

    flat = ret_in[...].astype(F32).reshape(seats, LANES).astype(BF)
    routed = weights[0] * dot(oh[0], flat) + weights[1] * dot(oh[1], flat)
    out[...] = (stream + (routed + shared_out)).astype(BF)
    for drain in drains:
        drain()


def shards(query_a, key_a, value_a, query_b, key_b, value_b, stop_a, stop_b, out_a, out_b, resid, mix_gain, ffn_gain,
           routes, gates, exp_gate, exp_up, exp_down, sh_gate, sh_up, sh_down):
    n_sp, n_tp = lax.axis_size("sp"), lax.axis_size("tp")
    rows = resid.shape[0]
    local, _, units = exp_gate.shape
    used = n_sp * CAP
    strips = rows // 16
    seats = n_sp * PADDED
    parts = 2
    nz = n_sp // 2
    up_steps = nz // 2
    down_steps = nz - up_steps
    operands = (
        query_a, key_a, value_a, query_b, key_b, value_b, stop_a.T, stop_b.T, out_a, out_b, resid,
        mix_gain.reshape(1, -1), ffn_gain.reshape(1, -1), routes.T, gates.T, exp_gate, exp_up, exp_down, sh_gate,
        sh_up, sh_down)
    dma = pltpu.SemaphoreType.DMA
    vmem = pltpu.VMEM
    held = [vmem(a.shape, a.dtype) for i, a in enumerate(operands) if i not in (9, 15, 16)]
    held[8] = vmem((2 * out_a.shape[0], out_a.shape[1]), BF)
    return pl.pallas_call(
        functools.partial(layer_kernel, n_sp, n_tp),
        out_shape=jax.ShapeDtypeStruct((rows, LANES), BF),
        in_specs=[pl.BlockSpec(memory_space=pl.ANY)] * len(operands),
        out_specs=pl.BlockSpec(memory_space=pltpu.VMEM),
        scratch_shapes=held + [
            vmem((nz, 4, 2 * rows, LANES), BF),
            vmem((rows, 2 * LANES), F32),
            vmem((rows, 2 * LANES), F32),
            vmem((rows, 2 * LANES), F32),
            vmem((2 * rows, 2 * rows), BF),
            vmem((n_tp, rows, LANES), BF),
            vmem((n_tp, rows, LANES), BF),
            vmem((8, 2 * LANES), F32),
            vmem((n_tp, 8, 2 * LANES), F32),
            vmem((n_sp, PADDED, LANES), BF),
            vmem((n_sp, PADDED, LANES), BF),
            vmem((n_sp, PADDED, LANES), BF),
            vmem((n_sp, PADDED, LANES), BF),
            vmem((strips, 16, 2 * units), BF),
            vmem((n_tp, 16, 2 * units), BF),
            vmem((16, units), BF),
            vmem((strips, 16, units), BF),
            vmem((parts, local, used // parts, LANES), BF),
            vmem((parts, n_tp, used // parts, LANES), BF),
            vmem((n_tp, LANES, 2 * LANES), BF),
            vmem((parts, used // parts, LANES), BF),
            vmem((parts, n_tp, used // parts, LANES), BF),
            vmem((local * used // parts, LANES), BF),
            vmem((2, rows, seats), BF),
            vmem((seats, 2 * LANES), BF),
            vmem((local * used // parts, seats // parts), BF),
            vmem((seats // parts, local * used // parts), BF),
            dma((len(held) + 1,)),
            pltpu.SemaphoreType.REGULAR(((nz // 4).bit_length() + 1,)),
            dma((up_steps, 4)),
            dma((up_steps, 4)),
            dma((down_steps, 4)),
            dma((down_steps, 4)),
            dma((nz + 1, 4)),
            dma((nz + 1, 4)),
            dma((2, n_tp)),
            dma((2, n_tp)),
            dma((2,)),
            dma((4 + 2 * parts, n_tp)),
            dma((4 + 2 * parts, n_tp)),
            dma((2, n_sp)),
            dma((2, n_sp)),
        ],
        compiler_params=pltpu.CompilerParams(
            collective_id=0, has_side_effects=True, vmem_limit_bytes=56 * 1024 * 1024),
    )(*operands)


def solution(mesh):
    row, col, both = P("tp", None), P("tp"), P("sp", "tp")
    in_specs = (both,) * 8 + (
        row, row, both, col, col, P("sp", None), P("sp", None),
        P("sp", "tp", None), P("sp", "tp", None), P("sp", None, "tp"), row, row, P(None, "tp"))
    return jax.shard_map(shards, mesh=mesh, in_specs=in_specs, out_specs=both, check_vma=False)
```

```python
import functools

import jax
import jax.numpy as jnp
from jax import lax
from jax.experimental import pallas as pl
from jax.experimental.pallas import tpu as pltpu
from jax.sharding import PartitionSpec as P

D = 2048
EPS = 1e-06
MESH = pl.DeviceIdType.MESH
BF = jnp.bfloat16
F32 = jnp.float32
LANES = 128
CAP = 5
PADDED = 24


def dot(a, b):
    return jnp.dot(a, b, preferred_element_type=F32)


def softplus_block(query, keys, stop, scale, later, valid):
    scores = lax.dot_general(query, keys, (((1,), (1,)), ((), ())), preferred_element_type=F32)
    z = scores * scale + stop
    sp = jnp.maximum(z, 0.0) + jnp.log(1.0 + jnp.exp(-jnp.abs(z)))
    if valid is not None:
        sp = jnp.where(valid, sp, 0.0)
    after = dot(sp.astype(BF), later)
    weight = jnp.exp(z - sp - after)
    if valid is not None:
        weight = jnp.where(valid, weight, 0.0)
    return weight.astype(BF), jnp.sum(sp, axis=1, keepdims=True)


def layer_kernel(n_sp, n_tp, *refs):
    (qa_h, ka_h, va_h, qb_h, kb_h, vb_h, sa_h, sb_h, oa_h, ob_h, resid_h, mg_h, fg_h, routes_h, gates_h,
     eg, eu, ed_h, sg_h, su_h, sd_h, out,
     qa, ka, va, qb, kb, vb, sa, sb, oab, resid, mg, fg, routes, gates, ed, sg, su, sd,
     buf, accn, accf, ln, later,
     part, rs, sts, st, dsp_out, dsp_in, ret_out, ret_in, shp, shr, shs, shh, xbuf, xin, wgu, hs, hin, obuf, oh,
     choose, smat, rmat,
     lsem, tokens, ssu, rsu, ssd, rsd, ssp, rsp, wsend, wrecv, wloc, tp_send, tp_recv, sp_send, sp_recv) = refs
    rows = resid.shape[0]
    local, units = ed.shape[0], ed.shape[1]
    quarters = n_tp // local
    used = n_sp * CAP
    seats = n_sp * PADDED
    parts = 2
    part_used = used // parts
    part_seats = seats // parts
    homes = n_sp // parts
    strips = rows // 16
    wide = 2 * LANES
    nz = n_sp // 2
    up_steps = nz // 2
    down_steps = nz - up_steps
    ups = (up_steps, up_steps, nz - 1 - down_steps, nz - 1 - down_steps)
    downs = tuple(nz - 1 - n for n in ups)
    sp = lax.axis_index("sp")
    tp = lax.axis_index("tp")
    z = sp // 2
    c = sp % 2
    up_id = (2 * ((z + 1) % nz) + c, tp)
    down_id = (2 * ((z + nz - 1) % nz) + c, tp)
    pair_id = (2 * z + 1 - c, tp)
    drains = []

    barrier = pltpu.get_barrier_semaphore()

    side = quarters
    row = [(sp, tp // side * side + (tp + k) % side) for k in range(1, side)]
    column_peers = [(sp, (tp + side * k) % n_tp) for k in range(1, n_tp // side)]
    across = [(2 * ((z + step) % nz) + 1 - c, tp) for step in (1, nz - 1)]
    first = [up_id, down_id, pair_id] + across + row + column_peers
    for peer in first:
        pl.semaphore_signal(barrier, inc=1, device_id=peer, device_id_type=MESH)

    def pass_on(which, peers):
        for peer in peers:
            pl.semaphore_signal(tokens.at[which], inc=1, device_id=peer, device_id_type=MESH)

    def along(distance):
        return [(2 * ((z + step) % nz) + c, tp) for step in (distance, nz - distance)]

    rounds = [1 << r for r in range((nz // 4).bit_length())]

    staged = [
        (ka_h, ka), (va_h, va), (kb_h, kb), (vb_h, vb), (routes_h, routes), (qa_h, qa), (qb_h, qb), (sa_h, sa),
        (sb_h, sb), (oa_h, oab.at[:LANES]), (ob_h, oab.at[LANES:]), (resid_h, resid), (mg_h, mg), (fg_h, fg), (gates_h, gates),
        (ed_h, ed), (sg_h, sg), (su_h, su), (sd_h, sd)]
    loads = [pltpu.make_async_copy(a, b, lsem.at[i]) for i, (a, b) in enumerate(staged)]
    for load in loads:
        load.start()

    def column(ref, k):
        return jnp.transpose(jnp.broadcast_to(ref[k : k + 1, :].astype(F32), (LANES, rows)))

    for load in loads[:4]:
        load.wait()
    pl.semaphore_wait(barrier, len(first))
    pass_on(0, row)
    pass_on(1, along(rounds[0]))

    mine = pl.ds(pl.multiple_of(c * rows, rows), rows)
    theirs = pl.ds(pl.multiple_of((1 - c) * rows, rows), rows)
    srcs = (ka, va, kb, vb)

    def place(block, a):
        return buf.at[block, a, mine, :]

    def twin(block, g, half):
        return buf.at[block, 2 * g : 2 * g + 2, half, :]

    def up_copy(step, a, src):
        return pltpu.make_async_remote_copy(
            src_ref=src, dst_ref=place(z + 1 - step, a), send_sem=ssu.at[step - 1, a // 2], recv_sem=rsu.at[step - 1, a],
            device_id=up_id, device_id_type=MESH)

    def down_copy(step, a, src):
        return pltpu.make_async_remote_copy(
            src_ref=src, dst_ref=place((z + step - 1) % nz, a), send_sem=ssd.at[step - 1, a // 2],
            recv_sem=rsd.at[step - 1, a], device_id=down_id, device_id_type=MESH)

    def pair_copy(index, block, a, src):
        return pltpu.make_async_remote_copy(
            src_ref=src, dst_ref=place(block, a), send_sem=ssp.at[index, a // 2], recv_sem=rsp.at[index, a // 2],
            device_id=pair_id, device_id_type=MESH)

    def landed(ref, sem):
        pltpu.make_async_copy(ref, ref, sem).wait()

    def sends_up(step, a):
        return (z < nz - 1) & (z + 1 - step >= 0) & (step <= ups[a])

    def sends_down(step, a):
        return ((z + step - 1) % nz <= downs[a] - 1) & (step <= downs[a])

    def gets_up(step, a):
        return (z - step >= 0) & (step <= ups[a])

    def gets_down(step, a):
        return ((z + step) % nz <= downs[a] - 1) & (step <= downs[a])

    def far(step, a):
        return (z + step >= nz) & (step <= downs[a])

    for a in range(4):
        @pl.when(sends_up(1, a))
        def _(a=a):
            up_copy(1, a, srcs[a]).start()

        @pl.when(sends_down(1, a))
        def _(a=a):
            down_copy(1, a, srcs[a]).start()

        pair_copy(0, z, a, srcs[a]).start()
        buf[z, a, mine, :] = srcs[a][...]

    def after_tp(k):
        return (tp + k) % n_tp

    def weights_copy(h, g):
        src = (eg, eu)[h].at[g // quarters, :, pl.ds(pl.multiple_of((g % quarters) * LANES, LANES), LANES)]
        dst = wgu.at[tp, :, pl.ds(h * LANES, LANES)]
        return src, dst

    def weights_remote(h, g):
        src, dst = weights_copy(h, g)
        return pltpu.make_async_remote_copy(
            src_ref=src, dst_ref=dst, send_sem=wsend.at[0], recv_sem=wrecv.at[0],
            device_id=(sp, g), device_id_type=MESH)

    span = 2 * rows
    j = lax.broadcasted_iota(jnp.int32, (span, span), 0)
    s = lax.broadcasted_iota(jnp.int32, (span, span), 1)
    later[...] = (j > s).astype(BF)
    accf[...] = jnp.zeros_like(accf)
    half = lax.broadcasted_iota(jnp.int32, (rows, LANES), 1) < LANES // 2

    def index_of(shape, dim):
        return lax.broadcasted_iota(jnp.int32, shape, dim).astype(F32)

    def exchange_weights():
        pl.semaphore_wait(tokens.at[0], len(row))

        @pl.loop(1, n_tp)
        def _(k):
            for h in range(2):
                weights_remote(h, after_tp(k)).start()

        for h in range(2):
            src, dst = weights_copy(h, tp)
            pltpu.make_async_copy(src, dst, wloc.at[h]).start()

    def seat_masks():
        i = index_of((local * part_used, LANES), 0)
        e = jnp.floor((i + 0.5) * (1.0 / part_used))
        i = i - part_used * e
        g = jnp.floor((i + 0.5) * (1.0 / CAP))
        seat = g * PADDED + e * CAP + (i - CAP * g)
        smat[...] = (index_of((local * part_used, part_seats), 1) == seat[:, 0:1]).astype(BF)
        i = index_of((part_seats, LANES), 0)
        g = jnp.floor((i + 0.5) * (1.0 / PADDED))
        i = i - PADDED * g
        e = jnp.floor((i + 0.5) * (1.0 / CAP))
        seat = jnp.where(e < local, e * part_used + g * CAP + (i - CAP * e), -1.0)
        rmat[...] = (index_of((part_seats, local * part_used), 1) == seat[:, 0:1]).astype(BF)

    def seat_rows():
        loads[4].wait()
        experts = local * n_sp
        e_at = index_of((rows, experts), 1)
        named_by = [column(routes, k) for k in range(2)]
        named = [e_at == named_by[k][:, 0:1] for k in range(2)]
        members = jnp.where(named[0] | named[1], 1.0, 0.0).astype(BF)
        prior = dot((index_of((rows, rows), 1) < index_of((rows, rows), 0)).astype(BF), members)
        hits = None
        for k in range(2):
            home = jnp.floor((named_by[k] + 0.5) * (1.0 / local))
            rank = jnp.sum(jnp.where(named[k], prior, 0.0), axis=1, keepdims=True)
            seat = home * PADDED + (named_by[k] - local * home) * CAP + rank
            oh[k] = (index_of((rows, seats), 1) == seat[:, 0:1]).astype(BF)
            tall = jnp.concatenate([seat, jnp.full((wide - rows, LANES), -1.0, F32)], axis=0)
            hit = index_of((seats, wide), 0) == jnp.transpose(tall)[0:1, :]
            hits = hit if hits is None else hits | hit
        choose[...] = hits.astype(BF)

    for load in loads[5:9]:
        load.wait()
    pl.semaphore_wait(tokens.at[1], 2)
    pass_on(2, along(rounds[1]))
    qa_all = qa[...]
    zero = jnp.zeros_like(qa_all)
    qa_heads = (jnp.where(half, qa_all, zero), jnp.where(half, zero, qa_all))
    stops = [column(sa, 0)[:, 0:1], column(sa, 1)[:, 0:1], column(sb, 0)[:, 0:1]]

    def group_a(block, valid=None):
        keys = buf[block, 0]
        values = buf[block, 1]
        pieces = [softplus_block(qa_heads[h], keys, stops[h], 64 ** -0.5, later[...], valid) for h in range(2)]
        added = jnp.where(half, dot(pieces[0][0], values), dot(pieces[1][0], values))
        return added, jnp.where(half, pieces[0][1], pieces[1][1])

    def group_b(block, valid=None):
        weight, total = softplus_block(qb[...], buf[block, 2], stops[2], 128 ** -0.5, later[...], valid)
        return dot(weight, buf[block, 3]), jnp.broadcast_to(total, (rows, LANES))

    groups = (group_a, group_b)

    def cols(g):
        return slice(g * LANES, (g + 1) * LANES)

    def near(g, step):
        block = z - step
        landed(twin(block, g, theirs), rsp.at[step, g])
        added, total = groups[g](block)
        accn[:, cols(g)] += jnp.exp(-ln[:, cols(g)]) * added
        ln[:, cols(g)] += total

    def distant(g, step):
        block = z + step - nz
        landed(twin(block, g, theirs), rsp.at[up_steps + step, g])
        added, total = groups[g](block)
        accf[:, cols(g)] = jnp.exp(-total) * accf[:, cols(g)] + added

    def poll_up(step, a):
        @pl.when(gets_up(step, a))
        def _():
            ref = place(z - step, a)
            landed(ref, rsu.at[step - 1, a])

            @pl.when((step < ups[a]) & (z < nz - 1))
            def _():
                up_copy(step + 1, a, ref).start()

            pair_copy(step, z - step, a, ref).start()

    def poll_down(step, a):
        @pl.when(gets_down(step, a))
        def _():
            block = (z + step) % nz
            ref = place(block, a)
            landed(ref, rsd.at[step - 1, a])

            @pl.when(step < downs[a])
            def _():
                down_copy(step + 1, a, ref).start()

            @pl.when(far(step, a))
            def _():
                pair_copy(up_steps + step, block, a, ref).start()

    row_at = lax.broadcasted_iota(jnp.int32, (rows, span), 0) + c * rows
    key_at = lax.broadcasted_iota(jnp.int32, (rows, span), 1)
    valid = key_at < row_at
    for g in range(2):
        landed(twin(z, g, theirs), rsp.at[0, g])
        added, total = groups[g](z, valid)
        accn[:, cols(g)] = added
        ln[:, cols(g)] = total
        for a in (2 * g, 2 * g + 1):
            poll_up(1, a)
            poll_down(1, a)

    for r in range(2, len(rounds)):
        pl.semaphore_wait(tokens.at[r], 2)
        pass_on(r + 1, along(rounds[r]))

    @pl.loop(2, up_steps + 1)
    def _(step):
        before = step - 1
        for when, piece in ((2, exchange_weights), (3, seat_rows), (4, seat_masks)):
            pl.when(step == when)(piece)
        for a in range(4):
            poll_up(step, a)
            poll_down(step, a)
            g = a // 2
            if a % 2 == 0:
                @pl.when(gets_up(before, a))
                def _():
                    near(g, before)
            else:
                @pl.when(far(before, a))
                def _():
                    distant(g, before)

    @pl.when(gets_up(up_steps, 0))
    def _():
        near(0, up_steps)

    @pl.when(far(down_steps, 2))
    def _():
        distant(1, down_steps)

    for load in loads[9:]:
        load.wait()

    pl.semaphore_wait(tokens.at[len(rounds)], 2)
    att = (accn[...] + jnp.exp(-ln[...]) * accf[...]).astype(BF)

    @drains.append
    def _():
        for g in range(2):
            landed(twin(z, g, mine), ssp.at[0, g])

        @pl.loop(1, up_steps + 1)
        def _(step):
            for g in range(2):
                @pl.when(sends_up(step, 2 * g))
                def _():
                    landed(twin(z + 1 - step, g, mine), ssu.at[step - 1, g])

                @pl.when(gets_up(step, 2 * g))
                def _():
                    landed(twin(z - step, g, mine), ssp.at[step, g])

        @pl.loop(1, down_steps + 1)
        def _(step):
            for g in range(2):
                @pl.when(sends_down(step, 2 * g))
                def _():
                    landed(twin((z + step - 1) % nz, g, mine), ssd.at[step - 1, g])

                @pl.when(far(step, 2 * g))
                def _():
                    landed(twin(z + step - nz, g, mine), ssp.at[up_steps + step, g])

        landed(wgu.at[: n_tp - 1], wsend.at[0])

    def tp_copy(phase, g, src, dst):
        return pltpu.make_async_remote_copy(
            src_ref=src, dst_ref=dst, send_sem=tp_send.at[phase], recv_sem=tp_recv.at[phase],
            device_id=(sp, g), device_id_type=MESH)

    def sp_copy(phase, d, src, dst, part_of=0):
        return pltpu.make_async_remote_copy(
            src_ref=src, dst_ref=dst, send_sem=sp_send.at[phase], recv_sem=sp_recv.at[phase * parts + part_of],
            device_id=(d, tp), device_id_type=MESH)

    def from_all(ref, phase):
        landed(ref.at[: n_tp - 1], tp_recv.at[phase])

    def tp_drain(phase, ref):
        drains.append(lambda: landed(ref, tp_send.at[phase]))

    @pl.loop(1, n_tp + 1)
    def _(k):
        g = after_tp(k)
        strip = pl.ds(pl.multiple_of(g * LANES, LANES), LANES)
        part[g] = dot(att, oab[:, strip]).astype(BF)

        @pl.when(k < n_tp)
        def _():
            tp_copy(0, g, part.at[g], rs.at[tp]).start()

    tp_drain(0, part.at[: n_tp - 1])

    def added_up(ref):
        total = ref[0].astype(F32)
        for g in range(1, n_tp):
            total = total + ref[g].astype(F32)
        return total

    rs[tp] = part[tp]
    from_all(rs, 0)
    mixed = added_up(rs)

    gained = mixed * mg[...]
    x = resid[...].astype(F32)
    lane = lax.broadcasted_iota(jnp.int32, (rows, LANES), 1)
    own = jnp.zeros((rows, LANES), F32)
    for k, product in enumerate((mixed * mixed, x * x, x * gained, gained * gained)):
        own = jnp.where(lane == k, jnp.sum(product, axis=1, keepdims=True), own)
    lines = jnp.transpose(jnp.concatenate([own, jnp.zeros((wide - rows, LANES), F32)], axis=0))[0:8, :]
    sts[...] = lines

    @pl.loop(1, n_tp)
    def _(k):
        tp_copy(1, after_tp(k), sts, st.at[tp]).start()

    tp_drain(1, st.at[: n_tp - 1])

    st[tp] = lines
    from_all(st, 1)
    lines = added_up(st)
    total = jnp.transpose(jnp.concatenate([lines, jnp.zeros((LANES - 8, wide), F32)], axis=0))[:rows, :]
    scale = lax.rsqrt(total[:, 0:1] / D + EPS)
    square = total[:, 1:2] + scale * (2.0 * total[:, 2:3] + scale * total[:, 3:4])
    stream = (x + gained * scale).astype(BF).astype(F32)
    scale = lax.rsqrt(jnp.maximum(square, 0.0) / D + EPS)
    normed = (stream * scale * fg[...]).astype(BF)

    tall = jnp.concatenate([normed, jnp.zeros((wide - rows, LANES), BF)], axis=0)
    dsp_out[...] = dot(choose[...], tall).reshape(n_sp, PADDED, LANES).astype(BF)

    def near_first(body):
        @pl.loop(0, nz)
        def _(k):
            reach = (k + 1) // 2
            away = (z + nz + reach * (2 * (k % 2) - 1)) % nz
            body(2 * away + 1 - c)

            @pl.when(k > 0)
            def _():
                body(2 * away + c)

    def berth(src, dst):
        return 2 * ((src // 2 + nz + nz // 4 - dst // 2) % nz) + src % 2

    def tenant(place):
        return 2 * ((z + nz - nz // 4 + place // 2) % nz) + place % 2

    def dispatch(d):
        return sp_copy(0, d, dsp_out.at[d], dsp_in.at[berth(sp, d)], berth(sp, d) // homes)

    near_first(lambda d: dispatch(d).start())
    drains.append(lambda: landed(dsp_out.at[: n_sp - 1], sp_send.at[0]))
    dsp_in[berth(sp, sp)] = dsp_out[sp]

    shp[:, :, :units] = dot(normed, sg[...]).reshape(strips, 16, units).astype(BF)
    shp[:, :, units:] = dot(normed, su[...]).reshape(strips, 16, units).astype(BF)

    @pl.loop(1, n_tp)
    def _(k):
        g = after_tp(k)

        @pl.when(g < strips)
        def _():
            tp_copy(2, g, shp.at[g], shr.at[tp]).start()

    @drains.append
    def _():
        @pl.when(tp < strips)
        def _():
            landed(shp.at[: strips - 1], tp_send.at[2])
            landed(shr.at[: n_tp - 1, :, :units], tp_send.at[3])

        @pl.when(tp >= strips)
        def _():
            landed(shp, tp_send.at[2])

    def gated(gate, up):
        return (gate / (1.0 + jnp.exp(-gate)) * up).astype(BF)

    def reduce_shared():
        @pl.when(tp < strips)
        def _():
            shr[tp] = shp[tp]
            from_all(shr, 2)
            both = added_up(shr)
            hidden = gated(both[:, :units], both[:, units:])
            shs[...] = hidden
            shh[tp] = hidden

            @pl.loop(1, n_tp)
            def _(k):
                tp_copy(3, after_tp(k), shs, shh.at[tp]).start()

    def send_rows(p):
        first_one = p * homes if p else 1
        landed(dsp_in.at[first_one : (p + 1) * homes], sp_recv.at[p])
        flat = dsp_in[p * homes : (p + 1) * homes].astype(F32).reshape(part_seats, LANES).astype(BF)
        xbuf[p] = dot(smat[...], flat).reshape(local, part_used, LANES).astype(BF)
        xin[p, tp] = xbuf[p, tp // quarters]

        @pl.loop(1, n_tp)
        def _(k):
            g = after_tp(k)
            tp_copy(4 + p, g, xbuf.at[p, g // quarters], xin.at[p, tp]).start()

        tp_drain(4 + p, xin.at[p, : n_tp - 1])

    def send_hidden(p):
        from_all(xin.at[p], 4 + p)
        x = jnp.concatenate([xin[p, g] for g in range(n_tp)], axis=1)
        both = dot(x, wgu[...].reshape(n_tp * LANES, 2 * LANES))
        hidden = gated(both[:, :LANES], both[:, LANES:])
        hs[p] = hidden
        hin[p, tp] = hidden

        @pl.loop(1, n_tp)
        def _(k):
            tp_copy(4 + parts + p, after_tp(k), hs.at[p], hin.at[p, tp]).start()

        tp_drain(4 + parts + p, hin.at[p, : n_tp - 1])

    def giving(place):
        d = tenant(place)
        return sp_copy(1, d, ret_out.at[place], ret_in.at[sp])

    def send_back(p):
        from_all(hin.at[p], 4 + parts + p)
        for e in range(local):
            h = jnp.concatenate([hin[p, quarters * e + q] for q in range(quarters)], axis=1)
            obuf[e * part_used : (e + 1) * part_used, :] = dot(h, ed[e]).astype(BF)
        made = dot(rmat[...], obuf[...]).reshape(homes, PADDED, LANES).astype(BF)
        ret_out[p * homes : (p + 1) * homes] = made

        @pl.loop(p * homes, (p + 1) * homes)
        def _(place):
            @pl.when(tenant(place) != sp)
            def _():
                giving(place).start()

    drains.append(lambda: landed(ret_out.at[: n_sp - 1], sp_send.at[1]))

    send_rows(0)
    reduce_shared()
    for h in range(2):
        src, dst = weights_copy(h, tp)
        pltpu.make_async_copy(src, dst, wloc.at[h]).wait()

    landed(wgu.at[: n_tp - 1], wrecv.at[0])
    for p in range(1, parts):
        send_rows(p)
        send_hidden(p - 1)
    send_hidden(parts - 1)
    for p in range(parts):
        send_back(p)
    ret_in[sp] = ret_out[berth(sp, sp)]
    weights = [column(gates, k) for k in range(2)]

    @pl.when(tp < strips)
    def _():
        landed(shh.at[: strips - 1], tp_recv.at[3])

    @pl.when(tp >= strips)
    def _():
        landed(shh, tp_recv.at[3])

    shared_out = dot(shh[...].reshape(rows, units), sd[...])

    landed(ret_in.at[: n_sp - 1], sp_recv.at[parts])
    flat = ret_in[...].astype(F32).reshape(seats, LANES).astype(BF)
    routed = weights[0] * dot(oh[0], flat) + weights[1] * dot(oh[1], flat)
    out[...] = (stream + (routed + shared_out)).astype(BF)
    for drain in drains:
        drain()


def shards(query_a, key_a, value_a, query_b, key_b, value_b, stop_a, stop_b, out_a, out_b, resid, mix_gain, ffn_gain,
           routes, gates, exp_gate, exp_up, exp_down, sh_gate, sh_up, sh_down):
    n_sp, n_tp = lax.axis_size("sp"), lax.axis_size("tp")
    rows = resid.shape[0]
    local, _, units = exp_gate.shape
    used = n_sp * CAP
    strips = rows // 16
    seats = n_sp * PADDED
    parts = 2
    nz = n_sp // 2
    up_steps = nz // 2
    down_steps = nz - up_steps
    operands = (
        query_a, key_a, value_a, query_b, key_b, value_b, stop_a.T, stop_b.T, out_a, out_b, resid,
        mix_gain.reshape(1, -1), ffn_gain.reshape(1, -1), routes.T, gates.T, exp_gate, exp_up, exp_down, sh_gate,
        sh_up, sh_down)
    dma = pltpu.SemaphoreType.DMA
    vmem = pltpu.VMEM
    held = [vmem(a.shape, a.dtype) for i, a in enumerate(operands) if i not in (9, 15, 16)]
    held[8] = vmem((2 * out_a.shape[0], out_a.shape[1]), BF)
    return pl.pallas_call(
        functools.partial(layer_kernel, n_sp, n_tp),
        out_shape=jax.ShapeDtypeStruct((rows, LANES), BF),
        in_specs=[pl.BlockSpec(memory_space=pl.ANY)] * len(operands),
        out_specs=pl.BlockSpec(memory_space=pltpu.VMEM),
        scratch_shapes=held + [
            vmem((nz, 4, 2 * rows, LANES), BF),
            vmem((rows, 2 * LANES), F32),
            vmem((rows, 2 * LANES), F32),
            vmem((rows, 2 * LANES), F32),
            vmem((2 * rows, 2 * rows), BF),
            vmem((n_tp, rows, LANES), BF),
            vmem((n_tp, rows, LANES), BF),
            vmem((8, 2 * LANES), F32),
            vmem((n_tp, 8, 2 * LANES), F32),
            vmem((n_sp, PADDED, LANES), BF),
            vmem((n_sp, PADDED, LANES), BF),
            vmem((n_sp, PADDED, LANES), BF),
            vmem((n_sp, PADDED, LANES), BF),
            vmem((strips, 16, 2 * units), BF),
            vmem((n_tp, 16, 2 * units), BF),
            vmem((16, units), BF),
            vmem((strips, 16, units), BF),
            vmem((parts, local, used // parts, LANES), BF),
            vmem((parts, n_tp, used // parts, LANES), BF),
            vmem((n_tp, LANES, 2 * LANES), BF),
            vmem((parts, used // parts, LANES), BF),
            vmem((parts, n_tp, used // parts, LANES), BF),
            vmem((local * used // parts, LANES), BF),
            vmem((2, rows, seats), BF),
            vmem((seats, 2 * LANES), BF),
            vmem((local * used // parts, seats // parts), BF),
            vmem((seats // parts, local * used // parts), BF),
            dma((len(held) + 1,)),
            pltpu.SemaphoreType.REGULAR(((nz // 4).bit_length() + 1,)),
            dma((up_steps, 2)),
            dma((up_steps, 4)),
            dma((down_steps, 2)),
            dma((down_steps, 4)),
            dma((nz + 1, 2)),
            dma((nz + 1, 2)),
            dma((1,)),
            dma((1,)),
            dma((2,)),
            dma((4 + 2 * parts,)),
            dma((4 + 2 * parts,)),
            dma((2,)),
            dma((parts + 1,)),
        ],
        compiler_params=pltpu.CompilerParams(
            collective_id=0, has_side_effects=True, vmem_limit_bytes=56 * 1024 * 1024),
    )(*operands)


def solution(mesh):
    row, col, both = P("tp", None), P("tp"), P("sp", "tp")
    in_specs = (both,) * 8 + (
        row, row, both, col, col, P("sp", None), P("sp", None),
        P("sp", "tp", None), P("sp", "tp", None), P("sp", None, "tp"), row, row, P(None, "tp"))
    return jax.shard_map(shards, mesh=mesh, in_specs=in_specs, out_specs=both, check_vma=False)
```

```python
import functools

import jax
import jax.numpy as jnp
from jax import lax
from jax.experimental import pallas as pl
from jax.experimental.pallas import tpu as pltpu
from jax.sharding import PartitionSpec as P

D = 2048
EPS = 1e-06
MESH = pl.DeviceIdType.MESH
BF = jnp.bfloat16
F32 = jnp.float32
LANES = 128
CAP = 5
PADDED = 24


def dot(a, b):
    return jnp.dot(a, b, preferred_element_type=F32)


def softplus_block(query, keys, stop, scale, later, valid):
    scores = lax.dot_general(query, keys, (((1,), (1,)), ((), ())), preferred_element_type=F32)
    z = scores * scale + stop
    sp = jnp.maximum(z, 0.0) + jnp.log(1.0 + jnp.exp(-jnp.abs(z)))
    if valid is not None:
        sp = jnp.where(valid, sp, 0.0)
    after = dot(sp.astype(BF), later)
    weight = jnp.exp(z - sp - after)
    if valid is not None:
        weight = jnp.where(valid, weight, 0.0)
    return weight.astype(BF), jnp.sum(sp, axis=1, keepdims=True)


def layer_kernel(n_sp, n_tp, *refs):
    (qa_h, ka_h, va_h, qb_h, kb_h, vb_h, sa_h, sb_h, oa_h, ob_h, resid_h, mg_h, fg_h, routes_h, gates_h,
     eg, eu, ed_h, sg_h, su_h, sd_h, out,
     qa, ka, va, qb, kb, vb, sa, sb, oab, resid, mg, fg, routes, gates, ed, sg, su, sd,
     buf, accn, accf, ln, later,
     part, rs, sts, st, dsp_out, dsp_in, ret_out, ret_in, shp, shr, shs, shh, xbuf, xin, wgu, hs, hin, obuf, oh,
     choose, smat, rmat,
     lsem, tokens, ssu, rsu, ssd, rsd, ssp, rsp, wsend, wrecv, wloc, tp_send, tp_recv, sp_send, sp_recv) = refs
    rows = resid.shape[0]
    local, units = ed.shape[0], ed.shape[1]
    quarters = n_tp // local
    used = n_sp * CAP
    seats = n_sp * PADDED
    parts = 2
    filled = local * CAP
    part_used = used // parts
    part_seats = seats // parts
    homes = n_sp // parts
    strips = rows // 16
    wide = 2 * LANES
    nz = n_sp // 2
    up_steps = nz // 2
    down_steps = nz - up_steps
    ups = (up_steps, up_steps, nz - 1 - down_steps, nz - 1 - down_steps)
    downs = tuple(nz - 1 - n for n in ups)
    sp = lax.axis_index("sp")
    tp = lax.axis_index("tp")
    z = sp // 2
    c = sp % 2
    up_id = (2 * ((z + 1) % nz) + c, tp)
    down_id = (2 * ((z + nz - 1) % nz) + c, tp)
    pair_id = (2 * z + 1 - c, tp)
    drains = []

    dsp_in[...] = jnp.zeros_like(dsp_in)
    ret_in[...] = jnp.zeros_like(ret_in)
    st[...] = jnp.zeros_like(st)
    barrier = pltpu.get_barrier_semaphore()

    side = quarters
    row = [(sp, tp // side * side + (tp + k) % side) for k in range(1, side)]
    column_peers = [(sp, (tp + side * k) % n_tp) for k in range(1, n_tp // side)]
    across = [(2 * ((z + step) % nz) + 1 - c, tp) for step in (1, nz - 1)]
    first = [up_id, down_id, pair_id] + across + row + column_peers
    for peer in first:
        pl.semaphore_signal(barrier, inc=1, device_id=peer, device_id_type=MESH)

    def pass_on(which, peers):
        for peer in peers:
            pl.semaphore_signal(tokens.at[which], inc=1, device_id=peer, device_id_type=MESH)

    def along(distance):
        return [(2 * ((z + step) % nz) + c, tp) for step in (distance, nz - distance)]

    rounds = [1 << r for r in range((nz // 4).bit_length())]

    staged = [
        (ka_h, ka), (va_h, va), (kb_h, kb), (vb_h, vb), (routes_h, routes), (qa_h, qa), (qb_h, qb), (sa_h, sa),
        (sb_h, sb), (oa_h, oab.at[:LANES]), (ob_h, oab.at[LANES:]), (resid_h, resid), (mg_h, mg), (fg_h, fg), (gates_h, gates),
        (ed_h, ed), (sg_h, sg), (su_h, su), (sd_h, sd)]
    loads = [pltpu.make_async_copy(a, b, lsem.at[i]) for i, (a, b) in enumerate(staged)]
    for load in loads:
        load.start()

    def column(ref, k):
        return jnp.transpose(jnp.broadcast_to(ref[k : k + 1, :].astype(F32), (LANES, rows)))

    for load in loads[:4]:
        load.wait()
    pl.semaphore_wait(barrier, len(first))
    pass_on(0, row)
    pass_on(1, along(rounds[0]))

    mine = pl.ds(pl.multiple_of(c * rows, rows), rows)
    theirs = pl.ds(pl.multiple_of((1 - c) * rows, rows), rows)
    srcs = (ka, va, kb, vb)

    def place(block, a):
        return buf.at[block, a, mine, :]

    def twin(block, g, half):
        return buf.at[block, 2 * g : 2 * g + 2, half, :]

    def up_copy(step, a, src):
        return pltpu.make_async_remote_copy(
            src_ref=src, dst_ref=place(z + 1 - step, a), send_sem=ssu.at[step - 1, a // 2], recv_sem=rsu.at[step - 1, a],
            device_id=up_id, device_id_type=MESH)

    def down_copy(step, a, src):
        return pltpu.make_async_remote_copy(
            src_ref=src, dst_ref=place((z + step - 1) % nz, a), send_sem=ssd.at[step - 1, a // 2],
            recv_sem=rsd.at[step - 1, a], device_id=down_id, device_id_type=MESH)

    def pair_copy(index, block, a, src):
        return pltpu.make_async_remote_copy(
            src_ref=src, dst_ref=place(block, a), send_sem=ssp.at[index, a // 2], recv_sem=rsp.at[index, a // 2],
            device_id=pair_id, device_id_type=MESH)

    def landed(ref, sem):
        pltpu.make_async_copy(ref, ref, sem).wait()

    def sends_up(step, a):
        return (z < nz - 1) & (z + 1 - step >= 0) & (step <= ups[a])

    def sends_down(step, a):
        return ((z + step - 1) % nz <= downs[a] - 1) & (step <= downs[a])

    def gets_up(step, a):
        return (z - step >= 0) & (step <= ups[a])

    def gets_down(step, a):
        return ((z + step) % nz <= downs[a] - 1) & (step <= downs[a])

    def far(step, a):
        return (z + step >= nz) & (step <= downs[a])

    for a in range(4):
        @pl.when(sends_up(1, a))
        def _(a=a):
            up_copy(1, a, srcs[a]).start()

        @pl.when(sends_down(1, a))
        def _(a=a):
            down_copy(1, a, srcs[a]).start()

        pair_copy(0, z, a, srcs[a]).start()
        buf[z, a, mine, :] = srcs[a][...]

    def after_tp(k):
        return (tp + k) % n_tp

    def weights_copy(h, g):
        src = (eg, eu)[h].at[g // quarters, :, pl.ds(pl.multiple_of((g % quarters) * LANES, LANES), LANES)]
        dst = wgu.at[tp, :, pl.ds(h * LANES, LANES)]
        return src, dst

    def weights_remote(h, g):
        src, dst = weights_copy(h, g)
        return pltpu.make_async_remote_copy(
            src_ref=src, dst_ref=dst, send_sem=wsend.at[0], recv_sem=wrecv.at[0],
            device_id=(sp, g), device_id_type=MESH)

    span = 2 * rows
    j = lax.broadcasted_iota(jnp.int32, (span, span), 0)
    s = lax.broadcasted_iota(jnp.int32, (span, span), 1)
    later[...] = (j > s).astype(BF)
    accf[...] = jnp.zeros_like(accf)
    half = lax.broadcasted_iota(jnp.int32, (rows, LANES), 1) < LANES // 2

    def index_of(shape, dim):
        return lax.broadcasted_iota(jnp.int32, shape, dim).astype(F32)

    def exchange_weights():
        pl.semaphore_wait(tokens.at[0], len(row))

        @pl.loop(1, n_tp)
        def _(k):
            for h in range(2):
                weights_remote(h, after_tp(k)).start()

        for h in range(2):
            src, dst = weights_copy(h, tp)
            pltpu.make_async_copy(src, dst, wloc.at[h]).start()

    def seat_masks():
        i = index_of((local * part_used, LANES), 0)
        e = jnp.floor((i + 0.5) * (1.0 / part_used))
        i = i - part_used * e
        g = jnp.floor((i + 0.5) * (1.0 / CAP))
        seat = g * PADDED + e * CAP + (i - CAP * g)
        smat[...] = (index_of((local * part_used, part_seats), 1) == seat[:, 0:1]).astype(BF)
        i = index_of((part_seats, LANES), 0)
        g = jnp.floor((i + 0.5) * (1.0 / PADDED))
        i = i - PADDED * g
        e = jnp.floor((i + 0.5) * (1.0 / CAP))
        seat = jnp.where(e < local, e * part_used + g * CAP + (i - CAP * e), -1.0)
        rmat[...] = (index_of((part_seats, local * part_used), 1) == seat[:, 0:1]).astype(BF)

    def seat_rows():
        loads[4].wait()
        experts = local * n_sp
        e_at = index_of((rows, experts), 1)
        named_by = [column(routes, k) for k in range(2)]
        named = [e_at == named_by[k][:, 0:1] for k in range(2)]
        members = jnp.where(named[0] | named[1], 1.0, 0.0).astype(BF)
        prior = dot((index_of((rows, rows), 1) < index_of((rows, rows), 0)).astype(BF), members)
        hits = None
        for k in range(2):
            home = jnp.floor((named_by[k] + 0.5) * (1.0 / local))
            rank = jnp.sum(jnp.where(named[k], prior, 0.0), axis=1, keepdims=True)
            seat = home * PADDED + (named_by[k] - local * home) * CAP + rank
            oh[k] = (index_of((rows, seats), 1) == seat[:, 0:1]).astype(BF)
            tall = jnp.concatenate([seat, jnp.full((wide - rows, LANES), -1.0, F32)], axis=0)
            hit = index_of((seats, wide), 0) == jnp.transpose(tall)[0:1, :]
            hits = hit if hits is None else hits | hit
        choose[...] = hits.astype(BF)

    for load in loads[5:9]:
        load.wait()
    pl.semaphore_wait(tokens.at[1], 2)
    pass_on(2, along(rounds[1]))
    qa_all = qa[...]
    zero = jnp.zeros_like(qa_all)
    qa_heads = (jnp.where(half, qa_all, zero), jnp.where(half, zero, qa_all))
    stops = [column(sa, 0)[:, 0:1], column(sa, 1)[:, 0:1], column(sb, 0)[:, 0:1]]

    def group_a(block, valid=None):
        keys = buf[block, 0]
        values = buf[block, 1]
        pieces = [softplus_block(qa_heads[h], keys, stops[h], 64 ** -0.5, later[...], valid) for h in range(2)]
        added = jnp.where(half, dot(pieces[0][0], values), dot(pieces[1][0], values))
        return added, jnp.where(half, pieces[0][1], pieces[1][1])

    def group_b(block, valid=None):
        weight, total = softplus_block(qb[...], buf[block, 2], stops[2], 128 ** -0.5, later[...], valid)
        return dot(weight, buf[block, 3]), jnp.broadcast_to(total, (rows, LANES))

    groups = (group_a, group_b)

    def cols(g):
        return slice(g * LANES, (g + 1) * LANES)

    def near(g, step):
        block = z - step
        landed(twin(block, g, theirs), rsp.at[step, g])
        added, total = groups[g](block)
        accn[:, cols(g)] += jnp.exp(-ln[:, cols(g)]) * added
        ln[:, cols(g)] += total

    def distant(g, step):
        block = z + step - nz
        landed(twin(block, g, theirs), rsp.at[up_steps + step, g])
        added, total = groups[g](block)
        accf[:, cols(g)] = jnp.exp(-total) * accf[:, cols(g)] + added

    def poll_up(step, a):
        @pl.when(gets_up(step, a))
        def _():
            ref = place(z - step, a)
            landed(ref, rsu.at[step - 1, a])

            @pl.when((step < ups[a]) & (z < nz - 1))
            def _():
                up_copy(step + 1, a, ref).start()

            pair_copy(step, z - step, a, ref).start()

    def poll_down(step, a):
        @pl.when(gets_down(step, a))
        def _():
            block = (z + step) % nz
            ref = place(block, a)
            landed(ref, rsd.at[step - 1, a])

            @pl.when(step < downs[a])
            def _():
                down_copy(step + 1, a, ref).start()

            @pl.when(far(step, a))
            def _():
                pair_copy(up_steps + step, block, a, ref).start()

    row_at = lax.broadcasted_iota(jnp.int32, (rows, span), 0) + c * rows
    key_at = lax.broadcasted_iota(jnp.int32, (rows, span), 1)
    valid = key_at < row_at
    for g in range(2):
        landed(twin(z, g, theirs), rsp.at[0, g])
        added, total = groups[g](z, valid)
        accn[:, cols(g)] = added
        ln[:, cols(g)] = total
        for a in (2 * g, 2 * g + 1):
            poll_up(1, a)
            poll_down(1, a)

    for r in range(2, len(rounds)):
        pl.semaphore_wait(tokens.at[r], 2)
        pass_on(r + 1, along(rounds[r]))

    @pl.loop(2, up_steps + 1)
    def _(step):
        before = step - 1
        for when, piece in ((2, exchange_weights), (3, seat_rows), (4, seat_masks)):
            pl.when(step == when)(piece)
        for a in range(4):
            poll_up(step, a)
            poll_down(step, a)
            g = a // 2
            if a % 2 == 0:
                @pl.when(gets_up(before, a))
                def _():
                    near(g, before)
            else:
                @pl.when(far(before, a))
                def _():
                    distant(g, before)

    @pl.when(gets_up(up_steps, 0))
    def _():
        near(0, up_steps)

    @pl.when(far(down_steps, 2))
    def _():
        distant(1, down_steps)

    for load in loads[9:]:
        load.wait()

    pl.semaphore_wait(tokens.at[len(rounds)], 2)
    att = (accn[...] + jnp.exp(-ln[...]) * accf[...]).astype(BF)

    @drains.append
    def _():
        for g in range(2):
            landed(twin(z, g, mine), ssp.at[0, g])

        @pl.loop(1, up_steps + 1)
        def _(step):
            for g in range(2):
                @pl.when(sends_up(step, 2 * g))
                def _():
                    landed(twin(z + 1 - step, g, mine), ssu.at[step - 1, g])

                @pl.when(gets_up(step, 2 * g))
                def _():
                    landed(twin(z - step, g, mine), ssp.at[step, g])

        @pl.loop(1, down_steps + 1)
        def _(step):
            for g in range(2):
                @pl.when(sends_down(step, 2 * g))
                def _():
                    landed(twin((z + step - 1) % nz, g, mine), ssd.at[step - 1, g])

                @pl.when(far(step, 2 * g))
                def _():
                    landed(twin(z + step - nz, g, mine), ssp.at[up_steps + step, g])

        landed(wgu.at[: n_tp - 1], wsend.at[0])

    def tp_copy(phase, g, src, dst):
        return pltpu.make_async_remote_copy(
            src_ref=src, dst_ref=dst, send_sem=tp_send.at[phase], recv_sem=tp_recv.at[phase],
            device_id=(sp, g), device_id_type=MESH)

    def sp_copy(phase, d, src, dst, part_of=0):
        return pltpu.make_async_remote_copy(
            src_ref=src, dst_ref=dst, send_sem=sp_send.at[phase], recv_sem=sp_recv.at[phase * parts + part_of],
            device_id=(d, tp), device_id_type=MESH)

    def from_all(ref, phase):
        landed(ref.at[: n_tp - 1], tp_recv.at[phase])

    def tp_drain(phase, ref):
        drains.append(lambda: landed(ref, tp_send.at[phase]))

    @pl.loop(1, n_tp + 1)
    def _(k):
        g = after_tp(k)
        strip = pl.ds(pl.multiple_of(g * LANES, LANES), LANES)
        part[g] = dot(att, oab[:, strip]).astype(BF)

        @pl.when(k < n_tp)
        def _():
            tp_copy(0, g, part.at[g], rs.at[tp]).start()

    tp_drain(0, part.at[: n_tp - 1])

    def added_up(ref):
        total = ref[0].astype(F32)
        for g in range(1, n_tp):
            total = total + ref[g].astype(F32)
        return total

    rs[tp] = part[tp]
    from_all(rs, 0)
    mixed = added_up(rs)

    gained = mixed * mg[...]
    x = resid[...].astype(F32)
    lane = lax.broadcasted_iota(jnp.int32, (rows, LANES), 1)
    own = jnp.zeros((rows, LANES), F32)
    for k, product in enumerate((mixed * mixed, x * x, x * gained, gained * gained)):
        own = jnp.where(lane == k, jnp.sum(product, axis=1, keepdims=True), own)
    lines = jnp.transpose(jnp.concatenate([own, jnp.zeros((wide - rows, LANES), F32)], axis=0))[0:8, :]
    sts[...] = lines

    @pl.loop(1, n_tp)
    def _(k):
        tp_copy(1, after_tp(k), sts.at[:4], st.at[tp, :4]).start()

    tp_drain(1, st.at[: n_tp - 1, :4])

    st[tp] = lines
    landed(st.at[: n_tp - 1, :4], tp_recv.at[1])
    lines = added_up(st)
    total = jnp.transpose(jnp.concatenate([lines, jnp.zeros((LANES - 8, wide), F32)], axis=0))[:rows, :]
    scale = lax.rsqrt(total[:, 0:1] / D + EPS)
    square = total[:, 1:2] + scale * (2.0 * total[:, 2:3] + scale * total[:, 3:4])
    stream = (x + gained * scale).astype(BF).astype(F32)
    scale = lax.rsqrt(jnp.maximum(square, 0.0) / D + EPS)
    normed = (stream * scale * fg[...]).astype(BF)

    tall = jnp.concatenate([normed, jnp.zeros((wide - rows, LANES), BF)], axis=0)
    dsp_out[...] = dot(choose[...], tall).reshape(n_sp, PADDED, LANES).astype(BF)

    def far_first(body):
        @pl.loop(0, nz)
        def _(turn):
            k = nz - 1 - turn
            reach = (k + 1) // 2
            away = (z + nz + reach * (2 * (k % 2) - 1)) % nz
            body(2 * away + 1 - c)

            @pl.when(k > 0)
            def _():
                body(2 * away + c)

    def berth(src, dst):
        return 2 * ((src // 2 + nz + nz // 4 - dst // 2) % nz) + src % 2

    def tenant(place):
        return 2 * ((z + nz - nz // 4 + place // 2) % nz) + place % 2

    def dispatch(d):
        return sp_copy(0, d, dsp_out.at[d, :filled], dsp_in.at[berth(sp, d), :filled], berth(sp, d) // homes)

    far_first(lambda d: dispatch(d).start())
    drains.append(lambda: landed(dsp_out.at[: n_sp - 1, :filled], sp_send.at[0]))
    dsp_in[berth(sp, sp)] = dsp_out[sp]

    shp[:, :, :units] = dot(normed, sg[...]).reshape(strips, 16, units).astype(BF)
    shp[:, :, units:] = dot(normed, su[...]).reshape(strips, 16, units).astype(BF)

    @pl.loop(1, n_tp)
    def _(k):
        g = after_tp(k)

        @pl.when(g < strips)
        def _():
            tp_copy(2, g, shp.at[g], shr.at[tp]).start()

    @drains.append
    def _():
        @pl.when(tp < strips)
        def _():
            landed(shp.at[: strips - 1], tp_send.at[2])
            landed(shr.at[: n_tp - 1, :, :units], tp_send.at[3])

        @pl.when(tp >= strips)
        def _():
            landed(shp, tp_send.at[2])

    def gated(gate, up):
        return (gate / (1.0 + jnp.exp(-gate)) * up).astype(BF)

    def reduce_shared():
        @pl.when(tp < strips)
        def _():
            shr[tp] = shp[tp]
            from_all(shr, 2)
            both = added_up(shr)
            hidden = gated(both[:, :units], both[:, units:])
            shs[...] = hidden
            shh[tp] = hidden

            @pl.loop(1, n_tp)
            def _(k):
                tp_copy(3, after_tp(k), shs, shh.at[tp]).start()

    def send_rows(p):
        first_one = p * homes if p else 1
        landed(dsp_in.at[first_one : (p + 1) * homes, :filled], sp_recv.at[p])
        flat = dsp_in[p * homes : (p + 1) * homes].astype(F32).reshape(part_seats, LANES).astype(BF)
        xbuf[p] = dot(smat[...], flat).reshape(local, part_used, LANES).astype(BF)
        xin[p, tp] = xbuf[p, tp // quarters]

        @pl.loop(1, n_tp)
        def _(k):
            g = after_tp(k)
            tp_copy(4 + p, g, xbuf.at[p, g // quarters], xin.at[p, tp]).start()

        tp_drain(4 + p, xin.at[p, : n_tp - 1])

    def send_hidden(p):
        from_all(xin.at[p], 4 + p)
        x = jnp.concatenate([xin[p, g] for g in range(n_tp)], axis=1)
        both = dot(x, wgu[...].reshape(n_tp * LANES, 2 * LANES))
        hidden = gated(both[:, :LANES], both[:, LANES:])
        hs[p] = hidden
        hin[p, tp] = hidden

        @pl.loop(1, n_tp)
        def _(k):
            tp_copy(4 + parts + p, after_tp(k), hs.at[p], hin.at[p, tp]).start()

        tp_drain(4 + parts + p, hin.at[p, : n_tp - 1])

    def giving(place):
        d = tenant(place)
        return sp_copy(1, d, ret_out.at[place, :filled], ret_in.at[sp, :filled])

    def send_back(p):
        from_all(hin.at[p], 4 + parts + p)
        for e in range(local):
            h = jnp.concatenate([hin[p, quarters * e + q] for q in range(quarters)], axis=1)
            obuf[e * part_used : (e + 1) * part_used, :] = dot(h, ed[e]).astype(BF)
        made = dot(rmat[...], obuf[...]).reshape(homes, PADDED, LANES).astype(BF)
        ret_out[p * homes : (p + 1) * homes] = made

        @pl.loop(p * homes, (p + 1) * homes)
        def _(place):
            @pl.when(tenant(place) != sp)
            def _():
                giving(place).start()

    drains.append(lambda: landed(ret_out.at[: n_sp - 1, :filled], sp_send.at[1]))

    send_rows(parts - 1)
    reduce_shared()
    for h in range(2):
        src, dst = weights_copy(h, tp)
        pltpu.make_async_copy(src, dst, wloc.at[h]).wait()

    landed(wgu.at[: n_tp - 1], wrecv.at[0])
    for p in reversed(range(parts - 1)):
        send_rows(p)
        send_hidden(p + 1)
    send_hidden(0)
    for p in reversed(range(parts)):
        send_back(p)
    ret_in[sp] = ret_out[berth(sp, sp)]
    weights = [column(gates, k) for k in range(2)]

    @pl.when(tp < strips)
    def _():
        landed(shh.at[: strips - 1], tp_recv.at[3])

    @pl.when(tp >= strips)
    def _():
        landed(shh, tp_recv.at[3])

    shared_out = dot(shh[...].reshape(rows, units), sd[...])

    landed(ret_in.at[: n_sp - 1, :filled], sp_recv.at[parts])
    flat = ret_in[...].astype(F32).reshape(seats, LANES).astype(BF)
    routed = weights[0] * dot(oh[0], flat) + weights[1] * dot(oh[1], flat)
    out[...] = (stream + (routed + shared_out)).astype(BF)
    for drain in drains:
        drain()


def shards(query_a, key_a, value_a, query_b, key_b, value_b, stop_a, stop_b, out_a, out_b, resid, mix_gain, ffn_gain,
           routes, gates, exp_gate, exp_up, exp_down, sh_gate, sh_up, sh_down):
    n_sp, n_tp = lax.axis_size("sp"), lax.axis_size("tp")
    rows = resid.shape[0]
    local, _, units = exp_gate.shape
    used = n_sp * CAP
    strips = rows // 16
    seats = n_sp * PADDED
    parts = 2
    nz = n_sp // 2
    up_steps = nz // 2
    down_steps = nz - up_steps
    operands = (
        query_a, key_a, value_a, query_b, key_b, value_b, stop_a.T, stop_b.T, out_a, out_b, resid,
        mix_gain.reshape(1, -1), ffn_gain.reshape(1, -1), routes.T, gates.T, exp_gate, exp_up, exp_down, sh_gate,
        sh_up, sh_down)
    dma = pltpu.SemaphoreType.DMA
    vmem = pltpu.VMEM
    held = [vmem(a.shape, a.dtype) for i, a in enumerate(operands) if i not in (9, 15, 16)]
    held[8] = vmem((2 * out_a.shape[0], out_a.shape[1]), BF)
    return pl.pallas_call(
        functools.partial(layer_kernel, n_sp, n_tp),
        out_shape=jax.ShapeDtypeStruct((rows, LANES), BF),
        in_specs=[pl.BlockSpec(memory_space=pl.ANY)] * len(operands),
        out_specs=pl.BlockSpec(memory_space=pltpu.VMEM),
        scratch_shapes=held + [
            vmem((nz, 4, 2 * rows, LANES), BF),
            vmem((rows, 2 * LANES), F32),
            vmem((rows, 2 * LANES), F32),
            vmem((rows, 2 * LANES), F32),
            vmem((2 * rows, 2 * rows), BF),
            vmem((n_tp, rows, LANES), BF),
            vmem((n_tp, rows, LANES), BF),
            vmem((8, 2 * LANES), F32),
            vmem((n_tp, 8, 2 * LANES), F32),
            vmem((n_sp, PADDED, LANES), BF),
            vmem((n_sp, PADDED, LANES), BF),
            vmem((n_sp, PADDED, LANES), BF),
            vmem((n_sp, PADDED, LANES), BF),
            vmem((strips, 16, 2 * units), BF),
            vmem((n_tp, 16, 2 * units), BF),
            vmem((16, units), BF),
            vmem((strips, 16, units), BF),
            vmem((parts, local, used // parts, LANES), BF),
            vmem((parts, n_tp, used // parts, LANES), BF),
            vmem((n_tp, LANES, 2 * LANES), BF),
            vmem((parts, used // parts, LANES), BF),
            vmem((parts, n_tp, used // parts, LANES), BF),
            vmem((local * used // parts, LANES), BF),
            vmem((2, rows, seats), BF),
            vmem((seats, 2 * LANES), BF),
            vmem((local * used // parts, seats // parts), BF),
            vmem((seats // parts, local * used // parts), BF),
            dma((len(held) + 1,)),
            pltpu.SemaphoreType.REGULAR(((nz // 4).bit_length() + 1,)),
            dma((up_steps, 2)),
            dma((up_steps, 4)),
            dma((down_steps, 2)),
            dma((down_steps, 4)),
            dma((nz + 1, 2)),
            dma((nz + 1, 2)),
            dma((1,)),
            dma((1,)),
            dma((2,)),
            dma((4 + 2 * parts,)),
            dma((4 + 2 * parts,)),
            dma((2,)),
            dma((parts + 1,)),
        ],
        compiler_params=pltpu.CompilerParams(
            collective_id=0, has_side_effects=True, vmem_limit_bytes=56 * 1024 * 1024),
    )(*operands)


def solution(mesh):
    row, col, both = P("tp", None), P("tp"), P("sp", "tp")
    in_specs = (both,) * 8 + (
        row, row, both, col, col, P("sp", None), P("sp", None),
        P("sp", "tp", None), P("sp", "tp", None), P("sp", None, "tp"), row, row, P(None, "tp"))
    return jax.shard_map(shards, mesh=mesh, in_specs=in_specs, out_specs=both, check_vma=False)
```

```python
import functools

import jax
import jax.numpy as jnp
from jax import lax
from jax.experimental import pallas as pl
from jax.experimental.pallas import tpu as pltpu
from jax.sharding import PartitionSpec as P

D = 2048
EPS = 1e-06
MESH = pl.DeviceIdType.MESH
BF = jnp.bfloat16
F32 = jnp.float32
LANES = 128
CAP = 5
PADDED = 24


def dot(a, b):
    return jnp.dot(a, b, preferred_element_type=F32)


def softplus_block(query, keys, stop, scale, later, valid):
    scores = lax.dot_general(query, keys, (((1,), (1,)), ((), ())), preferred_element_type=F32)
    z = scores * scale + stop
    sp = jnp.maximum(z, 0.0) + jnp.log(1.0 + jnp.exp(-jnp.abs(z)))
    if valid is not None:
        sp = jnp.where(valid, sp, 0.0)
    after = dot(sp.astype(BF), later)
    weight = jnp.exp(z - sp - after)
    if valid is not None:
        weight = jnp.where(valid, weight, 0.0)
    return weight.astype(BF), jnp.sum(sp, axis=1, keepdims=True)


def layer_kernel(n_sp, n_tp, *refs):
    (qa_h, ka_h, va_h, qb_h, kb_h, vb_h, sa_h, sb_h, oa_h, ob_h, resid_h, mg_h, fg_h, routes_h, gates_h,
     eg, eu, ed_h, sg_h, su_h, sd_h, out,
     qa, ka, va, qb, kb, vb, sa, sb, oab, resid, mg, fg, routes, gates, ed, sg, su, sd,
     buf, accn, accf, ln, later,
     part, rs, sts, st, dsp_out, dsp_in, ret_out, ret_in, shp, shr, shs, shh, xbuf, xin, wgu, hs, hin, obuf, oh,
     choose, smat, rmat,
     lsem, tokens, ssu, rsu, ssd, rsd, ssp, rsp, wsend, wrecv, wloc, tp_send, tp_recv, sp_send, sp_recv) = refs
    rows = resid.shape[0]
    local, units = ed.shape[0], ed.shape[1]
    quarters = n_tp // local
    used = n_sp * CAP
    seats = n_sp * PADDED
    parts = 2
    filled = local * CAP
    part_used = used // parts
    part_seats = seats // parts
    homes = n_sp // parts
    strips = rows // 16
    wide = 2 * LANES
    nz = n_sp // 2
    up_steps = nz // 2
    down_steps = nz - up_steps
    ups = (up_steps, up_steps, nz - 1 - down_steps, nz - 1 - down_steps)
    downs = tuple(nz - 1 - n for n in ups)
    sp = lax.axis_index("sp")
    tp = lax.axis_index("tp")
    z = sp // 2
    c = sp % 2
    up_id = (2 * ((z + 1) % nz) + c, tp)
    down_id = (2 * ((z + nz - 1) % nz) + c, tp)
    pair_id = (2 * z + 1 - c, tp)
    drains = []

    dsp_in[...] = jnp.zeros_like(dsp_in)
    ret_in[...] = jnp.zeros_like(ret_in)
    st[...] = jnp.zeros_like(st)
    barrier = pltpu.get_barrier_semaphore()

    side = quarters
    row = [(sp, tp // side * side + (tp + k) % side) for k in range(1, side)]
    column_peers = [(sp, (tp + side * k) % n_tp) for k in range(1, n_tp // side)]
    across = [(2 * ((z + step) % nz) + 1 - c, tp) for step in (1, nz - 1)]
    first = [up_id, down_id, pair_id] + across + row + column_peers
    for peer in first:
        pl.semaphore_signal(barrier, inc=1, device_id=peer, device_id_type=MESH)

    def pass_on(which, peers):
        for peer in peers:
            pl.semaphore_signal(tokens.at[which], inc=1, device_id=peer, device_id_type=MESH)

    def along(distance):
        return [(2 * ((z + step) % nz) + c, tp) for step in (distance, nz - distance)]

    rounds = [1 << r for r in range((nz // 4).bit_length())]

    staged = [
        (ka_h, ka), (va_h, va), (kb_h, kb), (vb_h, vb), (routes_h, routes), (qa_h, qa), (qb_h, qb), (sa_h, sa),
        (sb_h, sb), (oa_h, oab.at[:LANES]), (ob_h, oab.at[LANES:]), (resid_h, resid), (mg_h, mg), (fg_h, fg), (gates_h, gates),
        (ed_h, ed), (sg_h, sg), (su_h, su), (sd_h, sd)]
    loads = [pltpu.make_async_copy(a, b, lsem.at[i]) for i, (a, b) in enumerate(staged)]
    for load in loads:
        load.start()

    def column(ref, k):
        return jnp.transpose(jnp.broadcast_to(ref[k : k + 1, :].astype(F32), (LANES, rows)))

    for load in loads[:4]:
        load.wait()
    pl.semaphore_wait(barrier, len(first))
    pass_on(0, row)
    pass_on(1, along(rounds[0]))

    mine = pl.ds(pl.multiple_of(c * rows, rows), rows)
    theirs = pl.ds(pl.multiple_of((1 - c) * rows, rows), rows)
    srcs = (ka, va, kb, vb)

    def place(block, a):
        return buf.at[block, a, mine, :]

    def twin(block, g, half):
        return buf.at[block, 2 * g : 2 * g + 2, half, :]

    def up_copy(step, a, src):
        return pltpu.make_async_remote_copy(
            src_ref=src, dst_ref=place(z + 1 - step, a), send_sem=ssu.at[step - 1, a // 2], recv_sem=rsu.at[step - 1, a],
            device_id=up_id, device_id_type=MESH)

    def down_copy(step, a, src):
        return pltpu.make_async_remote_copy(
            src_ref=src, dst_ref=place((z + step - 1) % nz, a), send_sem=ssd.at[step - 1, a // 2],
            recv_sem=rsd.at[step - 1, a], device_id=down_id, device_id_type=MESH)

    def pair_copy(index, block, a, src):
        return pltpu.make_async_remote_copy(
            src_ref=src, dst_ref=place(block, a), send_sem=ssp.at[index, a // 2], recv_sem=rsp.at[index, a // 2],
            device_id=pair_id, device_id_type=MESH)

    def landed(ref, sem):
        pltpu.make_async_copy(ref, ref, sem).wait()

    def sends_up(step, a):
        return (z < nz - 1) & (z + 1 - step >= 0) & (step <= ups[a])

    def sends_down(step, a):
        return ((z + step - 1) % nz <= downs[a] - 1) & (step <= downs[a])

    def gets_up(step, a):
        return (z - step >= 0) & (step <= ups[a])

    def gets_down(step, a):
        return ((z + step) % nz <= downs[a] - 1) & (step <= downs[a])

    def far(step, a):
        return (z + step >= nz) & (step <= downs[a])

    for a in range(4):
        @pl.when(sends_up(1, a))
        def _(a=a):
            up_copy(1, a, srcs[a]).start()

        @pl.when(sends_down(1, a))
        def _(a=a):
            down_copy(1, a, srcs[a]).start()

        pair_copy(0, z, a, srcs[a]).start()
        buf[z, a, mine, :] = srcs[a][...]

    def after_tp(k):
        return (tp + k) % n_tp

    def weights_copy(h, g):
        src = (eg, eu)[h].at[g // quarters, :, pl.ds(pl.multiple_of((g % quarters) * LANES, LANES), LANES)]
        dst = wgu.at[tp, :, pl.ds(h * LANES, LANES)]
        return src, dst

    def weights_remote(h, g):
        src, dst = weights_copy(h, g)
        return pltpu.make_async_remote_copy(
            src_ref=src, dst_ref=dst, send_sem=wsend.at[0], recv_sem=wrecv.at[0],
            device_id=(sp, g), device_id_type=MESH)

    span = 2 * rows
    j = lax.broadcasted_iota(jnp.int32, (span, span), 0)
    s = lax.broadcasted_iota(jnp.int32, (span, span), 1)
    later[...] = (j > s).astype(BF)
    accf[...] = jnp.zeros_like(accf)
    half = lax.broadcasted_iota(jnp.int32, (rows, LANES), 1) < LANES // 2

    def index_of(shape, dim):
        return lax.broadcasted_iota(jnp.int32, shape, dim).astype(F32)

    def exchange_weights():
        pl.semaphore_wait(tokens.at[0], len(row))

        @pl.loop(1, n_tp)
        def _(k):
            for h in range(2):
                weights_remote(h, after_tp(k)).start()

        for h in range(2):
            src, dst = weights_copy(h, tp)
            pltpu.make_async_copy(src, dst, wloc.at[h]).start()

    def seat_masks():
        i = index_of((local * part_used, LANES), 0)
        e = jnp.floor((i + 0.5) * (1.0 / part_used))
        i = i - part_used * e
        g = jnp.floor((i + 0.5) * (1.0 / CAP))
        seat = g * PADDED + e * CAP + (i - CAP * g)
        smat[...] = (index_of((local * part_used, part_seats), 1) == seat[:, 0:1]).astype(BF)
        i = index_of((part_seats, LANES), 0)
        g = jnp.floor((i + 0.5) * (1.0 / PADDED))
        i = i - PADDED * g
        e = jnp.floor((i + 0.5) * (1.0 / CAP))
        seat = jnp.where(e < local, e * part_used + g * CAP + (i - CAP * e), -1.0)
        rmat[...] = (index_of((part_seats, local * part_used), 1) == seat[:, 0:1]).astype(BF)

    def seat_rows():
        loads[4].wait()
        experts = local * n_sp
        e_at = index_of((rows, experts), 1)
        named_by = [column(routes, k) for k in range(2)]
        named = [e_at == named_by[k][:, 0:1] for k in range(2)]
        members = jnp.where(named[0] | named[1], 1.0, 0.0).astype(BF)
        prior = dot((index_of((rows, rows), 1) < index_of((rows, rows), 0)).astype(BF), members)
        hits = None
        for k in range(2):
            home = jnp.floor((named_by[k] + 0.5) * (1.0 / local))
            rank = jnp.sum(jnp.where(named[k], prior, 0.0), axis=1, keepdims=True)
            seat = home * PADDED + (named_by[k] - local * home) * CAP + rank
            oh[k] = (index_of((rows, seats), 1) == seat[:, 0:1]).astype(BF)
            tall = jnp.concatenate([seat, jnp.full((wide - rows, LANES), -1.0, F32)], axis=0)
            hit = index_of((seats, wide), 0) == jnp.transpose(tall)[0:1, :]
            hits = hit if hits is None else hits | hit
        choose[...] = hits.astype(BF)

    for load in loads[5:9]:
        load.wait()
    pl.semaphore_wait(tokens.at[1], 2)
    pass_on(2, along(rounds[1]))
    qa_all = qa[...]
    zero = jnp.zeros_like(qa_all)
    qa_heads = (jnp.where(half, qa_all, zero), jnp.where(half, zero, qa_all))
    stops = [column(sa, 0)[:, 0:1], column(sa, 1)[:, 0:1], column(sb, 0)[:, 0:1]]

    def group_a(block, valid=None):
        keys = buf[block, 0]
        values = buf[block, 1]
        pieces = [softplus_block(qa_heads[h], keys, stops[h], 64 ** -0.5, later[...], valid) for h in range(2)]
        added = jnp.where(half, dot(pieces[0][0], values), dot(pieces[1][0], values))
        return added, jnp.where(half, pieces[0][1], pieces[1][1])

    def group_b(block, valid=None):
        weight, total = softplus_block(qb[...], buf[block, 2], stops[2], 128 ** -0.5, later[...], valid)
        return dot(weight, buf[block, 3]), jnp.broadcast_to(total, (rows, LANES))

    groups = (group_a, group_b)

    def cols(g):
        return slice(g * LANES, (g + 1) * LANES)

    def near(g, step):
        block = z - step
        landed(twin(block, g, theirs), rsp.at[step, g])
        added, total = groups[g](block)
        accn[:, cols(g)] += jnp.exp(-ln[:, cols(g)]) * added
        ln[:, cols(g)] += total

    def distant(g, step):
        block = z + step - nz
        landed(twin(block, g, theirs), rsp.at[up_steps + step, g])
        added, total = groups[g](block)
        accf[:, cols(g)] = jnp.exp(-total) * accf[:, cols(g)] + added

    def poll_up(step, a):
        @pl.when(gets_up(step, a))
        def _():
            ref = place(z - step, a)
            landed(ref, rsu.at[step - 1, a])

            @pl.when((step < ups[a]) & (z < nz - 1))
            def _():
                up_copy(step + 1, a, ref).start()

            pair_copy(step, z - step, a, ref).start()

    def poll_down(step, a):
        @pl.when(gets_down(step, a))
        def _():
            block = (z + step) % nz
            ref = place(block, a)
            landed(ref, rsd.at[step - 1, a])

            @pl.when(step < downs[a])
            def _():
                down_copy(step + 1, a, ref).start()

            @pl.when(far(step, a))
            def _():
                pair_copy(up_steps + step, block, a, ref).start()

    row_at = lax.broadcasted_iota(jnp.int32, (rows, span), 0) + c * rows
    key_at = lax.broadcasted_iota(jnp.int32, (rows, span), 1)
    valid = key_at < row_at
    for g in range(2):
        landed(twin(z, g, theirs), rsp.at[0, g])
        added, total = groups[g](z, valid)
        accn[:, cols(g)] = added
        ln[:, cols(g)] = total
        for a in (2 * g, 2 * g + 1):
            poll_up(1, a)
            poll_down(1, a)

    for r in range(2, len(rounds)):
        pl.semaphore_wait(tokens.at[r], 2)
        pass_on(r + 1, along(rounds[r]))

    @pl.loop(2, up_steps + 1)
    def _(step):
        before = step - 1
        for when, piece in ((2, exchange_weights), (3, seat_rows), (4, seat_masks)):
            pl.when(step == when)(piece)
        for a in range(4):
            poll_up(step, a)
            poll_down(step, a)
            g = a // 2
            if a % 2 == 0:
                @pl.when(gets_up(before, a))
                def _():
                    near(g, before)
            else:
                @pl.when(far(before, a))
                def _():
                    distant(g, before)

    @pl.when(gets_up(up_steps, 0))
    def _():
        near(0, up_steps)

    @pl.when(far(down_steps, 2))
    def _():
        distant(1, down_steps)

    for load in loads[9:]:
        load.wait()

    pl.semaphore_wait(tokens.at[len(rounds)], 2)
    att = (accn[...] + jnp.exp(-ln[...]) * accf[...]).astype(BF)

    @drains.append
    def _():
        for g in range(2):
            landed(twin(z, g, mine), ssp.at[0, g])

        @pl.loop(1, up_steps + 1)
        def _(step):
            for g in range(2):
                @pl.when(sends_up(step, 2 * g))
                def _():
                    landed(twin(z + 1 - step, g, mine), ssu.at[step - 1, g])

                @pl.when(gets_up(step, 2 * g))
                def _():
                    landed(twin(z - step, g, mine), ssp.at[step, g])

        @pl.loop(1, down_steps + 1)
        def _(step):
            for g in range(2):
                @pl.when(sends_down(step, 2 * g))
                def _():
                    landed(twin((z + step - 1) % nz, g, mine), ssd.at[step - 1, g])

                @pl.when(far(step, 2 * g))
                def _():
                    landed(twin(z + step - nz, g, mine), ssp.at[up_steps + step, g])

        landed(wgu.at[: n_tp - 1], wsend.at[0])

    def tp_copy(phase, g, src, dst):
        return pltpu.make_async_remote_copy(
            src_ref=src, dst_ref=dst, send_sem=tp_send.at[phase], recv_sem=tp_recv.at[phase],
            device_id=(sp, g), device_id_type=MESH)

    def sp_copy(phase, d, src, dst, part_of=0):
        return pltpu.make_async_remote_copy(
            src_ref=src, dst_ref=dst, send_sem=sp_send.at[phase], recv_sem=sp_recv.at[phase * parts + part_of],
            device_id=(d, tp), device_id_type=MESH)

    def from_all(ref, phase):
        landed(ref.at[: n_tp - 1], tp_recv.at[phase])

    def tp_drain(phase, ref):
        drains.append(lambda: landed(ref, tp_send.at[phase]))

    def hops(offset):
        return sum(min(n, side - n) for n in divmod(offset, side))

    offsets = sorted(range(1, n_tp), key=hops, reverse=True)
    owners = [(tp // side + o // side) % side * side + (tp + o) % side for o in offsets]

    def project(g):
        strip = pl.ds(pl.multiple_of(g * LANES, LANES), LANES)
        return dot(att, oab[:, strip]).astype(BF)

    for g in owners:
        part[g] = project(g)
        tp_copy(0, g, part.at[g], rs.at[tp]).start()

    tp_drain(0, part.at[: n_tp - 1])

    def added_up(ref):
        total = ref[0].astype(F32)
        for g in range(1, n_tp):
            total = total + ref[g].astype(F32)
        return total

    rs[tp] = project(tp)
    from_all(rs, 0)
    mixed = added_up(rs)

    gained = mixed * mg[...]
    x = resid[...].astype(F32)
    lane = lax.broadcasted_iota(jnp.int32, (rows, LANES), 1)
    own = jnp.zeros((rows, LANES), F32)
    for k, product in enumerate((mixed * mixed, x * x, x * gained, gained * gained)):
        own = jnp.where(lane == k, jnp.sum(product, axis=1, keepdims=True), own)
    lines = jnp.transpose(jnp.concatenate([own, jnp.zeros((wide - rows, LANES), F32)], axis=0))[0:8, :]
    sts[...] = lines

    for g in owners:
        tp_copy(1, g, sts.at[:4], st.at[tp, :4]).start()

    tp_drain(1, st.at[: n_tp - 1, :4])

    st[tp] = lines
    landed(st.at[: n_tp - 1, :4], tp_recv.at[1])
    lines = added_up(st)
    total = jnp.transpose(jnp.concatenate([lines, jnp.zeros((LANES - 8, wide), F32)], axis=0))[:rows, :]
    scale = lax.rsqrt(total[:, 0:1] / D + EPS)
    square = total[:, 1:2] + scale * (2.0 * total[:, 2:3] + scale * total[:, 3:4])
    stream = (x + gained * scale).astype(BF).astype(F32)
    scale = lax.rsqrt(jnp.maximum(square, 0.0) / D + EPS)
    normed = (stream * scale * fg[...]).astype(BF)

    tall = jnp.concatenate([normed, jnp.zeros((wide - rows, LANES), BF)], axis=0)
    dsp_out[...] = dot(choose[...], tall).reshape(n_sp, PADDED, LANES).astype(BF)

    def far_first(body):
        @pl.loop(0, nz)
        def _(turn):
            k = nz - 1 - turn
            reach = (k + 1) // 2
            away = (z + nz + reach * (2 * (k % 2) - 1)) % nz
            body(2 * away + 1 - c)

            @pl.when(k > 0)
            def _():
                body(2 * away + c)

    def berth(src, dst):
        return 2 * ((src // 2 + nz + nz // 4 - dst // 2) % nz) + src % 2

    def tenant(place):
        return 2 * ((z + nz - nz // 4 + place // 2) % nz) + place % 2

    def dispatch(d):
        return sp_copy(0, d, dsp_out.at[d, :filled], dsp_in.at[berth(sp, d), :filled], berth(sp, d) // homes)

    far_first(lambda d: dispatch(d).start())
    drains.append(lambda: landed(dsp_out.at[: n_sp - 1, :filled], sp_send.at[0]))
    dsp_in[berth(sp, sp)] = dsp_out[sp]

    shp[:, :, :units] = dot(normed, sg[...]).reshape(strips, 16, units).astype(BF)
    shp[:, :, units:] = dot(normed, su[...]).reshape(strips, 16, units).astype(BF)

    for g in owners:
        @pl.when(g < strips)
        def _(g=g):
            tp_copy(2, g, shp.at[g], shr.at[tp]).start()

    @drains.append
    def _():
        @pl.when(tp < strips)
        def _():
            landed(shp.at[: strips - 1], tp_send.at[2])
            landed(shr.at[: n_tp - 1, :, :units], tp_send.at[3])

        @pl.when(tp >= strips)
        def _():
            landed(shp, tp_send.at[2])

    def gated(gate, up):
        return (gate / (1.0 + jnp.exp(-gate)) * up).astype(BF)

    def reduce_shared():
        @pl.when(tp < strips)
        def _():
            shr[tp] = shp[tp]
            from_all(shr, 2)
            both = added_up(shr)
            hidden = gated(both[:, :units], both[:, units:])
            shs[...] = hidden
            shh[tp] = hidden

            for g in owners:
                tp_copy(3, g, shs, shh.at[tp]).start()

    def send_rows(p):
        first_one = p * homes if p else 1
        landed(dsp_in.at[first_one : (p + 1) * homes, :filled], sp_recv.at[p])
        flat = dsp_in[p * homes : (p + 1) * homes].astype(F32).reshape(part_seats, LANES).astype(BF)
        xbuf[p] = dot(smat[...], flat).reshape(local, part_used, LANES).astype(BF)
        xin[p, tp] = xbuf[p, tp // quarters]

        for g in owners:
            tp_copy(4 + p, g, xbuf.at[p, g // quarters], xin.at[p, tp]).start()

        tp_drain(4 + p, xin.at[p, : n_tp - 1])

    def send_hidden(p):
        from_all(xin.at[p], 4 + p)
        x = jnp.concatenate([xin[p, g] for g in range(n_tp)], axis=1)
        both = dot(x, wgu[...].reshape(n_tp * LANES, 2 * LANES))
        hidden = gated(both[:, :LANES], both[:, LANES:])
        hs[p] = hidden
        hin[p, tp] = hidden

        for g in owners:
            tp_copy(4 + parts + p, g, hs.at[p], hin.at[p, tp]).start()

        tp_drain(4 + parts + p, hin.at[p, : n_tp - 1])

    def giving(place):
        d = tenant(place)
        return sp_copy(1, d, ret_out.at[place, :filled], ret_in.at[sp, :filled])

    def send_back(p):
        from_all(hin.at[p], 4 + parts + p)
        for e in range(local):
            h = jnp.concatenate([hin[p, quarters * e + q] for q in range(quarters)], axis=1)
            obuf[e * part_used : (e + 1) * part_used, :] = dot(h, ed[e]).astype(BF)
        made = dot(rmat[...], obuf[...]).reshape(homes, PADDED, LANES).astype(BF)
        ret_out[p * homes : (p + 1) * homes] = made

        @pl.loop(p * homes, (p + 1) * homes)
        def _(place):
            @pl.when(tenant(place) != sp)
            def _():
                giving(place).start()

    drains.append(lambda: landed(ret_out.at[: n_sp - 1, :filled], sp_send.at[1]))

    send_rows(parts - 1)
    for h in range(2):
        src, dst = weights_copy(h, tp)
        pltpu.make_async_copy(src, dst, wloc.at[h]).wait()

    landed(wgu.at[: n_tp - 1], wrecv.at[0])
    for p in reversed(range(parts - 1)):
        send_rows(p)
        send_hidden(p + 1)
    reduce_shared()
    send_hidden(0)
    for p in reversed(range(parts)):
        send_back(p)
    ret_in[sp] = ret_out[berth(sp, sp)]
    weights = [column(gates, k) for k in range(2)]

    @pl.when(tp < strips)
    def _():
        landed(shh.at[: strips - 1], tp_recv.at[3])

    @pl.when(tp >= strips)
    def _():
        landed(shh, tp_recv.at[3])

    shared_out = dot(shh[...].reshape(rows, units), sd[...])

    landed(ret_in.at[: n_sp - 1, :filled], sp_recv.at[parts])
    flat = ret_in[...].astype(F32).reshape(seats, LANES).astype(BF)
    routed = weights[0] * dot(oh[0], flat) + weights[1] * dot(oh[1], flat)
    out[...] = (stream + (routed + shared_out)).astype(BF)
    for drain in drains:
        drain()


def shards(query_a, key_a, value_a, query_b, key_b, value_b, stop_a, stop_b, out_a, out_b, resid, mix_gain, ffn_gain,
           routes, gates, exp_gate, exp_up, exp_down, sh_gate, sh_up, sh_down):
    n_sp, n_tp = lax.axis_size("sp"), lax.axis_size("tp")
    rows = resid.shape[0]
    local, _, units = exp_gate.shape
    used = n_sp * CAP
    strips = rows // 16
    seats = n_sp * PADDED
    parts = 2
    nz = n_sp // 2
    up_steps = nz // 2
    down_steps = nz - up_steps
    operands = (
        query_a, key_a, value_a, query_b, key_b, value_b, stop_a.T, stop_b.T, out_a, out_b, resid,
        mix_gain.reshape(1, -1), ffn_gain.reshape(1, -1), routes.T, gates.T, exp_gate, exp_up, exp_down, sh_gate,
        sh_up, sh_down)
    dma = pltpu.SemaphoreType.DMA
    vmem = pltpu.VMEM
    held = [vmem(a.shape, a.dtype) for i, a in enumerate(operands) if i not in (9, 15, 16)]
    held[8] = vmem((2 * out_a.shape[0], out_a.shape[1]), BF)
    return pl.pallas_call(
        functools.partial(layer_kernel, n_sp, n_tp),
        out_shape=pltpu.VMEM((rows, LANES), BF),
        in_specs=[pl.BlockSpec(memory_space=pl.ANY)] * len(operands),
        out_specs=pl.BlockSpec(memory_space=pltpu.VMEM),
        scratch_shapes=held + [
            vmem((nz, 4, 2 * rows, LANES), BF),
            vmem((rows, 2 * LANES), F32),
            vmem((rows, 2 * LANES), F32),
            vmem((rows, 2 * LANES), F32),
            vmem((2 * rows, 2 * rows), BF),
            vmem((n_tp, rows, LANES), BF),
            vmem((n_tp, rows, LANES), BF),
            vmem((8, 2 * LANES), F32),
            vmem((n_tp, 8, 2 * LANES), F32),
            vmem((n_sp, PADDED, LANES), BF),
            vmem((n_sp, PADDED, LANES), BF),
            vmem((n_sp, PADDED, LANES), BF),
            vmem((n_sp, PADDED, LANES), BF),
            vmem((strips, 16, 2 * units), BF),
            vmem((n_tp, 16, 2 * units), BF),
            vmem((16, units), BF),
            vmem((strips, 16, units), BF),
            vmem((parts, local, used // parts, LANES), BF),
            vmem((parts, n_tp, used // parts, LANES), BF),
            vmem((n_tp, LANES, 2 * LANES), BF),
            vmem((parts, used // parts, LANES), BF),
            vmem((parts, n_tp, used // parts, LANES), BF),
            vmem((local * used // parts, LANES), BF),
            vmem((2, rows, seats), BF),
            vmem((seats, 2 * LANES), BF),
            vmem((local * used // parts, seats // parts), BF),
            vmem((seats // parts, local * used // parts), BF),
            dma((len(held) + 1,)),
            pltpu.SemaphoreType.REGULAR(((nz // 4).bit_length() + 1,)),
            dma((up_steps, 2)),
            dma((up_steps, 4)),
            dma((down_steps, 2)),
            dma((down_steps, 4)),
            dma((nz + 1, 2)),
            dma((nz + 1, 2)),
            dma((1,)),
            dma((1,)),
            dma((2,)),
            dma((4 + 2 * parts,)),
            dma((4 + 2 * parts,)),
            dma((2,)),
            dma((parts + 1,)),
        ],
        compiler_params=pltpu.CompilerParams(
            collective_id=0, has_side_effects=True, vmem_limit_bytes=56 * 1024 * 1024),
    )(*operands)


def solution(mesh):
    row, col, both = P("tp", None), P("tp"), P("sp", "tp")
    in_specs = (both,) * 8 + (
        row, row, both, col, col, P("sp", None), P("sp", None),
        P("sp", "tp", None), P("sp", "tp", None), P("sp", None, "tp"), row, row, P(None, "tp"))
    return jax.shard_map(shards, mesh=mesh, in_specs=in_specs, out_specs=both, check_vma=False)
```
